32 devices in a mesh: kv: 16 (over z, y, x), tp: 2 (over core).
Axes of the slice: x: 2, y: 2, z: 4, core: 2. Of those that a mesh axis runs over, the one named last changes fastest.
Arguments:
- tokens: bfloat16 [64, 2048], P('tp', 'kv'), may hold values from -60 to 60
- gain_mix: float32 [2048], P('kv'), may hold values from 0.1 to 1.9
- w_query: bfloat16 [2048, 2048], P('kv', 'tp'), may hold values from -0.125 to 0.125
- w_key: bfloat16 [2048, 2048], P('kv', 'tp'), may hold values from -0.125 to 0.125
- w_value: bfloat16 [2048, 2048], P('kv', 'tp'), may hold values from -0.125 to 0.125
- w_igate: bfloat16 [2048, 8], P('kv', 'tp'), may hold values from -0.125 to 0.125
- w_fgate: bfloat16 [2048, 8], P('kv', 'tp'), may hold values from -0.125 to 0.125
- bias_igate: float32 [8], P('tp'), may hold values from -3 to 3
- bias_fgate: float32 [8], P('tp'), may hold values from -3 to 3
- state_mem: float32 [64, 8, 256, 256], P('kv', 'tp'), may hold values from -2 to 2
- state_max: float32 [64, 8], P('kv', 'tp'), may hold values from -60 to 220
- keys_blk: bfloat16 [64, 8, 128, 256], P('kv', 'tp'), may hold values from -6 to 6
- values_blk: bfloat16 [64, 8, 128, 256], P('kv', 'tp'), may hold values from -6 to 6
- igate_blk: float32 [64, 8, 128], P('kv', 'tp'), may hold values from -10 to 220
- fgate_blk: float32 [64, 8, 128], P('kv', 'tp'), may hold values from -3 to 0
- lengths: int32 [64], P('kv'), may hold values from 1 to 127, 2048 in all
- gain_head: float32 [256], replicated, may hold values from 0.1 to 1.9
- w_mixout: bfloat16 [2048, 2048], P('tp', 'kv'), may hold values from -0.25 to 0.25
- gain_mlp: float32 [2048], P('kv'), may hold values from 0.1 to 1.9
- w_up: bfloat16 [2048, 8192], P('kv', 'tp'), may hold values from -0.125 to 0.125
- w_down: bfloat16 [8192, 2048], P('tp', 'kv'), may hold values from -0.0625 to 0.0625
Outputs:
- layer_out: bfloat16 [64, 2048], P('tp', 'kv')
The draws below stay inside these ranges and needn't reach their ends.
Inputs may be any that keep to these rules, and one draw needn't show every extreme that they name: `lengths`: entries of a sequence's block at or past its length are not live. The largest length is reached in every draw.
All inputs are finite; a program needn't handle non-finite values.
Results may differ from the reference program's by a relative error of at most 0.015.
Values may be sent and summed in bfloat16 or wider, within the bound.
A program may use at most 64 MiB of HBM per device.

```python
import math
import jax
import jax.numpy as jnp
import numpy as np
from jax import lax

D = 2048
CELL_FACETS = 8
HD = 256
FF = 8192
SEGMENT_LENGTH = 128
STREAM_TOTAL = 64
D_ML = 2048
N_TP = 2


def draw_tokens(key, part):
    addressing_arrays = jax.random.split(key, 1)
    base = jax.random.normal(addressing_arrays[0], (STREAM_TOTAL, D), jnp.float32)
    columns = jnp.exp(jnp.log(0.4) + jnp.log(10.0) * jnp.arange(D, dtype=jnp.float32) / (D - 1))
    values = jnp.clip(base, -6.0, 6.0)
    return jnp.clip(values * columns[None, :], -60.0, 60.0).astype(jnp.bfloat16)


def draw_state_max(key, part):
    return jax.random.uniform(key, (STREAM_TOTAL, CELL_FACETS), jnp.float32, -1.0, 2.0)


def draw_igate_blk(key, part):
    addressing_arrays = jax.random.split(key, 1)
    return jnp.clip(jax.random.normal(addressing_arrays[0], (STREAM_TOTAL, CELL_FACETS, SEGMENT_LENGTH), jnp.float32), -6.0, 6.0)


def draw_fgate_blk(key, part):
    addressing_arrays = jax.random.split(key, 7)
    share = 0.5
    quick = jax.random.bernoulli(addressing_arrays[0], share, (STREAM_TOTAL, CELL_FACETS, 1))
    quick_rate = jax.random.uniform(addressing_arrays[1], (STREAM_TOTAL, CELL_FACETS, 1), jnp.float32, 2.0, 4.0) / 40.0
    slow_rate = jax.random.uniform(addressing_arrays[2], (STREAM_TOTAL, CELL_FACETS, 1), jnp.float32, 0.1, 0.8) / SEGMENT_LENGTH
    seqfactor = jnp.exp(jax.random.uniform(addressing_arrays[3], (STREAM_TOTAL, 1, 1), jnp.float32, jnp.log(0.5), jnp.log(2.0)))
    shrinking_quotient = jnp.where(quick, quick_rate, slow_rate) * seqfactor
    arbitrary_shift = jax.random.uniform(addressing_arrays[4], (STREAM_TOTAL, CELL_FACETS, SEGMENT_LENGTH), jnp.float32, 0.5, 1.5)
    segment_clusters = jax.random.bernoulli(addressing_arrays[5], 3.0 / SEGMENT_LENGTH, (STREAM_TOTAL, CELL_FACETS, SEGMENT_LENGTH))
    training_loss = jnp.log(jax.random.uniform(addressing_arrays[6], (STREAM_TOTAL, CELL_FACETS, SEGMENT_LENGTH), jnp.float32, 0.5, 0.8))
    return -shrinking_quotient * arbitrary_shift + jnp.where(segment_clusters, training_loss, 0.0)


def level_of(own_key, dims, cuts, least, high):
    gain, own = 1.0, jax.random.fold_in(own_key, 6)
    for position, blocks in cuts:
        draws = jnp.exp(jax.random.uniform(jax.random.fold_in(own, position), (blocks,), jnp.float32, least / len(cuts), high / len(cuts)))
        gain = gain * jnp.repeat(draws, dims[position] // blocks).reshape([-1 if axis == position else 1 for axis in range(len(dims))])
    return gain


def split_up(count, total, most, skew):
    portions = [(1 << 20) // math.isqrt(standing ** skew) + 1 for standing in range(2, count + 1)]
    rest, holding = total - most - (count - 1), [1] * (count - 1)
    while rest > 0:
        candidates = [i for i in range(count - 1) if holding[i] < most]
        whole, budget = sum([portions[i] for i in candidates]), rest
        for i in candidates:
            extra = min(most - holding[i], max(1, budget * portions[i] // whole), rest)
            holding[i] = holding[i] + extra
            rest = rest - extra
    return np.array([most] + holding)


def ragged(rng, amount, total, reach, lean):
    if amount == 2:
        one = jax.random.randint(rng, (), max(1, total - reach), min(reach, total - 1) + 1)
        return jnp.stack([one, total - one])
    sizes = jnp.asarray(split_up(amount, total, reach, lean), jnp.int32)
    couples = (amount - 1) // 2
    giver, sink = sizes[1:1 + 2 * couples:2], sizes[2:2 + 2 * couples:2]
    room = jnp.minimum(giver - 1, reach - sink)
    moved = jax.random.randint(jax.random.fold_in(rng, 1), (couples,), 0, 1 << 20) % (room + 1)
    sizes = sizes.at[1:1 + 2 * couples:2].set(giver - moved).at[2:2 + 2 * couples:2].set(sink + moved)
    return sizes[jax.random.permutation(jax.random.fold_in(rng, 2), amount)]


def noise(own_key, dims, width, limit, shards=(), kind=jnp.bfloat16):
    entries = jax.random.normal(own_key, dims, jnp.float32) * width
    if len(shards) > 0:
        entries = level_of(own_key, dims, shards, -0.22, 0.18) * entries
    return jnp.clip(entries, min=-limit, max=limit).astype(kind)


def setup_inputs(seed: int = 0) -> dict:
    key_of = jax.random.split(jax.random.key(seed), 22)
    return {
        "tokens": draw_tokens(jax.random.fold_in(key_of[21], 71), 0),
        "gain_mix": jnp.clip(1.0 + 0.18 * jax.random.normal(key_of[1], (D,), jnp.float32), 0.1, 1.9),
        "w_query": noise(key_of[2], (D, D_ML), D ** -0.5, 0.125, ((0, 16), (1, 2))),
        "w_key": noise(key_of[3], (D, D_ML), D ** -0.5, 0.125, ((0, 16), (1, 2))),
        "w_value": noise(key_of[4], (D, D_ML), D ** -0.5, 0.125, ((0, 16), (1, 2))),
        "w_igate": noise(key_of[5], (D, CELL_FACETS), D ** -0.5, 0.125, ((0, 16), (1, 2))),
        "w_fgate": noise(key_of[6], (D, CELL_FACETS), D ** -0.5, 0.125, ((0, 16), (1, 2))),
        "bias_igate": noise(key_of[7], (CELL_FACETS,), 1.0, 3.0, ((0, 2),), jnp.float32),
        "bias_fgate": noise(key_of[8], (CELL_FACETS,), 1.0, 3.0, ((0, 2),), jnp.float32),
        "state_mem": noise(key_of[9], (STREAM_TOTAL, CELL_FACETS, HD, HD), 0.3, 2.0, ((0, 16), (1, 2)), jnp.float32),
        "state_max": draw_state_max(jax.random.fold_in(key_of[21], 71), 0),
        "keys_blk": noise(key_of[11], (STREAM_TOTAL, CELL_FACETS, SEGMENT_LENGTH, HD), 1.0, 6.0, ((0, 16), (1, 2))),
        "values_blk": noise(key_of[12], (STREAM_TOTAL, CELL_FACETS, SEGMENT_LENGTH, HD), 1.0, 6.0, ((0, 16), (1, 2))),
        "igate_blk": draw_igate_blk(jax.random.fold_in(key_of[21], 71), 0),
        "fgate_blk": draw_fgate_blk(jax.random.fold_in(key_of[21], 71), 0),
        "lengths": ragged(key_of[15], STREAM_TOTAL, STREAM_TOTAL * SEGMENT_LENGTH // 4, SEGMENT_LENGTH - 1, 2).astype(jnp.int32),
        "gain_head": jnp.clip(1.0 + 0.18 * jax.random.normal(key_of[16], (HD,), jnp.float32), 0.1, 1.9),
        "w_mixout": noise(key_of[17], (D_ML, D), (D_ML // 4) ** -0.5, 0.25, ((0, 2), (1, 16))),
        "gain_mlp": jnp.clip(1.0 + 0.18 * jax.random.normal(key_of[18], (D,), jnp.float32), 0.1, 1.9),
        "w_up": noise(key_of[19], (D, FF), D ** -0.5, 0.125, ((0, 16), (1, 2))),
        "w_down": noise(key_of[20], (FF, D), FF ** -0.5, 0.0625, ((0, 2), (1, 16))),
    }


EPS = 1e-06

def rms_factor(values):
    return lax.rsqrt(lax.optimization_barrier(jnp.mean(values * values, axis=-1, keepdims=True)) + EPS)

def memory_cell(query, key_new, value_new, input_gate, forget_gate, state_mem, state_max, keys_blk, values_blk, igate_blk, fgate_blk, lengths, gain_head):
    span = keys_blk.shape[2]
    head_size = query.shape[-1]
    positions = jnp.arange(span, dtype=jnp.int32)
    live_mask = positions[None, None, :] < lengths.astype(jnp.int32)[:, None, None]
    forget_live = jnp.where(live_mask, fgate_blk, 0.0)
    cumulative = jnp.cumsum(forget_live, axis=-1)
    total = cumulative[..., -1]
    suffix = total[..., None] - cumulative + forget_gate[..., None]
    past = igate_blk + suffix
    carried = state_max + total + forget_gate
    topmost = jnp.maximum(jnp.maximum(carried, input_gate), lax.optimization_barrier(jnp.max(jnp.where(live_mask, past, -jnp.inf), axis=-1)))
    scale = head_size ** (-0.5)
    query_f = query.astype(jnp.float32)
    scores = jnp.einsum('bhd,bhsd->bhs', query_f, keys_blk.astype(jnp.float32)) * scale
    weights = (jnp.where(live_mask, jnp.exp(past - topmost[..., None]), 0.0) * scores).astype(jnp.bfloat16)
    block_term = jnp.einsum('bhs,bhsd->bhd', weights.astype(jnp.float32), values_blk.astype(jnp.float32))
    state_term = jnp.einsum('bhvk,bhk->bhv', state_mem, query_f, precision=lax.Precision.HIGHEST) * jnp.exp(carried - topmost)[..., None]
    own_score = lax.optimization_barrier(jnp.sum(query_f * key_new.astype(jnp.float32), axis=-1)) * scale
    own_term = (jnp.exp(input_gate - topmost) * own_score)[..., None] * value_new.astype(jnp.float32)
    numerator = state_term + block_term + own_term
    normed = numerator * rms_factor(numerator) * gain_head
    return normed.astype(jnp.bfloat16).reshape(query.shape[0], -1)

def grouped_sum(left, right):
    left_groups = left.reshape(left.shape[0], N_TP, -1).astype(jnp.float32)
    right_groups = right.reshape(N_TP, -1, right.shape[1]).astype(jnp.float32)
    partials = jnp.einsum('bgc,gcd->gbd', left_groups, right_groups)
    rounded = lax.optimization_barrier(partials.astype(jnp.bfloat16))
    return lax.optimization_barrier(jnp.sum(rounded.astype(jnp.float32), axis=0))

def reference(tokens, gain_mix, w_query, w_key, w_value, w_igate, w_fgate, bias_igate, bias_fgate, state_mem, state_max, keys_blk, values_blk, igate_blk, fgate_blk, lengths, gain_head, w_mixout, gain_mlp, w_up, w_down):
    widened = tokens.astype(jnp.float32)
    factor_in = rms_factor(widened)
    scaled_in = (widened * gain_mix).astype(jnp.bfloat16)

    def project(weight):
        return jnp.dot(scaled_in, weight, preferred_element_type=jnp.float32) * factor_in
    query = project(w_query).astype(jnp.bfloat16).reshape(STREAM_TOTAL, CELL_FACETS, HD)
    key_new = project(w_key).astype(jnp.bfloat16).reshape(STREAM_TOTAL, CELL_FACETS, HD)
    value_new = project(w_value).astype(jnp.bfloat16).reshape(STREAM_TOTAL, CELL_FACETS, HD)
    input_gate = project(w_igate) + bias_igate
    forget_gate = jax.nn.log_sigmoid(project(w_fgate) + bias_fgate)
    mixed = memory_cell(query, key_new, value_new, input_gate, forget_gate, state_mem, state_max, keys_blk, values_blk, igate_blk, fgate_blk, lengths, gain_head)
    attended = grouped_sum(mixed, w_mixout)
    residual = (widened + attended).astype(jnp.bfloat16)
    restored = residual.astype(jnp.float32)
    factor_mid = rms_factor(restored)
    scaled_mid = (restored * gain_mlp).astype(jnp.bfloat16)
    upward = jnp.dot(scaled_mid, w_up, preferred_element_type=jnp.float32) * factor_mid
    hidden = jnp.square(jax.nn.relu(upward)).astype(jnp.bfloat16)
    return (restored + grouped_sum(hidden, w_down)).astype(jnp.bfloat16)
```

```python
import functools
from types import SimpleNamespace

import jax
import jax.numpy as jnp
from jax import lax
from jax.experimental import pallas as pl
from jax.experimental.pallas import tpu as pltpu
from jax.sharding import PartitionSpec as P

EPS = 1e-06
F32 = jnp.float32
BF16 = jnp.bfloat16
MESH = pl.DeviceIdType.MESH


def ceil_chunks(width):
    return 2 if width % 256 == 0 else 1


def inner_size(count):
    return max(d for d in range(1, count + 1) if count % d == 0 and d * d <= count)


def any_kernel(
    cfg,
    tokens,
    gain_mix,
    w_query,
    w_key,
    w_value,
    w_igate,
    w_fgate,
    bias_igate,
    bias_fgate,
    state_mem,
    state_max,
    keys_blk,
    values_blk,
    igate_blk,
    fgate_blk,
    lengths,
    gain_head,
    w_mixout,
    gain_mlp,
    w_up,
    w_down,
    out,
    wq_v,
    wk_v,
    wv_v,
    state_v,
    state_hi,
    state_lo,
    keys_v,
    values_v,
    wo_v,
    wu_v,
    wd_v,
    tok_all,
    proj_send,
    proj_recv,
    gate_send,
    gate_recv,
    mixed_all,
    mixed_rows,
    att_all,
    res_rows,
    sq_send,
    sq_recv,
    up_send,
    up_recv,
    hid_all,
    hid_rows,
    down_send,
    down_recv,
    local_sem,
    tok_ssem,
    tok_rsem,
    proj_ssem,
    proj_rsem,
    gate_ssem,
    gate_rsem,
    mix_ssem,
    mix_rsem,
    att_ssem,
    att_rsem,
    sq_ssem,
    sq_rsem,
    up_ssem,
    up_rsem,
    hid_ssem,
    hid_rsem,
    down_ssem,
    down_rsem,
):
    kv, tp, D = cfg
    me, core = lax.axis_index("kv"), lax.axis_index("tp")
    S, H, HD, _ = state_mem.shape
    B = keys_blk.shape[2]
    width = H * HD
    rows, feats = tokens.shape
    total_rows = rows * tp
    chunks, _, _, chunk = up_send.shape

    loads = [
        pltpu.make_async_copy(a, b, local_sem.at[i])
        for i, (a, b) in enumerate(
            (
                (w_query, wq_v),
                (w_key, wk_v),
                (w_value, wv_v),
                (state_mem, state_v),
                (keys_blk, keys_v),
                (values_blk, values_v),
                (w_mixout, wo_v),
                (w_up, wu_v),
                (w_down, wd_v),
            )
        )
    ]
    for load in loads:
        load.start()

    barrier = pltpu.get_barrier_semaphore()

    def greet_kv(d, carry):
        pl.semaphore_signal(
            barrier, inc=1, device_id=(lax.rem(me + d, kv), core), device_id_type=MESH
        )
        return carry

    def greet_tp(d, carry):
        pl.semaphore_signal(
            barrier, inc=1, device_id=(me, lax.rem(core + d, tp)), device_id_type=MESH
        )
        return carry

    lax.fori_loop(1, tp, greet_tp, 0)
    lax.fori_loop(1, kv, greet_kv, 0)

    lane = lax.broadcasted_iota(jnp.int32, (H, 128), 1)
    sub = lax.broadcasted_iota(jnp.int32, (H, 128), 0)
    pick_i = (lane == sub).astype(F32).astype(BF16)
    pick_f = (lane == sub + H).astype(F32).astype(BF16)
    w_gates = (
        jnp.dot(w_igate[...], pick_i, preferred_element_type=F32)
        + jnp.dot(w_fgate[...], pick_f, preferred_element_type=F32)
    ).astype(BF16)

    row = lax.broadcasted_iota(jnp.int32, (S, 1), 0)
    length = jnp.zeros((S, 1), jnp.int32)
    for s in range(S):
        length = jnp.where(row == s, lengths[s], length)
    live = lax.broadcasted_iota(jnp.int32, (S, B), 1) < length
    later = (
        lax.broadcasted_iota(jnp.int32, (B, B), 0) > lax.broadcasted_iota(jnp.int32, (B, B), 1)
    ).astype(F32)
    base = []
    for h in range(H):
        forget = jnp.where(live, fgate_blk[:, h, :], 0.0)
        suffix = jnp.dot(
            forget, later, preferred_element_type=F32, precision=lax.Precision.HIGHEST
        )
        past = jnp.where(live, igate_blk[:, h, :] + suffix, -jnp.inf)
        carried = state_max[:, h : h + 1] + jnp.sum(forget, axis=1, keepdims=True)
        base.append((past, jnp.max(past, axis=1, keepdims=True), carried))
    pl.semaphore_wait(barrier, kv + tp - 2)

    def to_kv(d, src, dst, ssem, rsem):
        return pltpu.make_async_remote_copy(
            src_ref=src,
            dst_ref=dst,
            send_sem=ssem,
            recv_sem=rsem,
            device_id=(lax.rem(me + d, kv), core),
            device_id_type=MESH,
        )

    def to_tp(d, src, dst, ssem, rsem):
        return pltpu.make_async_remote_copy(
            src_ref=src,
            dst_ref=dst,
            send_sem=ssem,
            recv_sem=rsem,
            device_id=(me, lax.rem(core + d, tp)),
            device_id_type=MESH,
        )

    def each(n, make, act):
        def step(d, carry):
            act(make(d))
            return carry

        lax.fori_loop(1, n, step, 0)

    start = lambda copy: copy.start()
    wait_send = lambda copy: copy.wait_send()
    wait_recv = lambda copy: copy.wait_recv()


    inner = inner_size(kv)
    outer = kv // inner
    z, p = me // inner, lax.rem(me, inner)

    def at(dz, dp):
        return lax.rem(z + dz + outer, outer) * inner + lax.rem(p + dp + inner, inner)

    def remote(src, dst, ssem, rsem, target):
        return pltpu.make_async_remote_copy(
            src_ref=src,
            dst_ref=dst,
            send_sem=ssem,
            recv_sem=rsem,
            device_id=(target, core),
            device_id_type=MESH,
        )

    def rs_inner(send, recv, ssem, rsem, dz, dp):
        i = dz * inner + dp
        return remote(send(at(dz, dp)), recv(i), ssem(i), rsem(i), at(0, dp))

    def rs_outer(send, recv, ssem, rsem, dz):
        i = dz * inner
        return remote(send(at(dz, 0)), recv(i), ssem(i), rsem(i), at(dz, 0))

    def rs_start(refs):
        for dz in list(range(1, outer)) + [0]:
            each(inner, lambda dp, dz=dz: rs_inner(*refs, dz, dp), start)

    def rs_group(refs, dz):
        send, recv = refs[:2]

        def add(dp, total):
            rs_inner(*refs, dz, dp).wait_recv()
            return total + recv(dz * inner + dp)[...].astype(F32)

        return lax.fori_loop(1, inner, add, send(at(dz, 0))[...].astype(F32))

    def rs_middle(refs):
        send = refs[0]
        for dz in range(1, outer):
            send(at(dz, 0))[...] = rs_group(refs, dz).astype(BF16)
            rs_outer(*refs, dz).start()

    def rs_end(refs):
        recv = refs[1]

        def add(dz, total):
            rs_outer(*refs, dz).wait_recv()
            return total + recv(dz * inner)[...].astype(F32)

        return lax.fori_loop(1, outer, add, rs_group(refs, 0))

    def rs_close(refs):
        for dz in range(outer):
            each(inner, lambda dp, dz=dz: rs_inner(*refs, dz, dp), wait_send)
        each(outer, lambda dz: rs_outer(*refs, dz), wait_send)

    def ag_outer(block, ssem, rsem, dz, slot):
        i = dz * inner
        return remote(block(slot), block(slot), ssem(i), rsem(i), at(dz, 0))

    def ag_inner(block, ssem, rsem, dz, dp, slot):
        i = dz * inner + dp
        return remote(block(slot), block(slot), ssem(i), rsem(i), at(0, dp))

    def ag_start(refs):
        each(outer, lambda dz: ag_outer(*refs, dz, me), start)
        each(inner, lambda dp: ag_inner(*refs, 0, dp, me), start)

    def ag_relay(refs):
        for dz in range(1, outer):
            ag_outer(*refs, dz, at(-dz, 0)).wait_recv()
            each(inner, lambda dp, dz=dz: ag_inner(*refs, dz, dp, at(-dz, 0)), start)

    def ag_end(refs):
        for dz in range(outer):
            each(inner, lambda dp, dz=dz: ag_inner(*refs, dz, dp, at(-dz, -dp)), wait_recv)

    def ag_close(refs):
        each(outer, lambda dz: ag_outer(*refs, dz, me), wait_send)
        for dz in range(outer):
            each(inner, lambda dp, dz=dz: ag_inner(*refs, dz, dp, at(-dz, 0)), wait_send)

    def views(c, *refs):
        return tuple(lambda i, ref=ref: ref.at[c, i] for ref in refs)

    def tok_out(d):
        return to_tp(d, tokens, tok_all.at[core], tok_ssem.at[d], tok_rsem.at[d])

    def tok_in(d):
        slot = lax.rem(core - d + tp, tp)
        return to_tp(d, tokens, tok_all.at[slot], tok_ssem.at[d], tok_rsem.at[d])

    each(tp, tok_out, start)
    tok_all[core] = tokens[...]

    each(tp, tok_in, wait_recv)
    widened = tok_all[...].astype(F32).reshape(total_rows, feats)
    square_in = jnp.sum(widened * widened, axis=1, keepdims=True)
    scaled_in = (widened * gain_mix[...]).astype(BF16)

    gates = jnp.dot(scaled_in, w_gates, preferred_element_type=F32)
    lane_r = lax.broadcasted_iota(jnp.int32, gates.shape, 1)
    gates = jnp.where(lane_r == 2 * H, square_in, gates)
    for j in range(kv):
        gate_send[j] = gates[j * S : (j + 1) * S]

    def gate_out(d):
        return to_kv(
            d, gate_send.at[lax.rem(me + d, kv)], gate_recv.at[d], gate_ssem.at[d], gate_rsem.at[d]
        )

    each(kv, gate_out, start)

    proj_refs = [views(i, proj_send, proj_recv, proj_ssem, proj_rsem) for i in range(1)]
    for i, w in enumerate((wq_v, wk_v, wv_v)):
        loads[i].wait()
        part = jnp.dot(scaled_in, w[...], preferred_element_type=F32)
        for j in range(kv):
            proj_send[0, j, :, i * width : (i + 1) * width] = part[j * S : (j + 1) * S].astype(BF16)
    rs_start(proj_refs[0])

    for refs in proj_refs:
        rs_middle(refs)
    loads[3].wait()

    def split(i, carry):
        s, h = i // H, lax.rem(i, H)
        full = state_v[s, h]
        hi = full.astype(BF16)
        state_hi[s, h] = hi
        state_lo[s, h] = (full - hi.astype(F32)).astype(BF16)
        return carry

    lax.fori_loop(0, S * H, split, 0)
    loads[4].wait()
    loads[5].wait()

    def gate_add(d, total):
        gate_out(d).wait_recv()
        return total + gate_recv[d]

    gate_sum = lax.fori_loop(1, kv, gate_add, gate_send[me])
    factor_in = lax.rsqrt(gate_sum[:, 2 * H : 2 * H + 1] / D + EPS)
    gate_sum = gate_sum * factor_in

    projected = (rs_end(proj_refs[0]) * factor_in).astype(BF16)
    query, key_new, value_new = (projected[:, i * width : (i + 1) * width] for i in range(3))

    scale = HD ** (-0.5)
    contract = (((1,), (1,)), ((), ()))
    mixed = []
    for h in range(H):
        cols = slice(h * HD, (h + 1) * HD)
        q, k, v = query[:, cols], key_new[:, cols], value_new[:, cols]
        past, past_top, carried = base[h]
        ig = gate_sum[:, h : h + 1] + bias_igate[h]
        raw = gate_sum[:, H + h : H + h + 1] + bias_fgate[h]
        fg = jnp.minimum(raw, 0.0) - jnp.log1p(jnp.exp(-jnp.abs(raw)))
        carried = carried + fg
        top = jnp.maximum(jnp.maximum(carried, ig), past_top + fg)
        decay = jnp.exp(past + (fg - top))
        scores = jnp.zeros((S, B), F32)
        state_term = jnp.zeros((S, HD), F32)
        for s in range(S):
            mine = row == s
            got = lax.dot_general(q, keys_v[s, h], contract, preferred_element_type=F32)
            scores = jnp.where(mine, got, scores)
            mem = lax.dot_general(
                q, state_hi[s, h], contract, preferred_element_type=F32
            ) + lax.dot_general(q, state_lo[s, h], contract, preferred_element_type=F32)
            state_term = jnp.where(mine, mem, state_term)
        weights = (decay * (scores * scale)).astype(BF16)
        block_term = jnp.zeros((S, HD), F32)
        for s in range(S):
            got = jnp.dot(weights, values_v[s, h], preferred_element_type=F32)
            block_term = jnp.where(row == s, got, block_term)
        own = jnp.sum(q.astype(F32) * k.astype(F32), axis=1, keepdims=True) * scale
        numerator = (
            state_term * jnp.exp(carried - top)
            + block_term
            + (jnp.exp(ig - top) * own) * v.astype(F32)
        )
        spread = jnp.mean(numerator * numerator, axis=1, keepdims=True)
        mixed_all[me, :, cols] = (numerator * lax.rsqrt(spread + EPS) * gain_head[...]).astype(BF16)

    def mix_out(d):
        return to_kv(d, mixed_all.at[me], mixed_all.at[me], mix_ssem.at[d], mix_rsem.at[d])

    def mix_in(d):
        slot = lax.rem(me - d + kv, kv)
        return to_kv(d, mixed_all.at[me], mixed_all.at[slot], mix_ssem.at[d], mix_rsem.at[d])

    each(kv, mix_out, start)
    for i in (6, 7, 8):
        loads[i].wait()
    each(kv, mix_in, wait_recv)
    for j in range(kv):
        mixed_rows[j * S : (j + 1) * S] = mixed_all[j].astype(F32)
    att_all[core] = jnp.dot(
        mixed_rows[...].astype(BF16), wo_v[...], preferred_element_type=F32
    ).astype(BF16)

    def att_out(d):
        return to_tp(d, att_all.at[core], att_all.at[core], att_ssem.at[d], att_rsem.at[d])

    def att_in(d):
        slot = lax.rem(core - d + tp, tp)
        return to_tp(d, att_all.at[core], att_all.at[slot], att_ssem.at[d], att_rsem.at[d])

    each(tp, att_out, start)
    each(tp, att_in, wait_recv)
    attended = att_all[0].astype(F32)
    for t in range(1, tp):
        attended = attended + att_all[t].astype(F32)
    restored = (widened + attended).astype(BF16).astype(F32)
    res_rows[...] = restored.reshape(tp, rows, feats)
    square_mid = jnp.sum(restored * restored, axis=1, keepdims=True)
    square_wide = jnp.broadcast_to(square_mid, (total_rows, 128))
    for j in range(kv):
        sq_send[j] = square_wide[j * S : (j + 1) * S]

    def sq_out(d):
        return to_kv(
            d, sq_send.at[lax.rem(me + d, kv)], sq_recv.at[d], sq_ssem.at[d], sq_rsem.at[d]
        )

    each(kv, sq_out, start)
    scaled_mid = (restored * gain_mlp[...]).astype(BF16)

    up_refs = [views(c, up_send, up_recv, up_ssem, up_rsem) for c in range(chunks)]
    hid_refs = [views(c, hid_all, hid_ssem, hid_rsem) for c in range(chunks)]

    for c in range(chunks):
        part = jnp.dot(
            scaled_mid, wu_v[:, c * chunk : (c + 1) * chunk], preferred_element_type=F32
        )
        for j in range(kv):
            up_send[c, j] = part[j * S : (j + 1) * S].astype(BF16)
        rs_start(up_refs[c])

    def sq_add(d, total):
        sq_out(d).wait_recv()
        return total + sq_recv[d]

    square_sum = lax.fori_loop(1, kv, sq_add, sq_send[me])
    factor_mid = lax.rsqrt(square_sum[:, 0:1] / D + EPS)

    for refs in up_refs:
        rs_middle(refs)
    for c in range(chunks):
        active = jnp.maximum(rs_end(up_refs[c]) * factor_mid, 0.0)
        hid_all[c, me] = (active * active).astype(BF16)
        ag_start(hid_refs[c])
        if c > 0:
            ag_relay(hid_refs[c - 1])
    ag_relay(hid_refs[-1])

    down = jnp.zeros((total_rows, feats), F32)
    for c in range(chunks):
        ag_end(hid_refs[c])
        for j in range(kv):
            hid_rows[j * S : (j + 1) * S] = hid_all[c, j].astype(F32)
        down = down + jnp.dot(
            hid_rows[...].astype(BF16),
            wd_v[c * chunk : (c + 1) * chunk],
            preferred_element_type=F32,
        )
    down_send[...] = down.astype(BF16).reshape(tp, rows, feats)

    def down_out(d):
        return to_tp(
            d, down_send.at[lax.rem(core + d, tp)], down_recv.at[d], down_ssem.at[d], down_rsem.at[d]
        )

    each(tp, down_out, start)

    each(tp, tok_out, wait_send)
    each(kv, gate_out, wait_send)
    for refs in proj_refs + up_refs:
        rs_close(refs)
    for refs in hid_refs:
        ag_close(refs)
    each(kv, mix_out, wait_send)
    each(tp, att_out, wait_send)
    each(kv, sq_out, wait_send)

    def down_add(d, total):
        down_out(d).wait_recv()
        return total + down_recv[d].astype(F32)

    total = lax.fori_loop(1, tp, down_add, down_send[core].astype(F32))
    out[...] = (res_rows[core] + total).astype(out.dtype)
    each(tp, down_out, wait_send)


def any_body(kv, tp, *args):
    (
        tokens,
        gain_mix,
        w_query,
        w_key,
        w_value,
        w_igate,
        w_fgate,
        bias_igate,
        bias_fgate,
        state_mem,
        state_max,
        keys_blk,
        values_blk,
        igate_blk,
        fgate_blk,
        lengths,
        gain_head,
        w_mixout,
        gain_mlp,
        w_up,
        w_down,
    ) = args
    rows, feats = tokens.shape
    S, H, HD, _ = state_mem.shape
    width = H * HD
    hidden = w_up.shape[1]
    chunks = ceil_chunks(hidden)
    chunk = hidden // chunks
    vm = pl.BlockSpec(memory_space=pltpu.VMEM)
    sm = pl.BlockSpec(memory_space=pltpu.SMEM)
    hbm = pl.BlockSpec(memory_space=pl.ANY)
    in_specs = [
        vm,
        vm,
        hbm,
        hbm,
        hbm,
        vm,
        vm,
        sm,
        sm,
        hbm,
        vm,
        hbm,
        hbm,
        vm,
        vm,
        sm,
        vm,
        hbm,
        vm,
        hbm,
        hbm,
    ]
    V = pltpu.VMEM
    dma = pltpu.SemaphoreType.DMA
    scratch = [
        V(w_query.shape, BF16),
        V(w_key.shape, BF16),
        V(w_value.shape, BF16),
        V(state_mem.shape, F32),
        V(state_mem.shape, BF16),
        V(state_mem.shape, BF16),
        V(keys_blk.shape, BF16),
        V(values_blk.shape, BF16),
        V(w_mixout.shape, BF16),
        V(w_up.shape, BF16),
        V(w_down.shape, BF16),
        V((tp, rows, feats), BF16),
        V((1, kv, S, 3 * width), BF16),
        V((1, kv, S, 3 * width), BF16),
        V((kv, S, 128), F32),
        V((kv, S, 128), F32),
        V((kv, S, width), BF16),
        V((kv * S, width), F32),
        V((tp, kv * S, feats), BF16),
        V((tp, rows, feats), F32),
        V((kv, S, 128), F32),
        V((kv, S, 128), F32),
        V((chunks, kv, S, chunk), BF16),
        V((chunks, kv, S, chunk), BF16),
        V((chunks, kv, S, chunk), BF16),
        V((kv * S, chunk), F32),
        V((tp, rows, feats), BF16),
        V((tp, rows, feats), BF16),
        dma((9,)),
        dma((tp,)),
        dma((tp,)),
        dma((1, kv)),
        dma((1, kv)),
        dma((kv,)),
        dma((kv,)),
        dma((kv,)),
        dma((kv,)),
        dma((tp,)),
        dma((tp,)),
        dma((kv,)),
        dma((kv,)),
        dma((chunks, kv)),
        dma((chunks, kv)),
        dma((chunks, kv)),
        dma((chunks, kv)),
        dma((tp,)),
        dma((tp,)),
    ]
    return pl.pallas_call(
        functools.partial(any_kernel, (kv, tp, kv * feats)),
        out_shape=jax.ShapeDtypeStruct((rows, feats), BF16),
        in_specs=in_specs,
        out_specs=vm,
        scratch_shapes=scratch,
        compiler_params=pltpu.CompilerParams(
            collective_id=0, has_side_effects=True, vmem_limit_bytes=56 * 1024 * 1024
        ),
    )(
        tokens,
        gain_mix.reshape(1, -1),
        w_query,
        w_key,
        w_value,
        w_igate,
        w_fgate,
        bias_igate,
        bias_fgate,
        state_mem,
        state_max,
        keys_blk,
        values_blk,
        igate_blk,
        fgate_blk,
        lengths,
        gain_head.reshape(1, -1),
        w_mixout,
        gain_mlp.reshape(1, -1),
        w_up,
        w_down,
    )


def flip(index, mask):
    bit = 1
    while bit <= mask:
        if mask & bit:
            index = index + bit * (1 - 2 * lax.rem(lax.div(index, bit), 2))
        bit *= 2
    return index


def stages(kv):
    inner = inner_size(kv)
    outer = kv // inner
    if (inner, outer) != (4, 4):
        return (([m for m in range(inner)], [m * inner for m in range(outer)]),)
    ways = (((1, 2), (4, 8)), ((1, 4), (2, 8)), ((2, 4), (1, 8)))
    return tuple(tuple([0, a, b, a + b] for a, b in way) for way in ways)


def kernel(cfg, names, *refs):
    kv, tp, D = cfg
    r = SimpleNamespace(**dict(zip(names, refs, strict=True)))
    me, core = lax.axis_index("kv"), lax.axis_index("tp")
    inner = inner_size(kv)
    outer = kv // inner
    other = 1 - core
    ways = stages(kv)

    def split(way):
        def place(masks):
            total, step = 0, 1
            while step < len(masks):
                total = total + step * lax.rem(lax.div(me, masks[step]), 2)
                step *= 2
            return total

        return place(way[1]), place(way[0])
    S, H, HD, _ = r.state_mem.shape
    B = r.fgate_blk.shape[2]
    width = H * HD
    R, F = r.tokens.shape
    per = kv // tp
    half = lax.div(me, per)
    jj_me = lax.rem(me, per)
    chunks, _, _, CW = r.up_send.shape
    proj_way = [ways[a % len(ways)] for a in range(3)]
    up_way = [ways[c % len(ways)] for c in range(chunks)]

    barrier = pltpu.get_barrier_semaphore()

    def greet(target, c):
        pl.semaphore_signal(barrier, inc=1, device_id=(target, c), device_id_type=MESH)

    for m in reversed(range(1, kv)):
        target = flip(me, m)
        greet(target, core)
        greet(target, other)
    greet(me, other)

    taken = iter(range(r.local_sem.shape[0]))

    def load(whole, *pieces):
        sem = r.local_sem.at[next(taken)]
        for i, piece in enumerate(pieces):
            dst = whole if len(pieces) == 1 else whole.at[i]
            pltpu.make_async_copy(piece, dst, sem).start()
        return pltpu.make_async_copy(whole, whole, sem)

    got_tokens = load(r.v_tokens, r.tokens)
    got_gain_mix = load(r.v_gain_mix, r.gain_mix)
    got_w_gate = load(r.v_w_gate, r.w_igate, r.w_fgate)
    got_w_qkv = load(r.v_w_qkv, r.w_query, r.w_key, r.w_value)
    got_blk = [
        load(r.v_gate_blk, r.fgate_blk, r.igate_blk),
        load(r.v_lengths, r.lengths),
        load(r.v_state_max, r.state_max),
        load(r.v_bias, r.bias_igate, r.bias_fgate),
    ]
    got_memory = [
        load(r.v_state_mem, r.state_mem),
        load(r.v_kv_blk, r.keys_blk, r.values_blk),
        load(r.v_gain_head, r.gain_head),
    ]
    got_gain_mlp = load(r.v_gain_mlp, r.gain_mlp)
    got_w_mixout = load(r.v_w_mixout.at[0], r.w_mixout)
    got_w_up = load(r.v_w_up.at[0], r.w_up)
    got_w_down = load(r.v_w_down.at[0], r.w_down)

    def loaded(copies):
        for copy in copies:
            copy.wait()

    def remote(src, dst, ssem, rsem, target, c):
        return pltpu.make_async_remote_copy(
            src_ref=src,
            dst_ref=dst,
            send_sem=ssem,
            recv_sem=rsem,
            device_id=(target, c),
            device_id_type=MESH,
        )

    def drain(ref, sem):
        remote(ref, ref, sem, sem, me, other).wait_send()

    loaded([got_tokens, got_gain_mix, got_w_gate])
    lane = lax.broadcasted_iota(jnp.int32, (H, 128), 1)
    sub = lax.broadcasted_iota(jnp.int32, (H, 128), 0)
    pick_i = (lane == sub).astype(F32).astype(BF16)
    pick_f = (lane == sub + H).astype(F32).astype(BF16)
    first = (((0,), (0,)), ((), ()))
    w_gates = (
        lax.dot_general(r.v_w_gate[0], pick_i, first, preferred_element_type=F32)
        + lax.dot_general(r.v_w_gate[1], pick_f, first, preferred_element_type=F32)
    ).astype(BF16)
    lane_r = lax.broadcasted_iota(jnp.int32, (R, 128), 1)
    gain_mix = r.v_gain_mix[...]
    gate_send = r.gate_send
    proj_send, proj_recv, proj_mid, proj_last = r.proj_send, r.proj_recv, r.proj_mid, r.proj_last

    def project(rows, group):
        scaled = (rows * gain_mix).astype(BF16)
        square = jnp.sum(rows * rows, axis=1, keepdims=True)
        gates = jnp.dot(scaled, w_gates, preferred_element_type=F32)
        gates = jnp.where(lane_r == 2 * H, square, gates)
        for jj in range(per):
            gate_send[group * per + jj] = gates[jj * S : (jj + 1) * S]
        for i in range(3):
            part = jnp.dot(scaled, r.v_w_qkv[i], preferred_element_type=F32)
            for jj in range(per):
                proj_send[i, group * per + jj] = part[jj * S : (jj + 1) * S].astype(BF16)

    own_rows = r.v_tokens[...].astype(F32)
    got_w_qkv.wait()
    project(own_rows, core)

    loaded(got_blk)
    row = lax.broadcasted_iota(jnp.int32, (S, 1), 0)
    eye_s = lax.broadcasted_iota(jnp.int32, (S, S), 0) == lax.broadcasted_iota(jnp.int32, (S, S), 1)
    length = jnp.sum(
        jnp.where(eye_s, r.v_lengths[...].astype(F32), 0.0), axis=1, keepdims=True
    )
    live = lax.broadcasted_iota(jnp.int32, (S, B), 1).astype(F32) < length
    later = (
        lax.broadcasted_iota(jnp.int32, (B, B), 0) > lax.broadcasted_iota(jnp.int32, (B, B), 1)
    ).astype(F32)
    base = []
    for h in range(H):
        forget = jnp.where(live, r.v_gate_blk[0, :, h, :], 0.0)
        suffix = jnp.dot(
            forget, later, preferred_element_type=F32, precision=lax.Precision.HIGHEST
        )
        past = jnp.where(live, r.v_gate_blk[1, :, h, :] + suffix, -jnp.inf)
        carried = r.v_state_max[:, h : h + 1] + jnp.sum(forget, axis=1, keepdims=True)
        base.append((past, jnp.max(past, axis=1, keepdims=True), carried))
    pl.semaphore_wait(barrier, kv * tp - 1)

    tok_copy = remote(
        r.v_tokens, r.tok_peer, r.pair_ssem.at[0], r.pair_rsem.at[0], me, other
    )
    tok_copy.start()

    def pair(i, ref):
        return remote(ref.at[0], ref.at[1], r.pair_ssem.at[i], r.pair_rsem.at[i], me, other)

    pairs = [pair(1, r.v_w_mixout), pair(2, r.v_w_up), pair(3, r.v_w_down)]

    def proj_one(a, mz, mp):
        first, second = proj_way[a]
        return remote(
            proj_send.at[a, flip(me, first[mp] + second[mz])],
            proj_recv.at[a, mz, mp],
            r.proj_ssem,
            r.proj_rsem.at[a, mz // (outer // 2)],
            flip(me, first[mp]),
            other,
        )

    def proj_two(a, mz):
        return remote(
            proj_mid.at[a, mz],
            proj_last.at[a, mz],
            r.mid_ssem.at[0],
            r.mid_rsem.at[a],
            flip(me, proj_way[a][1][mz]),
            other,
        )

    far = [mz for mz in reversed(range(outer)) if mz >= outer // 2]
    near = [mz for mz in reversed(range(outer)) if mz < outer // 2]
    peers = list(reversed(range(inner)))

    def send_groups(a, groups):
        for mz in groups:
            for mp in peers:
                proj_one(a, mz, mp).start()

    def gate_copy(m):
        return remote(
            gate_send.at[flip(me, m)],
            r.gate_recv.at[m],
            r.gate_ssem,
            r.gate_rsem,
            flip(me, m),
            core,
        )

    far_m = [m for m in reversed(range(1, kv)) if m >= per]
    near_m = [m for m in reversed(range(1, kv)) if m < per]

    @pl.when(core != half)
    def _():
        for m in far_m:
            gate_copy(m).start()
        for a in range(3):
            send_groups(a, far)

    tok_copy.wait_recv()
    peer_rows = r.tok_peer[...].astype(F32)
    project(peer_rows, other)

    @pl.when(core == half)
    def _():
        for m in far_m:
            gate_copy(m).start()
        send_groups(0, far)

    for m in near_m:
        gate_copy(m).start()
    send_groups(0, near)

    @pl.when(core == half)
    def _():
        for a in (1, 2):
            send_groups(a, far)

    for a in (1, 2):
        send_groups(a, near)

    got_w_mixout.wait()
    pairs[0].start()

    loaded(got_memory)

    def narrow(i, carry):
        s, h = lax.div(i, H), lax.rem(i, H)
        r.state_t[s, h] = r.v_state_mem[s, h].T.astype(BF16)
        r.keys_t[s, h] = r.v_kv_blk[0, s, h].T
        return carry

    lax.fori_loop(0, S * H, narrow, 0)

    def summed(ref):
        total = ref[0].astype(F32)
        for i in range(1, ref.shape[0]):
            total = total + ref[i].astype(F32)
        return total

    def proj_middle(a):
        for side, groups in ((1, far), (0, near)):
            drain(
                proj_recv.at[a, pl.ds(side * (outer // 2), outer // 2)], r.proj_rsem.at[a, side]
            )
            for mz in groups:
                proj_mid[a, mz] = summed(proj_recv.at[a, mz]).astype(BF16)
                proj_two(a, mz).start()

    def proj_end(a):
        drain(proj_last.at[a], r.mid_rsem.at[a])
        return (summed(proj_last.at[a]) * factor_in).astype(BF16)

    proj_middle(0)
    proj_middle(1)
    proj_middle(2)
    got_w_up.wait()
    pairs[1].start()
    drain(r.gate_recv.at[pl.ds(1, kv - 1)], r.gate_rsem)
    gate_sum = gate_send[me]
    for m in range(1, kv):
        gate_sum = gate_sum + r.gate_recv[m]
    factor_in = lax.rsqrt(gate_sum[:, 2 * H : 2 * H + 1] / D + EPS)
    gate_sum = gate_sum * factor_in
    query = proj_end(0)

    scale = HD ** (-0.5)
    cells = []
    for h in range(H):
        q = query[:, h * HD : (h + 1) * HD]
        past, past_top, carried = base[h]
        ig = gate_sum[:, h : h + 1] + r.v_bias[0, :, h : h + 1]
        raw = gate_sum[:, H + h : H + h + 1] + r.v_bias[1, :, h : h + 1]
        fg = jnp.minimum(raw, 0.0) - jnp.log1p(jnp.exp(-jnp.abs(raw)))
        carried = carried + fg
        top = jnp.maximum(jnp.maximum(carried, ig), past_top + fg)
        decay = jnp.exp(past + (fg - top))
        scores = jnp.zeros((S, B), F32)
        state_term = jnp.zeros((S, HD), F32)
        for s in range(S):
            mine = row == s
            got = jnp.dot(q, r.keys_t[s, h], preferred_element_type=F32)
            scores = jnp.where(mine, got, scores)
            mem = jnp.dot(q, r.state_t[s, h], preferred_element_type=F32)
            state_term = jnp.where(mine, mem, state_term)
        weights = (decay * (scores * scale)).astype(BF16)
        block_term = jnp.zeros((S, HD), F32)
        for s in range(S):
            got = jnp.dot(weights, r.v_kv_blk[1, s, h], preferred_element_type=F32)
            block_term = jnp.where(row == s, got, block_term)
        cells.append((state_term * jnp.exp(carried - top) + block_term, jnp.exp(ig - top)))

    key_new = proj_end(1)
    value_new = proj_end(2)
    for h in range(H):
        cols = slice(h * HD, (h + 1) * HD)
        q, k, v = query[:, cols], key_new[:, cols], value_new[:, cols]
        older, entering = cells[h]
        own = jnp.sum(q.astype(F32) * k.astype(F32), axis=1, keepdims=True) * scale
        numerator = older + (entering * own) * v.astype(F32)
        spread = jnp.mean(numerator * numerator, axis=1, keepdims=True)
        r.mixed_own[:, cols] = (
            numerator * lax.rsqrt(spread + EPS) * r.v_gain_head[...]
        ).astype(BF16)

    mixed_all = r.mixed_all
    slot = lax.rem(half + core, 2)
    mine_at = slot * per + jj_me

    def mix_copy(m):
        return remote(
            r.mixed_own,
            mixed_all.at[mine_at],
            r.mix_ssem,
            r.mix_rsem,
            flip(me, m),
            half,
        )

    for m in reversed(range(1, kv)):
        mix_copy(m).start()

    @pl.when(slot == 1)
    def _():
        mix_copy(0).start()

    @pl.when(slot == 0)
    def _():
        mixed_all[mine_at] = r.mixed_own[...]

    loaded([got_w_down, got_gain_mlp])
    pairs[0].wait()

    @pl.when(half == core)
    def _():
        drain(mixed_all.at[pl.ds(0, kv - 1)], r.mix_rsem)

    @pl.when(half != core)
    def _():
        drain(mixed_all, r.mix_rsem)

    mixed_rows = r.mixed_rows
    attended = jnp.zeros((R, F), F32)
    for c in range(tp):
        for jj in range(per):
            mixed_rows[jj * S : (jj + 1) * S, c * width : (c + 1) * width] = mixed_all[
                c * per + jj
            ].astype(F32)
        attended = attended + jnp.dot(
            mixed_rows[:, c * width : (c + 1) * width].astype(BF16),
            r.v_w_mixout[c],
            preferred_element_type=F32,
        ).astype(BF16).astype(F32)

    restored = (own_rows + attended).astype(BF16).astype(F32)
    r.res_rows[...] = restored
    scaled_mid = (restored * r.v_gain_mlp[...]).astype(BF16)

    up_send, up_recv, up_mid, up_last = r.up_send, r.up_recv, r.up_mid, r.up_last

    def up_one(c, mz, mp):
        place = split(up_way[c])
        return remote(
            up_send.at[c, flip(place[0], mz) * inner + flip(place[1], mp)],
            up_recv.at[c, mz, mp],
            r.up_ssem,
            r.up_rsem.at[c, mz // (outer // 2)],
            flip(me, up_way[c][0][mp]),
            other,
        )

    def up_two(c, mz):
        return remote(
            up_mid.at[c, mz],
            up_last.at[c, mz],
            r.mid_ssem.at[1],
            r.up_lsem.at[c],
            flip(me, up_way[c][1][mz]),
            other,
        )

    parts = chunks // tp
    span = kv * CW

    def up_start(c, groups):
        for mz in groups:
            for mp in peers:
                up_one(c, mz, mp).start()

    def up_compute(c):
        if c == parts:
            pairs[1].wait()
        begin = (c % parts) * span
        part = jnp.dot(
            scaled_mid,
            r.v_w_up[c // parts, :, begin : begin + span],
            preferred_element_type=F32,
        ).astype(BF16)
        for j in range(kv):
            up_send[c, j] = part[:, j * CW : (j + 1) * CW]

    plan = [(c, side) for c in range(chunks) for side in (1, 0)]
    for i, (c, side) in enumerate(plan):
        if c not in [x for x, _ in plan[:i]]:
            up_compute(c)
        up_start(c, far if side else near)
    pairs[2].start()

    square_mid = jnp.sum(restored * restored, axis=1, keepdims=True)
    eye_r = lax.broadcasted_iota(jnp.int32, (R, 128), 0) == lane_r
    r.sq_all[0] = jnp.sum(jnp.where(eye_r, square_mid, 0.0), axis=0, keepdims=True)

    def sq_copy(m):
        return remote(
            r.sq_all.at[0],
            r.sq_all.at[m],
            r.sq_ssem,
            r.sq_rsem,
            flip(me, m),
            core,
        )

    for m in reversed(range(1, kv)):
        sq_copy(m).start()

    def up_middle(c, side):
        drain(up_recv.at[c, pl.ds(side * (outer // 2), outer // 2)], r.up_rsem.at[c, side])
        for mz in far if side else near:
            up_mid[c, mz] = summed(up_recv.at[c, mz]).astype(BF16)
            up_two(c, mz).start()

    hid_mid, hid_all = r.hid_mid, r.hid_all

    def hid_near(c, mp):
        mine = hid_all.at[c, 0, split(up_way[c])[1]]
        return remote(
            mine,
            mine,
            r.hid_ssem.at[2],
            r.hid_rsem.at[c],
            flip(me, up_way[c][0][mp]),
            core,
        )

    def hid_one(c, mz):
        return remote(
            hid_all.at[c, 0, split(up_way[c])[1]],
            hid_mid.at[c, mz],
            r.hid_ssem.at[0],
            r.hid_msem.at[c, mz - 1],
            flip(me, up_way[c][1][mz]),
            other,
        )

    def hid_two(c, mz, mp):
        return remote(
            hid_mid.at[c, mz],
            hid_all.at[c, mz, split(up_way[c])[1]],
            r.hid_ssem.at[1],
            r.hid_rsem.at[c],
            flip(me, up_way[c][0][mp]),
            other,
        )

    def hid_start(c):
        drain(up_last.at[c], r.up_lsem.at[c])
        active = jnp.maximum(summed(up_last.at[c]), 0.0)
        hid_all[c, 0, split(up_way[c])[1]] = (active * active).astype(BF16)
        for mz in reversed(range(1, outer)):
            hid_one(c, mz).start()
        for mp in peers[:-1]:
            hid_near(c, mp).start()

    def hid_relay(c, mz):
        drain(hid_mid.at[c, mz], r.hid_msem.at[c, mz - 1])
        for mp in peers:
            hid_two(c, mz, mp).start()

    def hops(mz):
        return 1.8 + 0.7 * ((mz & 1) + 2 * (mz >> 1)) if mz else 0.9

    steps, ready = [], [0.0] * chunks
    for i, (c, side) in enumerate(plan):
        due = 3.2 * (i + 1) / len(plan) + 2.8
        steps.append((due, up_middle, c, side))
        ready[c] = max([ready[c], *(due + hops(mz) for mz in (far if side else near))])
    for c in range(chunks):
        steps.append((ready[c] + 0.2, hid_start, c))
        for mz in range(1, outer):
            steps.append((ready[c] + 0.4 + hops(mz), hid_relay, c, mz))
    order = [step[1:] for step in sorted(steps, key=lambda step: step[0])]
    for step, *which in order:
        step(*which)

    tok_copy.wait_send()
    drain(r.gate_recv.at[pl.ds(1, kv - 1)], r.gate_ssem)
    drain(proj_recv, r.proj_ssem)
    drain(proj_last, r.mid_ssem.at[0])

    @pl.when(slot == 0)
    def _():
        drain(mixed_all.at[pl.ds(0, kv - 1)], r.mix_ssem)

    @pl.when(slot == 1)
    def _():
        drain(mixed_all, r.mix_ssem)

    drain(r.sq_all.at[pl.ds(1, kv - 1)], r.sq_ssem)
    drain(up_recv, r.up_ssem)
    drain(up_last, r.mid_ssem.at[1])
    pairs[2].wait()
    drain(r.sq_all.at[pl.ds(1, kv - 1)], r.sq_rsem)
    squares = r.sq_all[0]
    for m in range(1, kv):
        squares = squares + r.sq_all[m]
    square_sum = jnp.sum(jnp.where(eye_r, squares, 0.0), axis=1, keepdims=True)
    factor_mid = lax.rsqrt(square_sum / D + EPS)
    drain(hid_mid.at[:, pl.ds(1, outer - 1)], r.hid_ssem.at[0])
    drain(hid_all.at[:, 0, pl.ds(1, inner - 1)], r.hid_ssem.at[2])

    flat = r.up_send.at[0]
    down = jnp.zeros((R, F), F32)
    for c in range(chunks):
        drain(flat.at[pl.ds(0, kv - 1)], r.hid_rsem.at[c])
        for mz in range(outer):
            group = flip(split(up_way[c])[0], mz)
            begin = pl.multiple_of((c % parts) * span + group * (inner * CW), inner * CW)
            down = down + jnp.dot(
                jnp.concatenate([hid_all[c, mz, pt] for pt in range(inner)], axis=1),
                r.v_w_down[c // parts, pl.ds(begin, inner * CW), :],
                preferred_element_type=F32,
            )
    r.out[...] = (r.res_rows[...] + down * (factor_mid * factor_mid)).astype(BF16)
    drain(hid_all.at[:, pl.ds(1, outer - 1)], r.hid_ssem.at[1])


def named(
    tokens,
    gain_mix,
    w_query,
    w_key,
    w_value,
    w_igate,
    w_fgate,
    bias_igate,
    bias_fgate,
    state_mem,
    state_max,
    keys_blk,
    values_blk,
    igate_blk,
    fgate_blk,
    lengths,
    gain_head,
    w_mixout,
    gain_mlp,
    w_up,
    w_down,
):
    return SimpleNamespace(**locals())


def body(kv, tp, *args):
    a = named(*args)
    a.gain_mix, a.gain_head, a.gain_mlp, a.bias_igate, a.bias_fgate, a.lengths = (
        x.reshape(1, -1)
        for x in (a.gain_mix, a.gain_head, a.gain_mlp, a.bias_igate, a.bias_fgate, a.lengths)
    )
    a.w_igate, a.w_fgate = a.w_igate.T, a.w_fgate.T
    rows, feats = a.tokens.shape
    S, H, HD, _ = a.state_mem.shape
    B = a.keys_blk.shape[2]
    width = H * HD
    inner = inner_size(kv)
    outer = kv // inner
    per = kv // tp
    hidden = a.w_up.shape[1]
    chunks = tp * max(n for n in (1, 2) if hidden % (n * kv * 128) == 0)
    cw = hidden * tp // (chunks * kv)
    V = pltpu.VMEM
    dma = pltpu.SemaphoreType.DMA

    def room(x, *many):
        return V((*many, *x.shape), x.dtype)

    scratch = dict(
        v_tokens=room(a.tokens),
        v_gain_mix=room(a.gain_mix),
        v_lengths=room(a.lengths),
        v_state_max=room(a.state_max),
        v_gain_head=room(a.gain_head),
        v_gain_mlp=room(a.gain_mlp),
        v_state_mem=room(a.state_mem),
        v_w_gate=room(a.w_igate, 2),
        v_w_qkv=room(a.w_query, 3),
        v_gate_blk=room(a.fgate_blk, 2),
        v_bias=room(a.bias_igate, 2),
        v_kv_blk=room(a.keys_blk, 2),
        v_w_mixout=room(a.w_mixout, tp),
        v_w_up=room(a.w_up, tp),
        v_w_down=room(a.w_down, tp),
        state_t=V(a.state_mem.shape, BF16),
        keys_t=V((S, H, HD, B), BF16),
        tok_peer=room(a.tokens),
        proj_send=V((3, kv, S, width), BF16),
        proj_recv=V((3, outer, inner, S, width), BF16),
        proj_mid=V((3, outer, S, width), BF16),
        proj_last=V((3, outer, S, width), BF16),
        gate_send=V((kv, S, 128), F32),
        gate_recv=V((kv, S, 128), F32),
        mixed_own=V((S, width), BF16),
        mixed_all=V((tp * per, S, width), BF16),
        mixed_rows=V((rows, tp * width), F32),
        res_rows=V((rows, feats), F32),
        sq_all=V((kv, 1, 128), F32),
        up_send=V((chunks, kv, rows, cw), BF16),
        up_recv=V((chunks, outer, inner, rows, cw), BF16),
        up_mid=V((chunks, outer, rows, cw), BF16),
        up_last=V((chunks, outer, rows, cw), BF16),
        hid_mid=V((chunks, outer, rows, cw), BF16),
        hid_all=V((chunks, outer, inner, rows, cw), BF16),
        local_sem=dma((15,)),
        pair_ssem=dma((4,)),
        pair_rsem=dma((4,)),
        proj_ssem=dma,
        proj_rsem=dma((3, 2)),
        mid_ssem=dma((2,)),
        mid_rsem=dma((3,)),
        gate_ssem=dma,
        gate_rsem=dma,
        mix_ssem=dma,
        mix_rsem=dma,
        sq_ssem=dma,
        sq_rsem=dma,
        up_ssem=dma,
        up_rsem=dma((chunks, 2)),
        up_lsem=dma((chunks,)),
        hid_ssem=dma((3,)),
        hid_msem=dma((chunks, outer - 1)),
        hid_rsem=dma((chunks,)),
    )
    operands = vars(a)
    names = (*operands, "out", *scratch)
    return pl.pallas_call(
        functools.partial(kernel, (kv, tp, kv * feats), names),
        out_shape=V((rows, feats), BF16),
        in_specs=[pl.BlockSpec(memory_space=pl.ANY)] * len(operands),
        out_specs=pl.BlockSpec(memory_space=V),
        scratch_shapes=list(scratch.values()),
        compiler_params=pltpu.CompilerParams(
            collective_id=0, has_side_effects=True, vmem_limit_bytes=56 * 1024 * 1024
        ),
    )(*operands.values())


def suits(kv, tp, *args):
    a = named(*args)
    inner = inner_size(kv)
    outer = kv // inner
    return (
        tp == 2
        and kv & (kv - 1) == 0
        and outer > 1
        and inner > 1
        and a.tokens.shape[1] % 128 == 0
        and a.tokens.shape[0] <= 128
        and a.w_up.shape[1] % (kv * 128) == 0
    )


def either(kv, tp, *args):
    return (body if suits(kv, tp, *args) else any_body)(kv, tp, *args)


def solution(mesh):
    in_specs = (
        P("tp", "kv"),
        P("kv"),
        P("kv", "tp"),
        P("kv", "tp"),
        P("kv", "tp"),
        P("kv", "tp"),
        P("kv", "tp"),
        P("tp"),
        P("tp"),
        P("kv", "tp", None, None),
        P("kv", "tp"),
        P("kv", "tp", None, None),
        P("kv", "tp", None, None),
        P("kv", "tp", None),
        P("kv", "tp", None),
        P("kv"),
        P(),
        P("tp", "kv"),
        P("kv"),
        P("kv", "tp"),
        P("tp", "kv"),
    )
    out_specs = P("tp", "kv")
    run = functools.partial(either, mesh.shape["kv"], mesh.shape["tp"])
    return jax.shard_map(run, mesh=mesh, in_specs=in_specs, out_specs=out_specs, check_vma=False)
```

```python
import functools
from types import SimpleNamespace

import jax
import jax.numpy as jnp
from jax import lax
from jax.experimental import pallas as pl
from jax.experimental.pallas import tpu as pltpu
from jax.sharding import PartitionSpec as P

EPS = 1e-06
F32 = jnp.float32
BF16 = jnp.bfloat16
MESH = pl.DeviceIdType.MESH


def ceil_chunks(width):
    return 2 if width % 256 == 0 else 1


def inner_size(count):
    return max(d for d in range(1, count + 1) if count % d == 0 and d * d <= count)


def any_kernel(
    cfg,
    tokens,
    gain_mix,
    w_query,
    w_key,
    w_value,
    w_igate,
    w_fgate,
    bias_igate,
    bias_fgate,
    state_mem,
    state_max,
    keys_blk,
    values_blk,
    igate_blk,
    fgate_blk,
    lengths,
    gain_head,
    w_mixout,
    gain_mlp,
    w_up,
    w_down,
    out,
    wq_v,
    wk_v,
    wv_v,
    state_v,
    state_hi,
    state_lo,
    keys_v,
    values_v,
    wo_v,
    wu_v,
    wd_v,
    tok_all,
    proj_send,
    proj_recv,
    gate_send,
    gate_recv,
    mixed_all,
    mixed_rows,
    att_all,
    res_rows,
    sq_send,
    sq_recv,
    up_send,
    up_recv,
    hid_all,
    hid_rows,
    down_send,
    down_recv,
    local_sem,
    tok_ssem,
    tok_rsem,
    proj_ssem,
    proj_rsem,
    gate_ssem,
    gate_rsem,
    mix_ssem,
    mix_rsem,
    att_ssem,
    att_rsem,
    sq_ssem,
    sq_rsem,
    up_ssem,
    up_rsem,
    hid_ssem,
    hid_rsem,
    down_ssem,
    down_rsem,
):
    kv, tp, D = cfg
    me, core = lax.axis_index("kv"), lax.axis_index("tp")
    S, H, HD, _ = state_mem.shape
    B = keys_blk.shape[2]
    width = H * HD
    rows, feats = tokens.shape
    total_rows = rows * tp
    chunks, _, _, chunk = up_send.shape

    loads = [
        pltpu.make_async_copy(a, b, local_sem.at[i])
        for i, (a, b) in enumerate(
            (
                (w_query, wq_v),
                (w_key, wk_v),
                (w_value, wv_v),
                (state_mem, state_v),
                (keys_blk, keys_v),
                (values_blk, values_v),
                (w_mixout, wo_v),
                (w_up, wu_v),
                (w_down, wd_v),
            )
        )
    ]
    for load in loads:
        load.start()

    barrier = pltpu.get_barrier_semaphore()

    def greet_kv(d, carry):
        pl.semaphore_signal(
            barrier, inc=1, device_id=(lax.rem(me + d, kv), core), device_id_type=MESH
        )
        return carry

    def greet_tp(d, carry):
        pl.semaphore_signal(
            barrier, inc=1, device_id=(me, lax.rem(core + d, tp)), device_id_type=MESH
        )
        return carry

    lax.fori_loop(1, tp, greet_tp, 0)
    lax.fori_loop(1, kv, greet_kv, 0)

    lane = lax.broadcasted_iota(jnp.int32, (H, 128), 1)
    sub = lax.broadcasted_iota(jnp.int32, (H, 128), 0)
    pick_i = (lane == sub).astype(F32).astype(BF16)
    pick_f = (lane == sub + H).astype(F32).astype(BF16)
    w_gates = (
        jnp.dot(w_igate[...], pick_i, preferred_element_type=F32)
        + jnp.dot(w_fgate[...], pick_f, preferred_element_type=F32)
    ).astype(BF16)

    row = lax.broadcasted_iota(jnp.int32, (S, 1), 0)
    length = jnp.zeros((S, 1), jnp.int32)
    for s in range(S):
        length = jnp.where(row == s, lengths[s], length)
    live = lax.broadcasted_iota(jnp.int32, (S, B), 1) < length
    later = (
        lax.broadcasted_iota(jnp.int32, (B, B), 0) > lax.broadcasted_iota(jnp.int32, (B, B), 1)
    ).astype(F32)
    base = []
    for h in range(H):
        forget = jnp.where(live, fgate_blk[:, h, :], 0.0)
        suffix = jnp.dot(
            forget, later, preferred_element_type=F32, precision=lax.Precision.HIGHEST
        )
        past = jnp.where(live, igate_blk[:, h, :] + suffix, -jnp.inf)
        carried = state_max[:, h : h + 1] + jnp.sum(forget, axis=1, keepdims=True)
        base.append((past, jnp.max(past, axis=1, keepdims=True), carried))
    pl.semaphore_wait(barrier, kv + tp - 2)

    def to_kv(d, src, dst, ssem, rsem):
        return pltpu.make_async_remote_copy(
            src_ref=src,
            dst_ref=dst,
            send_sem=ssem,
            recv_sem=rsem,
            device_id=(lax.rem(me + d, kv), core),
            device_id_type=MESH,
        )

    def to_tp(d, src, dst, ssem, rsem):
        return pltpu.make_async_remote_copy(
            src_ref=src,
            dst_ref=dst,
            send_sem=ssem,
            recv_sem=rsem,
            device_id=(me, lax.rem(core + d, tp)),
            device_id_type=MESH,
        )

    def each(n, make, act):
        def step(d, carry):
            act(make(d))
            return carry

        lax.fori_loop(1, n, step, 0)

    start = lambda copy: copy.start()
    wait_send = lambda copy: copy.wait_send()
    wait_recv = lambda copy: copy.wait_recv()


    inner = inner_size(kv)
    outer = kv // inner
    z, p = me // inner, lax.rem(me, inner)

    def at(dz, dp):
        return lax.rem(z + dz + outer, outer) * inner + lax.rem(p + dp + inner, inner)

    def remote(src, dst, ssem, rsem, target):
        return pltpu.make_async_remote_copy(
            src_ref=src,
            dst_ref=dst,
            send_sem=ssem,
            recv_sem=rsem,
            device_id=(target, core),
            device_id_type=MESH,
        )

    def rs_inner(send, recv, ssem, rsem, dz, dp):
        i = dz * inner + dp
        return remote(send(at(dz, dp)), recv(i), ssem(i), rsem(i), at(0, dp))

    def rs_outer(send, recv, ssem, rsem, dz):
        i = dz * inner
        return remote(send(at(dz, 0)), recv(i), ssem(i), rsem(i), at(dz, 0))

    def rs_start(refs):
        for dz in list(range(1, outer)) + [0]:
            each(inner, lambda dp, dz=dz: rs_inner(*refs, dz, dp), start)

    def rs_group(refs, dz):
        send, recv = refs[:2]

        def add(dp, total):
            rs_inner(*refs, dz, dp).wait_recv()
            return total + recv(dz * inner + dp)[...].astype(F32)

        return lax.fori_loop(1, inner, add, send(at(dz, 0))[...].astype(F32))

    def rs_middle(refs):
        send = refs[0]
        for dz in range(1, outer):
            send(at(dz, 0))[...] = rs_group(refs, dz).astype(BF16)
            rs_outer(*refs, dz).start()

    def rs_end(refs):
        recv = refs[1]

        def add(dz, total):
            rs_outer(*refs, dz).wait_recv()
            return total + recv(dz * inner)[...].astype(F32)

        return lax.fori_loop(1, outer, add, rs_group(refs, 0))

    def rs_close(refs):
        for dz in range(outer):
            each(inner, lambda dp, dz=dz: rs_inner(*refs, dz, dp), wait_send)
        each(outer, lambda dz: rs_outer(*refs, dz), wait_send)

    def ag_outer(block, ssem, rsem, dz, slot):
        i = dz * inner
        return remote(block(slot), block(slot), ssem(i), rsem(i), at(dz, 0))

    def ag_inner(block, ssem, rsem, dz, dp, slot):
        i = dz * inner + dp
        return remote(block(slot), block(slot), ssem(i), rsem(i), at(0, dp))

    def ag_start(refs):
        each(outer, lambda dz: ag_outer(*refs, dz, me), start)
        each(inner, lambda dp: ag_inner(*refs, 0, dp, me), start)

    def ag_relay(refs):
        for dz in range(1, outer):
            ag_outer(*refs, dz, at(-dz, 0)).wait_recv()
            each(inner, lambda dp, dz=dz: ag_inner(*refs, dz, dp, at(-dz, 0)), start)

    def ag_end(refs):
        for dz in range(outer):
            each(inner, lambda dp, dz=dz: ag_inner(*refs, dz, dp, at(-dz, -dp)), wait_recv)

    def ag_close(refs):
        each(outer, lambda dz: ag_outer(*refs, dz, me), wait_send)
        for dz in range(outer):
            each(inner, lambda dp, dz=dz: ag_inner(*refs, dz, dp, at(-dz, 0)), wait_send)

    def views(c, *refs):
        return tuple(lambda i, ref=ref: ref.at[c, i] for ref in refs)

    def tok_out(d):
        return to_tp(d, tokens, tok_all.at[core], tok_ssem.at[d], tok_rsem.at[d])

    def tok_in(d):
        slot = lax.rem(core - d + tp, tp)
        return to_tp(d, tokens, tok_all.at[slot], tok_ssem.at[d], tok_rsem.at[d])

    each(tp, tok_out, start)
    tok_all[core] = tokens[...]

    each(tp, tok_in, wait_recv)
    widened = tok_all[...].astype(F32).reshape(total_rows, feats)
    square_in = jnp.sum(widened * widened, axis=1, keepdims=True)
    scaled_in = (widened * gain_mix[...]).astype(BF16)

    gates = jnp.dot(scaled_in, w_gates, preferred_element_type=F32)
    lane_r = lax.broadcasted_iota(jnp.int32, gates.shape, 1)
    gates = jnp.where(lane_r == 2 * H, square_in, gates)
    for j in range(kv):
        gate_send[j] = gates[j * S : (j + 1) * S]

    def gate_out(d):
        return to_kv(
            d, gate_send.at[lax.rem(me + d, kv)], gate_recv.at[d], gate_ssem.at[d], gate_rsem.at[d]
        )

    each(kv, gate_out, start)

    proj_refs = [views(i, proj_send, proj_recv, proj_ssem, proj_rsem) for i in range(1)]
    for i, w in enumerate((wq_v, wk_v, wv_v)):
        loads[i].wait()
        part = jnp.dot(scaled_in, w[...], preferred_element_type=F32)
        for j in range(kv):
            proj_send[0, j, :, i * width : (i + 1) * width] = part[j * S : (j + 1) * S].astype(BF16)
    rs_start(proj_refs[0])

    for refs in proj_refs:
        rs_middle(refs)
    loads[3].wait()

    def split(i, carry):
        s, h = i // H, lax.rem(i, H)
        full = state_v[s, h]
        hi = full.astype(BF16)
        state_hi[s, h] = hi
        state_lo[s, h] = (full - hi.astype(F32)).astype(BF16)
        return carry

    lax.fori_loop(0, S * H, split, 0)
    loads[4].wait()
    loads[5].wait()

    def gate_add(d, total):
        gate_out(d).wait_recv()
        return total + gate_recv[d]

    gate_sum = lax.fori_loop(1, kv, gate_add, gate_send[me])
    factor_in = lax.rsqrt(gate_sum[:, 2 * H : 2 * H + 1] / D + EPS)
    gate_sum = gate_sum * factor_in

    projected = (rs_end(proj_refs[0]) * factor_in).astype(BF16)
    query, key_new, value_new = (projected[:, i * width : (i + 1) * width] for i in range(3))

    scale = HD ** (-0.5)
    contract = (((1,), (1,)), ((), ()))
    mixed = []
    for h in range(H):
        cols = slice(h * HD, (h + 1) * HD)
        q, k, v = query[:, cols], key_new[:, cols], value_new[:, cols]
        past, past_top, carried = base[h]
        ig = gate_sum[:, h : h + 1] + bias_igate[h]
        raw = gate_sum[:, H + h : H + h + 1] + bias_fgate[h]
        fg = jnp.minimum(raw, 0.0) - jnp.log1p(jnp.exp(-jnp.abs(raw)))
        carried = carried + fg
        top = jnp.maximum(jnp.maximum(carried, ig), past_top + fg)
        decay = jnp.exp(past + (fg - top))
        scores = jnp.zeros((S, B), F32)
        state_term = jnp.zeros((S, HD), F32)
        for s in range(S):
            mine = row == s
            got = lax.dot_general(q, keys_v[s, h], contract, preferred_element_type=F32)
            scores = jnp.where(mine, got, scores)
            mem = lax.dot_general(
                q, state_hi[s, h], contract, preferred_element_type=F32
            ) + lax.dot_general(q, state_lo[s, h], contract, preferred_element_type=F32)
            state_term = jnp.where(mine, mem, state_term)
        weights = (decay * (scores * scale)).astype(BF16)
        block_term = jnp.zeros((S, HD), F32)
        for s in range(S):
            got = jnp.dot(weights, values_v[s, h], preferred_element_type=F32)
            block_term = jnp.where(row == s, got, block_term)
        own = jnp.sum(q.astype(F32) * k.astype(F32), axis=1, keepdims=True) * scale
        numerator = (
            state_term * jnp.exp(carried - top)
            + block_term
            + (jnp.exp(ig - top) * own) * v.astype(F32)
        )
        spread = jnp.mean(numerator * numerator, axis=1, keepdims=True)
        mixed_all[me, :, cols] = (numerator * lax.rsqrt(spread + EPS) * gain_head[...]).astype(BF16)

    def mix_out(d):
        return to_kv(d, mixed_all.at[me], mixed_all.at[me], mix_ssem.at[d], mix_rsem.at[d])

    def mix_in(d):
        slot = lax.rem(me - d + kv, kv)
        return to_kv(d, mixed_all.at[me], mixed_all.at[slot], mix_ssem.at[d], mix_rsem.at[d])

    each(kv, mix_out, start)
    for i in (6, 7, 8):
        loads[i].wait()
    each(kv, mix_in, wait_recv)
    for j in range(kv):
        mixed_rows[j * S : (j + 1) * S] = mixed_all[j].astype(F32)
    att_all[core] = jnp.dot(
        mixed_rows[...].astype(BF16), wo_v[...], preferred_element_type=F32
    ).astype(BF16)

    def att_out(d):
        return to_tp(d, att_all.at[core], att_all.at[core], att_ssem.at[d], att_rsem.at[d])

    def att_in(d):
        slot = lax.rem(core - d + tp, tp)
        return to_tp(d, att_all.at[core], att_all.at[slot], att_ssem.at[d], att_rsem.at[d])

    each(tp, att_out, start)
    each(tp, att_in, wait_recv)
    attended = att_all[0].astype(F32)
    for t in range(1, tp):
        attended = attended + att_all[t].astype(F32)
    restored = (widened + attended).astype(BF16).astype(F32)
    res_rows[...] = restored.reshape(tp, rows, feats)
    square_mid = jnp.sum(restored * restored, axis=1, keepdims=True)
    square_wide = jnp.broadcast_to(square_mid, (total_rows, 128))
    for j in range(kv):
        sq_send[j] = square_wide[j * S : (j + 1) * S]

    def sq_out(d):
        return to_kv(
            d, sq_send.at[lax.rem(me + d, kv)], sq_recv.at[d], sq_ssem.at[d], sq_rsem.at[d]
        )

    each(kv, sq_out, start)
    scaled_mid = (restored * gain_mlp[...]).astype(BF16)

    up_refs = [views(c, up_send, up_recv, up_ssem, up_rsem) for c in range(chunks)]
    hid_refs = [views(c, hid_all, hid_ssem, hid_rsem) for c in range(chunks)]

    for c in range(chunks):
        part = jnp.dot(
            scaled_mid, wu_v[:, c * chunk : (c + 1) * chunk], preferred_element_type=F32
        )
        for j in range(kv):
            up_send[c, j] = part[j * S : (j + 1) * S].astype(BF16)
        rs_start(up_refs[c])

    def sq_add(d, total):
        sq_out(d).wait_recv()
        return total + sq_recv[d]

    square_sum = lax.fori_loop(1, kv, sq_add, sq_send[me])
    factor_mid = lax.rsqrt(square_sum[:, 0:1] / D + EPS)

    for refs in up_refs:
        rs_middle(refs)
    for c in range(chunks):
        active = jnp.maximum(rs_end(up_refs[c]) * factor_mid, 0.0)
        hid_all[c, me] = (active * active).astype(BF16)
        ag_start(hid_refs[c])
        if c > 0:
            ag_relay(hid_refs[c - 1])
    ag_relay(hid_refs[-1])

    down = jnp.zeros((total_rows, feats), F32)
    for c in range(chunks):
        ag_end(hid_refs[c])
        for j in range(kv):
            hid_rows[j * S : (j + 1) * S] = hid_all[c, j].astype(F32)
        down = down + jnp.dot(
            hid_rows[...].astype(BF16),
            wd_v[c * chunk : (c + 1) * chunk],
            preferred_element_type=F32,
        )
    down_send[...] = down.astype(BF16).reshape(tp, rows, feats)

    def down_out(d):
        return to_tp(
            d, down_send.at[lax.rem(core + d, tp)], down_recv.at[d], down_ssem.at[d], down_rsem.at[d]
        )

    each(tp, down_out, start)

    each(tp, tok_out, wait_send)
    each(kv, gate_out, wait_send)
    for refs in proj_refs + up_refs:
        rs_close(refs)
    for refs in hid_refs:
        ag_close(refs)
    each(kv, mix_out, wait_send)
    each(tp, att_out, wait_send)
    each(kv, sq_out, wait_send)

    def down_add(d, total):
        down_out(d).wait_recv()
        return total + down_recv[d].astype(F32)

    total = lax.fori_loop(1, tp, down_add, down_send[core].astype(F32))
    out[...] = (res_rows[core] + total).astype(out.dtype)
    each(tp, down_out, wait_send)


def any_body(kv, tp, *args):
    (
        tokens,
        gain_mix,
        w_query,
        w_key,
        w_value,
        w_igate,
        w_fgate,
        bias_igate,
        bias_fgate,
        state_mem,
        state_max,
        keys_blk,
        values_blk,
        igate_blk,
        fgate_blk,
        lengths,
        gain_head,
        w_mixout,
        gain_mlp,
        w_up,
        w_down,
    ) = args
    rows, feats = tokens.shape
    S, H, HD, _ = state_mem.shape
    width = H * HD
    hidden = w_up.shape[1]
    chunks = ceil_chunks(hidden)
    chunk = hidden // chunks
    vm = pl.BlockSpec(memory_space=pltpu.VMEM)
    sm = pl.BlockSpec(memory_space=pltpu.SMEM)
    hbm = pl.BlockSpec(memory_space=pl.ANY)
    in_specs = [
        vm,
        vm,
        hbm,
        hbm,
        hbm,
        vm,
        vm,
        sm,
        sm,
        hbm,
        vm,
        hbm,
        hbm,
        vm,
        vm,
        sm,
        vm,
        hbm,
        vm,
        hbm,
        hbm,
    ]
    V = pltpu.VMEM
    dma = pltpu.SemaphoreType.DMA
    scratch = [
        V(w_query.shape, BF16),
        V(w_key.shape, BF16),
        V(w_value.shape, BF16),
        V(state_mem.shape, F32),
        V(state_mem.shape, BF16),
        V(state_mem.shape, BF16),
        V(keys_blk.shape, BF16),
        V(values_blk.shape, BF16),
        V(w_mixout.shape, BF16),
        V(w_up.shape, BF16),
        V(w_down.shape, BF16),
        V((tp, rows, feats), BF16),
        V((1, kv, S, 3 * width), BF16),
        V((1, kv, S, 3 * width), BF16),
        V((kv, S, 128), F32),
        V((kv, S, 128), F32),
        V((kv, S, width), BF16),
        V((kv * S, width), F32),
        V((tp, kv * S, feats), BF16),
        V((tp, rows, feats), F32),
        V((kv, S, 128), F32),
        V((kv, S, 128), F32),
        V((chunks, kv, S, chunk), BF16),
        V((chunks, kv, S, chunk), BF16),
        V((chunks, kv, S, chunk), BF16),
        V((kv * S, chunk), F32),
        V((tp, rows, feats), BF16),
        V((tp, rows, feats), BF16),
        dma((9,)),
        dma((tp,)),
        dma((tp,)),
        dma((1, kv)),
        dma((1, kv)),
        dma((kv,)),
        dma((kv,)),
        dma((kv,)),
        dma((kv,)),
        dma((tp,)),
        dma((tp,)),
        dma((kv,)),
        dma((kv,)),
        dma((chunks, kv)),
        dma((chunks, kv)),
        dma((chunks, kv)),
        dma((chunks, kv)),
        dma((tp,)),
        dma((tp,)),
    ]
    return pl.pallas_call(
        functools.partial(any_kernel, (kv, tp, kv * feats)),
        out_shape=jax.ShapeDtypeStruct((rows, feats), BF16),
        in_specs=in_specs,
        out_specs=vm,
        scratch_shapes=scratch,
        compiler_params=pltpu.CompilerParams(
            collective_id=0, has_side_effects=True, vmem_limit_bytes=56 * 1024 * 1024
        ),
    )(
        tokens,
        gain_mix.reshape(1, -1),
        w_query,
        w_key,
        w_value,
        w_igate,
        w_fgate,
        bias_igate,
        bias_fgate,
        state_mem,
        state_max,
        keys_blk,
        values_blk,
        igate_blk,
        fgate_blk,
        lengths,
        gain_head.reshape(1, -1),
        w_mixout,
        gain_mlp.reshape(1, -1),
        w_up,
        w_down,
    )


def flip(index, mask):
    bit = 1
    while bit <= mask:
        if mask & bit:
            index = index + bit * (1 - 2 * lax.rem(lax.div(index, bit), 2))
        bit *= 2
    return index


def stages(kv):
    inner = inner_size(kv)
    outer = kv // inner
    if (inner, outer) != (4, 4):
        return (([m for m in range(inner)], [m * inner for m in range(outer)]),)
    ways = (((1, 2), (4, 8)), ((1, 4), (2, 8)), ((2, 4), (1, 8)))
    return tuple(tuple([0, a, b, a + b] for a, b in way) for way in ways)


def kernel(cfg, names, *refs):
    kv, tp, D = cfg
    r = SimpleNamespace(**dict(zip(names, refs, strict=True)))
    me, core = lax.axis_index("kv"), lax.axis_index("tp")
    inner = inner_size(kv)
    outer = kv // inner
    other = 1 - core
    ways = stages(kv)

    def split(way):
        def place(masks):
            total, step = 0, 1
            while step < len(masks):
                total = total + step * lax.rem(lax.div(me, masks[step]), 2)
                step *= 2
            return total

        return place(way[1]), place(way[0])
    S, H, HD, _ = r.state_mem.shape
    B = r.fgate_blk.shape[2]
    width = H * HD
    R, F = r.tokens.shape
    per = kv // tp
    half = lax.div(me, per)
    jj_me = lax.rem(me, per)
    chunks, _, _, CW = r.up_send.shape
    proj_way = [ways[a % len(ways)] for a in range(4)]
    up_way = [ways[c % len(ways)] for c in range(chunks)]

    cube = kv // 2
    barrier = pltpu.get_barrier_semaphore()

    def greet(target, c):
        pl.semaphore_signal(barrier, inc=1, device_id=(target, c), device_id_type=MESH)

    for m in reversed(range(1, cube)):
        greet(flip(me, m), 1)
    greet(me, other)

    @pl.when(core == 1)
    def _():
        greet(flip(me, cube), 1)


    taken = iter(range(r.local_sem.shape[0]))

    def load(whole, *pieces):
        sem = r.local_sem.at[next(taken)]
        for i, piece in enumerate(pieces):
            dst = whole if len(pieces) == 1 else whole.at[i]
            pltpu.make_async_copy(piece, dst, sem).start()
        return pltpu.make_async_copy(whole, whole, sem)

    got_tokens = load(r.v_tokens, r.tokens)
    got_gain_mix = load(r.v_gain_mix, r.gain_mix)
    got_w_gate = load(r.v_w_gate, r.w_igate, r.w_fgate)
    got_w_qkv = load(r.v_w_qkv, r.w_query, r.w_key, r.w_value)
    got_blk = [
        load(r.v_gate_blk, r.fgate_blk, r.igate_blk),
        load(r.v_lengths, r.lengths),
        load(r.v_state_max, r.state_max),
        load(r.v_bias, r.bias_igate, r.bias_fgate),
    ]
    got_memory = [
        load(r.v_state_mem, r.state_mem),
        load(r.v_kv_blk, r.keys_blk, r.values_blk),
        load(r.v_gain_head, r.gain_head),
    ]
    got_gain_mlp = load(r.v_gain_mlp, r.gain_mlp)
    got_w_mixout = load(r.v_w_mixout.at[0], r.w_mixout)
    got_w_up = load(r.v_w_up.at[0], r.w_up)
    got_w_down = load(r.v_w_down.at[0], r.w_down)

    def loaded(copies):
        for copy in copies:
            copy.wait()

    def remote(src, dst, ssem, rsem, target, c):
        return pltpu.make_async_remote_copy(
            src_ref=src,
            dst_ref=dst,
            send_sem=ssem,
            recv_sem=rsem,
            device_id=(target, c),
            device_id_type=MESH,
        )

    def drain(ref, sem):
        remote(ref, ref, sem, sem, me, other).wait_send()

    tok_copy = remote(
        r.v_tokens, r.tok_peer, r.pair_ssem.at[0], r.pair_rsem.at[0], me, other
    )
    got_tokens.wait()

    @pl.when(core == 0)
    def _():
        pl.semaphore_wait(barrier, 1)
        tok_copy.start()

    loaded([got_gain_mix, got_w_gate])
    lane = lax.broadcasted_iota(jnp.int32, (H, 128), 1)
    sub = lax.broadcasted_iota(jnp.int32, (H, 128), 0)
    pick_i = (lane == sub).astype(F32).astype(BF16)
    pick_f = (lane == sub + H).astype(F32).astype(BF16)
    first = (((0,), (0,)), ((), ()))
    w_gates = (
        lax.dot_general(r.v_w_gate[0], pick_i, first, preferred_element_type=F32)
        + lax.dot_general(r.v_w_gate[1], pick_f, first, preferred_element_type=F32)
    ).astype(BF16)
    lane_r = lax.broadcasted_iota(jnp.int32, (R, 128), 1)
    gain_mix = r.v_gain_mix[...]
    gate_send = r.gate_send
    proj_send = r.proj_send
    send_of = [*(proj_send.at[a] for a in range(3)), gate_send]
    recv_of = [*(r.proj_recv.at[a] for a in range(3)), r.gate_recv]
    mid_of = [*(r.proj_mid.at[a] for a in range(3)), r.gate_mid]
    last_of = [*(r.proj_last.at[a] for a in range(3)), r.gate_last]

    def project(rows, group):
        scaled = (rows * gain_mix).astype(BF16)
        square = jnp.sum(rows * rows, axis=1, keepdims=True)
        gates = jnp.dot(scaled, w_gates, preferred_element_type=F32)
        gates = jnp.where(lane_r == 2 * H, square, gates)
        for jj in range(per):
            gate_send[group * per + jj] = gates[jj * S : (jj + 1) * S]
        for i in range(3):
            part = jnp.dot(scaled, r.v_w_qkv[i], preferred_element_type=F32)
            for jj in range(per):
                proj_send[i, group * per + jj] = part[jj * S : (jj + 1) * S].astype(BF16)

    own_rows = r.v_tokens[...].astype(F32)
    got_w_qkv.wait()
    project(own_rows, core)

    loaded(got_blk)
    row = lax.broadcasted_iota(jnp.int32, (S, 1), 0)
    eye_s = lax.broadcasted_iota(jnp.int32, (S, S), 0) == lax.broadcasted_iota(jnp.int32, (S, S), 1)
    length = jnp.sum(
        jnp.where(eye_s, r.v_lengths[...].astype(F32), 0.0), axis=1, keepdims=True
    )
    live = lax.broadcasted_iota(jnp.int32, (S, B), 1).astype(F32) < length
    later = (
        lax.broadcasted_iota(jnp.int32, (B, B), 0) > lax.broadcasted_iota(jnp.int32, (B, B), 1)
    ).astype(F32)
    base = []
    for h in range(H):
        forget = jnp.where(live, r.v_gate_blk[0, :, h, :], 0.0)
        suffix = jnp.dot(
            forget, later, preferred_element_type=F32, precision=lax.Precision.HIGHEST
        )
        past = jnp.where(live, r.v_gate_blk[1, :, h, :] + suffix, -jnp.inf)
        carried = r.v_state_max[:, h : h + 1] + jnp.sum(forget, axis=1, keepdims=True)
        base.append((past, jnp.max(past, axis=1, keepdims=True), carried))
    tok_copy.wait_recv()

    @pl.when(core == 1)
    def _():
        tok_copy.start()

    project(r.tok_peer[...].astype(F32), other)

    @pl.when(core == 1)
    def _():
        pl.semaphore_wait(barrier, 2 * cube)
        pl.semaphore_signal(r.go_sem, inc=1, device_id=(me, other), device_id_type=MESH)
        pl.semaphore_signal(
            r.half_sem, inc=1, device_id=(flip(me, cube), core), device_id_type=MESH
        )

    @pl.when(core == 0)
    def _():
        pl.semaphore_wait(r.go_sem, 1)


    def pair(i, ref):
        return remote(ref.at[0], ref.at[1], r.pair_ssem.at[i], r.pair_rsem.at[i], me, other)

    pairs = [pair(1, r.v_w_mixout), pair(2, r.v_w_up), pair(3, r.v_w_down)]

    def proj_one(a, mz, mp):
        first, second = proj_way[a]
        return remote(
            send_of[a].at[flip(me, first[mp] + second[mz])],
            recv_of[a].at[mz, mp],
            r.proj_ssem.at[a],
            r.proj_rsem.at[a, mz // (outer // 2)],
            flip(me, first[mp]),
            other,
        )

    def proj_two(a, mz):
        return remote(
            mid_of[a].at[mz],
            last_of[a].at[mz],
            r.mid_ssem.at[a],
            r.mid_rsem.at[a],
            flip(me, proj_way[a][1][mz]),
            other,
        )

    far = [mz for mz in reversed(range(outer)) if mz >= outer // 2]
    near = [mz for mz in reversed(range(outer)) if mz < outer // 2]
    peers = list(reversed(range(inner)))

    def send_groups(a, groups):
        for mz in groups:
            for mp in peers:
                proj_one(a, mz, mp).start()

    for a in (3, 0, 1, 2):
        send_groups(a, far)
        send_groups(a, near)

    got_w_mixout.wait()
    pairs[0].start()

    loaded(got_memory)

    def narrow(i, carry):
        s, h = lax.div(i, H), lax.rem(i, H)
        r.state_t[s, h] = r.v_state_mem[s, h].T.astype(BF16)
        r.keys_t[s, h] = r.v_kv_blk[0, s, h].T
        return carry

    lax.fori_loop(0, S * H, narrow, 0)

    def summed(ref):
        total = ref[0].astype(F32)
        for i in range(1, ref.shape[0]):
            total = total + ref[i].astype(F32)
        return total

    def proj_middle(a):
        for side, groups in ((1, far), (0, near)):
            drain(
                recv_of[a].at[pl.ds(side * (outer // 2), outer // 2)], r.proj_rsem.at[a, side]
            )
            for mz in groups:
                mid_of[a][mz] = summed(recv_of[a].at[mz]).astype(mid_of[a].dtype)
                proj_two(a, mz).start()

    def proj_end(a):
        drain(last_of[a], r.mid_rsem.at[a])
        return summed(last_of[a])

    @pl.when(core == 1)
    def _():
        pl.semaphore_wait(r.half_sem, 1)
        pl.semaphore_signal(r.half_sem, inc=1, device_id=(me, other), device_id_type=MESH)

    @pl.when(core == 0)
    def _():
        pl.semaphore_wait(r.half_sem, 1)

    for a in (3, 0, 1, 2):
        proj_middle(a)
    got_w_up.wait()
    pairs[1].start()
    gate_sum = proj_end(3)
    factor_in = lax.rsqrt(gate_sum[:, 2 * H : 2 * H + 1] / D + EPS)
    gate_sum = gate_sum * factor_in
    scale = HD ** (-0.5)
    shares = []
    for h in range(H):
        past, past_top, carried = base[h]
        ig = gate_sum[:, h : h + 1] + r.v_bias[0, :, h : h + 1]
        raw = gate_sum[:, H + h : H + h + 1] + r.v_bias[1, :, h : h + 1]
        fg = jnp.minimum(raw, 0.0) - jnp.log1p(jnp.exp(-jnp.abs(raw)))
        carried = carried + fg
        top = jnp.maximum(jnp.maximum(carried, ig), past_top + fg)
        shares.append((jnp.exp(past + (fg - top)) * scale, jnp.exp(carried - top), jnp.exp(ig - top)))
    query = (proj_end(0) * factor_in).astype(BF16)

    cells = []
    for h in range(H):
        q = query[:, h * HD : (h + 1) * HD]
        decay, remaining, entering = shares[h]
        scores = jnp.zeros((S, B), F32)
        state_term = jnp.zeros((S, HD), F32)
        for s in range(S):
            mine = row == s
            got = jnp.dot(q, r.keys_t[s, h], preferred_element_type=F32)
            scores = jnp.where(mine, got, scores)
            mem = jnp.dot(q, r.state_t[s, h], preferred_element_type=F32)
            state_term = jnp.where(mine, mem, state_term)
        weights = (decay * scores).astype(BF16)
        block_term = jnp.zeros((S, HD), F32)
        for s in range(S):
            got = jnp.dot(weights, r.v_kv_blk[1, s, h], preferred_element_type=F32)
            block_term = jnp.where(row == s, got, block_term)
        cells.append((state_term * remaining + block_term, entering))

    key_new = (proj_end(1) * factor_in).astype(BF16)
    value_new = (proj_end(2) * factor_in).astype(BF16)
    for h in range(H):
        cols = slice(h * HD, (h + 1) * HD)
        q, k, v = query[:, cols], key_new[:, cols], value_new[:, cols]
        older, entering = cells[h]
        own = jnp.sum(q.astype(F32) * k.astype(F32), axis=1, keepdims=True) * scale
        numerator = older + (entering * own) * v.astype(F32)
        spread = jnp.mean(numerator * numerator, axis=1, keepdims=True)
        r.mixed_own[:, cols] = (
            numerator * lax.rsqrt(spread + EPS) * r.v_gain_head[...]
        ).astype(BF16)

    mixed_all = r.mixed_all
    slot = lax.rem(half + core, 2)
    mine_at = slot * per + jj_me

    def mix_copy(m):
        return remote(
            r.mixed_own,
            mixed_all.at[mine_at],
            r.mix_ssem,
            r.mix_rsem,
            flip(me, m),
            half,
        )

    for m in reversed(range(1, kv)):
        mix_copy(m).start()

    @pl.when(slot == 1)
    def _():
        mix_copy(0).start()

    @pl.when(slot == 0)
    def _():
        mixed_all[mine_at] = r.mixed_own[...]

    loaded([got_w_down, got_gain_mlp])
    pairs[0].wait()

    @pl.when(half == core)
    def _():
        drain(mixed_all.at[pl.ds(0, kv - 1)], r.mix_rsem)

    @pl.when(half != core)
    def _():
        drain(mixed_all, r.mix_rsem)

    mixed_rows = r.mixed_rows
    attended = jnp.zeros((R, F), F32)
    for c in range(tp):
        for jj in range(per):
            mixed_rows[jj * S : (jj + 1) * S, c * width : (c + 1) * width] = mixed_all[
                c * per + jj
            ].astype(F32)
        attended = attended + jnp.dot(
            mixed_rows[:, c * width : (c + 1) * width].astype(BF16),
            r.v_w_mixout[c],
            preferred_element_type=F32,
        ).astype(BF16).astype(F32)

    restored = (own_rows + attended).astype(BF16).astype(F32)
    r.res_rows[...] = restored
    scaled_mid = (restored * r.v_gain_mlp[...]).astype(BF16)

    up_send, up_recv, up_mid, up_last = r.up_send, r.up_recv, r.up_mid, r.up_last

    def up_one(c, mz, mp):
        place = split(up_way[c])
        return remote(
            up_send.at[c, flip(place[0], mz) * inner + flip(place[1], mp)],
            up_recv.at[c, mz, mp],
            r.up_ssem,
            r.up_rsem.at[c, mz // (outer // 2)],
            flip(me, up_way[c][0][mp]),
            other,
        )

    def up_two(c, mz):
        return remote(
            up_mid.at[c, mz],
            up_last.at[c, mz],
            r.mid_ssem.at[4],
            r.up_lsem.at[c],
            flip(me, up_way[c][1][mz]),
            other,
        )

    parts = chunks // tp
    span = kv * CW

    def up_start(c, groups):
        for mz in groups:
            for mp in peers:
                up_one(c, mz, mp).start()

    def up_compute(c):
        if c == parts:
            pairs[1].wait()
        begin = (c % parts) * span
        part = jnp.dot(
            scaled_mid,
            r.v_w_up[c // parts, :, begin : begin + span],
            preferred_element_type=F32,
        ).astype(BF16)
        for j in range(kv):
            up_send[c, j] = part[:, j * CW : (j + 1) * CW]

    plan = [(c, side) for c in range(chunks) for side in (1, 0)]
    for i, (c, side) in enumerate(plan):
        if c not in [x for x, _ in plan[:i]]:
            up_compute(c)
        up_start(c, far if side else near)
    pairs[2].start()

    square_mid = jnp.sum(restored * restored, axis=1, keepdims=True)
    eye_r = lax.broadcasted_iota(jnp.int32, (R, 128), 0) == lane_r
    r.sq_all[0] = jnp.sum(jnp.where(eye_r, square_mid, 0.0), axis=0, keepdims=True)

    def sq_copy(m):
        return remote(
            r.sq_all.at[0],
            r.sq_all.at[m],
            r.sq_ssem,
            r.sq_rsem,
            flip(me, m),
            core,
        )

    for m in reversed(range(1, kv)):
        sq_copy(m).start()

    def up_middle(c, side):
        drain(up_recv.at[c, pl.ds(side * (outer // 2), outer // 2)], r.up_rsem.at[c, side])
        for mz in far if side else near:
            up_mid[c, mz] = summed(up_recv.at[c, mz]).astype(BF16)
            up_two(c, mz).start()

    hid_mid, hid_all = r.hid_mid, r.hid_all

    def hid_near(c, mp):
        mine = hid_all.at[c, 0, split(up_way[c])[1]]
        return remote(
            mine,
            mine,
            r.hid_ssem.at[2],
            r.hid_rsem.at[c],
            flip(me, up_way[c][0][mp]),
            core,
        )

    def hid_one(c, mz):
        return remote(
            hid_all.at[c, 0, split(up_way[c])[1]],
            hid_mid.at[c, mz],
            r.hid_ssem.at[0],
            r.hid_msem.at[c, mz - 1],
            flip(me, up_way[c][1][mz]),
            other,
        )

    def hid_two(c, mz, mp):
        return remote(
            hid_mid.at[c, mz],
            hid_all.at[c, mz, split(up_way[c])[1]],
            r.hid_ssem.at[1],
            r.hid_rsem.at[c],
            flip(me, up_way[c][0][mp]),
            other,
        )

    def hid_start(c):
        drain(up_last.at[c], r.up_lsem.at[c])
        active = jnp.maximum(summed(up_last.at[c]), 0.0)
        hid_all[c, 0, split(up_way[c])[1]] = (active * active).astype(BF16)
        for mz in reversed(range(1, outer)):
            hid_one(c, mz).start()
        for mp in peers[:-1]:
            hid_near(c, mp).start()

    def hid_relay(c, mz):
        drain(hid_mid.at[c, mz], r.hid_msem.at[c, mz - 1])
        for mp in peers:
            hid_two(c, mz, mp).start()

    def hops(mz):
        return 1.8 + 0.7 * ((mz & 1) + 2 * (mz >> 1)) if mz else 0.9

    steps, ready = [], [0.0] * chunks
    for i, (c, side) in enumerate(plan):
        due = 3.2 * (i + 1) / len(plan) + 2.8
        steps.append((due, up_middle, c, side))
        ready[c] = max([ready[c], *(due + hops(mz) for mz in (far if side else near))])
    for c in range(chunks):
        steps.append((ready[c] + 0.2, hid_start, c))
        for mz in range(1, outer):
            steps.append((ready[c] + 0.4 + hops(mz), hid_relay, c, mz))
    order = [step[1:] for step in sorted(steps, key=lambda step: step[0])]
    for step, *which in order:
        step(*which)

    tok_copy.wait_send()
    for a in range(4):
        drain(recv_of[a], r.proj_ssem.at[a])
        drain(last_of[a], r.mid_ssem.at[a])

    @pl.when(slot == 0)
    def _():
        drain(mixed_all.at[pl.ds(0, kv - 1)], r.mix_ssem)

    @pl.when(slot == 1)
    def _():
        drain(mixed_all, r.mix_ssem)

    drain(r.sq_all.at[pl.ds(1, kv - 1)], r.sq_ssem)
    drain(up_recv, r.up_ssem)
    drain(up_last, r.mid_ssem.at[4])
    pairs[2].wait()
    drain(r.sq_all.at[pl.ds(1, kv - 1)], r.sq_rsem)
    squares = r.sq_all[0]
    for m in range(1, kv):
        squares = squares + r.sq_all[m]
    square_sum = jnp.sum(jnp.where(eye_r, squares, 0.0), axis=1, keepdims=True)
    factor_mid = lax.rsqrt(square_sum / D + EPS)
    drain(hid_mid.at[:, pl.ds(1, outer - 1)], r.hid_ssem.at[0])
    drain(hid_all.at[:, 0, pl.ds(1, inner - 1)], r.hid_ssem.at[2])

    flat = r.up_send.at[0]
    down = jnp.zeros((R, F), F32)
    for c in range(chunks):
        drain(flat.at[pl.ds(0, kv - 1)], r.hid_rsem.at[c])
        for mz in range(outer):
            group = flip(split(up_way[c])[0], mz)
            begin = pl.multiple_of((c % parts) * span + group * (inner * CW), inner * CW)
            down = down + jnp.dot(
                jnp.concatenate([hid_all[c, mz, pt] for pt in range(inner)], axis=1),
                r.v_w_down[c // parts, pl.ds(begin, inner * CW), :],
                preferred_element_type=F32,
            )
    r.out[...] = (r.res_rows[...] + down * (factor_mid * factor_mid)).astype(BF16)
    drain(hid_all.at[:, pl.ds(1, outer - 1)], r.hid_ssem.at[1])


def named(
    tokens,
    gain_mix,
    w_query,
    w_key,
    w_value,
    w_igate,
    w_fgate,
    bias_igate,
    bias_fgate,
    state_mem,
    state_max,
    keys_blk,
    values_blk,
    igate_blk,
    fgate_blk,
    lengths,
    gain_head,
    w_mixout,
    gain_mlp,
    w_up,
    w_down,
):
    return SimpleNamespace(**locals())


def body(kv, tp, *args):
    a = named(*args)
    a.gain_mix, a.gain_head, a.gain_mlp, a.bias_igate, a.bias_fgate, a.lengths = (
        x.reshape(1, -1)
        for x in (a.gain_mix, a.gain_head, a.gain_mlp, a.bias_igate, a.bias_fgate, a.lengths)
    )
    a.w_igate, a.w_fgate = a.w_igate.T, a.w_fgate.T
    rows, feats = a.tokens.shape
    S, H, HD, _ = a.state_mem.shape
    B = a.keys_blk.shape[2]
    width = H * HD
    inner = inner_size(kv)
    outer = kv // inner
    per = kv // tp
    hidden = a.w_up.shape[1]
    chunks = tp * max(n for n in (1, 2) if hidden % (n * kv * 128) == 0)
    cw = hidden * tp // (chunks * kv)
    V = pltpu.VMEM
    dma = pltpu.SemaphoreType.DMA

    def room(x, *many):
        return V((*many, *x.shape), x.dtype)

    scratch = dict(
        v_tokens=room(a.tokens),
        v_gain_mix=room(a.gain_mix),
        v_lengths=room(a.lengths),
        v_state_max=room(a.state_max),
        v_gain_head=room(a.gain_head),
        v_gain_mlp=room(a.gain_mlp),
        v_state_mem=room(a.state_mem),
        v_w_gate=room(a.w_igate, 2),
        v_w_qkv=room(a.w_query, 3),
        v_gate_blk=room(a.fgate_blk, 2),
        v_bias=room(a.bias_igate, 2),
        v_kv_blk=room(a.keys_blk, 2),
        v_w_mixout=room(a.w_mixout, tp),
        v_w_up=room(a.w_up, tp),
        v_w_down=room(a.w_down, tp),
        state_t=V(a.state_mem.shape, BF16),
        keys_t=V((S, H, HD, B), BF16),
        tok_peer=room(a.tokens),
        proj_send=V((3, kv, S, width), BF16),
        proj_recv=V((3, outer, inner, S, width), BF16),
        proj_mid=V((3, outer, S, width), BF16),
        proj_last=V((3, outer, S, width), BF16),
        gate_send=V((kv, S, 128), F32),
        gate_recv=V((outer, inner, S, 128), F32),
        gate_mid=V((outer, S, 128), F32),
        gate_last=V((outer, S, 128), F32),
        mixed_own=V((S, width), BF16),
        mixed_all=V((tp * per, S, width), BF16),
        mixed_rows=V((rows, tp * width), F32),
        res_rows=V((rows, feats), F32),
        sq_all=V((kv, 1, 128), F32),
        up_send=V((chunks, kv, rows, cw), BF16),
        up_recv=V((chunks, outer, inner, rows, cw), BF16),
        up_mid=V((chunks, outer, rows, cw), BF16),
        up_last=V((chunks, outer, rows, cw), BF16),
        hid_mid=V((chunks, outer, rows, cw), BF16),
        hid_all=V((chunks, outer, inner, rows, cw), BF16),
        local_sem=dma((15,)),
        pair_ssem=dma((4,)),
        pair_rsem=dma((4,)),
        proj_ssem=dma((4,)),
        proj_rsem=dma((4, 2)),
        mid_ssem=dma((5,)),
        mid_rsem=dma((4,)),
        mix_ssem=dma,
        mix_rsem=dma,
        sq_ssem=dma,
        sq_rsem=dma,
        up_ssem=dma,
        up_rsem=dma((chunks, 2)),
        up_lsem=dma((chunks,)),
        hid_ssem=dma((3,)),
        hid_msem=dma((chunks, outer - 1)),
        hid_rsem=dma((chunks,)),
        go_sem=pltpu.SemaphoreType.REGULAR,
        half_sem=pltpu.SemaphoreType.REGULAR,
    )
    operands = vars(a)
    names = (*operands, "out", *scratch)
    return pl.pallas_call(
        functools.partial(kernel, (kv, tp, kv * feats), names),
        out_shape=V((rows, feats), BF16),
        in_specs=[pl.BlockSpec(memory_space=pl.ANY)] * len(operands),
        out_specs=pl.BlockSpec(memory_space=V),
        scratch_shapes=list(scratch.values()),
        compiler_params=pltpu.CompilerParams(
            collective_id=0, has_side_effects=True, vmem_limit_bytes=56 * 1024 * 1024
        ),
    )(*operands.values())


def suits(kv, tp, *args):
    a = named(*args)
    inner = inner_size(kv)
    outer = kv // inner
    return (
        tp == 2
        and kv & (kv - 1) == 0
        and outer > 1
        and inner > 1
        and a.tokens.shape[1] % 128 == 0
        and a.tokens.shape[0] <= 128
        and a.w_up.shape[1] % (kv * 128) == 0
    )


def either(kv, tp, *args):
    return (body if suits(kv, tp, *args) else any_body)(kv, tp, *args)


def solution(mesh):
    in_specs = (
        P("tp", "kv"),
        P("kv"),
        P("kv", "tp"),
        P("kv", "tp"),
        P("kv", "tp"),
        P("kv", "tp"),
        P("kv", "tp"),
        P("tp"),
        P("tp"),
        P("kv", "tp", None, None),
        P("kv", "tp"),
        P("kv", "tp", None, None),
        P("kv", "tp", None, None),
        P("kv", "tp", None),
        P("kv", "tp", None),
        P("kv"),
        P(),
        P("tp", "kv"),
        P("kv"),
        P("kv", "tp"),
        P("tp", "kv"),
    )
    out_specs = P("tp", "kv")
    run = functools.partial(either, mesh.shape["kv"], mesh.shape["tp"])
    return jax.shard_map(run, mesh=mesh, in_specs=in_specs, out_specs=out_specs, check_vma=False)
```

```python
import functools
from types import SimpleNamespace

import jax
import jax.numpy as jnp
from jax import lax
from jax.experimental import pallas as pl
from jax.experimental.pallas import tpu as pltpu
from jax.sharding import PartitionSpec as P

EPS = 1e-06
F32 = jnp.float32
BF16 = jnp.bfloat16
MESH = pl.DeviceIdType.MESH


def ceil_chunks(width):
    return 2 if width % 256 == 0 else 1


def inner_size(count):
    return max(d for d in range(1, count + 1) if count % d == 0 and d * d <= count)


def any_kernel(
    cfg,
    tokens,
    gain_mix,
    w_query,
    w_key,
    w_value,
    w_igate,
    w_fgate,
    bias_igate,
    bias_fgate,
    state_mem,
    state_max,
    keys_blk,
    values_blk,
    igate_blk,
    fgate_blk,
    lengths,
    gain_head,
    w_mixout,
    gain_mlp,
    w_up,
    w_down,
    out,
    wq_v,
    wk_v,
    wv_v,
    state_v,
    state_hi,
    state_lo,
    keys_v,
    values_v,
    wo_v,
    wu_v,
    wd_v,
    tok_all,
    proj_send,
    proj_recv,
    gate_send,
    gate_recv,
    mixed_all,
    mixed_rows,
    att_all,
    res_rows,
    sq_send,
    sq_recv,
    up_send,
    up_recv,
    hid_all,
    hid_rows,
    down_send,
    down_recv,
    local_sem,
    tok_ssem,
    tok_rsem,
    proj_ssem,
    proj_rsem,
    gate_ssem,
    gate_rsem,
    mix_ssem,
    mix_rsem,
    att_ssem,
    att_rsem,
    sq_ssem,
    sq_rsem,
    up_ssem,
    up_rsem,
    hid_ssem,
    hid_rsem,
    down_ssem,
    down_rsem,
):
    kv, tp, D = cfg
    me, core = lax.axis_index("kv"), lax.axis_index("tp")
    S, H, HD, _ = state_mem.shape
    B = keys_blk.shape[2]
    width = H * HD
    rows, feats = tokens.shape
    total_rows = rows * tp
    chunks, _, _, chunk = up_send.shape

    loads = [
        pltpu.make_async_copy(a, b, local_sem.at[i])
        for i, (a, b) in enumerate(
            (
                (w_query, wq_v),
                (w_key, wk_v),
                (w_value, wv_v),
                (state_mem, state_v),
                (keys_blk, keys_v),
                (values_blk, values_v),
                (w_mixout, wo_v),
                (w_up, wu_v),
                (w_down, wd_v),
            )
        )
    ]
    for load in loads:
        load.start()

    barrier = pltpu.get_barrier_semaphore()

    def greet_kv(d, carry):
        pl.semaphore_signal(
            barrier, inc=1, device_id=(lax.rem(me + d, kv), core), device_id_type=MESH
        )
        return carry

    def greet_tp(d, carry):
        pl.semaphore_signal(
            barrier, inc=1, device_id=(me, lax.rem(core + d, tp)), device_id_type=MESH
        )
        return carry

    lax.fori_loop(1, tp, greet_tp, 0)
    lax.fori_loop(1, kv, greet_kv, 0)

    lane = lax.broadcasted_iota(jnp.int32, (H, 128), 1)
    sub = lax.broadcasted_iota(jnp.int32, (H, 128), 0)
    pick_i = (lane == sub).astype(F32).astype(BF16)
    pick_f = (lane == sub + H).astype(F32).astype(BF16)
    w_gates = (
        jnp.dot(w_igate[...], pick_i, preferred_element_type=F32)
        + jnp.dot(w_fgate[...], pick_f, preferred_element_type=F32)
    ).astype(BF16)

    row = lax.broadcasted_iota(jnp.int32, (S, 1), 0)
    length = jnp.zeros((S, 1), jnp.int32)
    for s in range(S):
        length = jnp.where(row == s, lengths[s], length)
    live = lax.broadcasted_iota(jnp.int32, (S, B), 1) < length
    later = (
        lax.broadcasted_iota(jnp.int32, (B, B), 0) > lax.broadcasted_iota(jnp.int32, (B, B), 1)
    ).astype(F32)
    base = []
    for h in range(H):
        forget = jnp.where(live, fgate_blk[:, h, :], 0.0)
        suffix = jnp.dot(
            forget, later, preferred_element_type=F32, precision=lax.Precision.HIGHEST
        )
        past = jnp.where(live, igate_blk[:, h, :] + suffix, -jnp.inf)
        carried = state_max[:, h : h + 1] + jnp.sum(forget, axis=1, keepdims=True)
        base.append((past, jnp.max(past, axis=1, keepdims=True), carried))
    pl.semaphore_wait(barrier, kv + tp - 2)

    def to_kv(d, src, dst, ssem, rsem):
        return pltpu.make_async_remote_copy(
            src_ref=src,
            dst_ref=dst,
            send_sem=ssem,
            recv_sem=rsem,
            device_id=(lax.rem(me + d, kv), core),
            device_id_type=MESH,
        )

    def to_tp(d, src, dst, ssem, rsem):
        return pltpu.make_async_remote_copy(
            src_ref=src,
            dst_ref=dst,
            send_sem=ssem,
            recv_sem=rsem,
            device_id=(me, lax.rem(core + d, tp)),
            device_id_type=MESH,
        )

    def each(n, make, act):
        def step(d, carry):
            act(make(d))
            return carry

        lax.fori_loop(1, n, step, 0)

    start = lambda copy: copy.start()
    wait_send = lambda copy: copy.wait_send()
    wait_recv = lambda copy: copy.wait_recv()


    inner = inner_size(kv)
    outer = kv // inner
    z, p = me // inner, lax.rem(me, inner)

    def at(dz, dp):
        return lax.rem(z + dz + outer, outer) * inner + lax.rem(p + dp + inner, inner)

    def remote(src, dst, ssem, rsem, target):
        return pltpu.make_async_remote_copy(
            src_ref=src,
            dst_ref=dst,
            send_sem=ssem,
            recv_sem=rsem,
            device_id=(target, core),
            device_id_type=MESH,
        )

    def rs_inner(send, recv, ssem, rsem, dz, dp):
        i = dz * inner + dp
        return remote(send(at(dz, dp)), recv(i), ssem(i), rsem(i), at(0, dp))

    def rs_outer(send, recv, ssem, rsem, dz):
        i = dz * inner
        return remote(send(at(dz, 0)), recv(i), ssem(i), rsem(i), at(dz, 0))

    def rs_start(refs):
        for dz in list(range(1, outer)) + [0]:
            each(inner, lambda dp, dz=dz: rs_inner(*refs, dz, dp), start)

    def rs_group(refs, dz):
        send, recv = refs[:2]

        def add(dp, total):
            rs_inner(*refs, dz, dp).wait_recv()
            return total + recv(dz * inner + dp)[...].astype(F32)

        return lax.fori_loop(1, inner, add, send(at(dz, 0))[...].astype(F32))

    def rs_middle(refs):
        send = refs[0]
        for dz in range(1, outer):
            send(at(dz, 0))[...] = rs_group(refs, dz).astype(BF16)
            rs_outer(*refs, dz).start()

    def rs_end(refs):
        recv = refs[1]

        def add(dz, total):
            rs_outer(*refs, dz).wait_recv()
            return total + recv(dz * inner)[...].astype(F32)

        return lax.fori_loop(1, outer, add, rs_group(refs, 0))

    def rs_close(refs):
        for dz in range(outer):
            each(inner, lambda dp, dz=dz: rs_inner(*refs, dz, dp), wait_send)
        each(outer, lambda dz: rs_outer(*refs, dz), wait_send)

    def ag_outer(block, ssem, rsem, dz, slot):
        i = dz * inner
        return remote(block(slot), block(slot), ssem(i), rsem(i), at(dz, 0))

    def ag_inner(block, ssem, rsem, dz, dp, slot):
        i = dz * inner + dp
        return remote(block(slot), block(slot), ssem(i), rsem(i), at(0, dp))

    def ag_start(refs):
        each(outer, lambda dz: ag_outer(*refs, dz, me), start)
        each(inner, lambda dp: ag_inner(*refs, 0, dp, me), start)

    def ag_relay(refs):
        for dz in range(1, outer):
            ag_outer(*refs, dz, at(-dz, 0)).wait_recv()
            each(inner, lambda dp, dz=dz: ag_inner(*refs, dz, dp, at(-dz, 0)), start)

    def ag_end(refs):
        for dz in range(outer):
            each(inner, lambda dp, dz=dz: ag_inner(*refs, dz, dp, at(-dz, -dp)), wait_recv)

    def ag_close(refs):
        each(outer, lambda dz: ag_outer(*refs, dz, me), wait_send)
        for dz in range(outer):
            each(inner, lambda dp, dz=dz: ag_inner(*refs, dz, dp, at(-dz, 0)), wait_send)

    def views(c, *refs):
        return tuple(lambda i, ref=ref: ref.at[c, i] for ref in refs)

    def tok_out(d):
        return to_tp(d, tokens, tok_all.at[core], tok_ssem.at[d], tok_rsem.at[d])

    def tok_in(d):
        slot = lax.rem(core - d + tp, tp)
        return to_tp(d, tokens, tok_all.at[slot], tok_ssem.at[d], tok_rsem.at[d])

    each(tp, tok_out, start)
    tok_all[core] = tokens[...]

    each(tp, tok_in, wait_recv)
    widened = tok_all[...].astype(F32).reshape(total_rows, feats)
    square_in = jnp.sum(widened * widened, axis=1, keepdims=True)
    scaled_in = (widened * gain_mix[...]).astype(BF16)

    gates = jnp.dot(scaled_in, w_gates, preferred_element_type=F32)
    lane_r = lax.broadcasted_iota(jnp.int32, gates.shape, 1)
    gates = jnp.where(lane_r == 2 * H, square_in, gates)
    for j in range(kv):
        gate_send[j] = gates[j * S : (j + 1) * S]

    def gate_out(d):
        return to_kv(
            d, gate_send.at[lax.rem(me + d, kv)], gate_recv.at[d], gate_ssem.at[d], gate_rsem.at[d]
        )

    each(kv, gate_out, start)

    proj_refs = [views(i, proj_send, proj_recv, proj_ssem, proj_rsem) for i in range(1)]
    for i, w in enumerate((wq_v, wk_v, wv_v)):
        loads[i].wait()
        part = jnp.dot(scaled_in, w[...], preferred_element_type=F32)
        for j in range(kv):
            proj_send[0, j, :, i * width : (i + 1) * width] = part[j * S : (j + 1) * S].astype(BF16)
    rs_start(proj_refs[0])

    for refs in proj_refs:
        rs_middle(refs)
    loads[3].wait()

    def split(i, carry):
        s, h = i // H, lax.rem(i, H)
        full = state_v[s, h]
        hi = full.astype(BF16)
        state_hi[s, h] = hi
        state_lo[s, h] = (full - hi.astype(F32)).astype(BF16)
        return carry

    lax.fori_loop(0, S * H, split, 0)
    loads[4].wait()
    loads[5].wait()

    def gate_add(d, total):
        gate_out(d).wait_recv()
        return total + gate_recv[d]

    gate_sum = lax.fori_loop(1, kv, gate_add, gate_send[me])
    factor_in = lax.rsqrt(gate_sum[:, 2 * H : 2 * H + 1] / D + EPS)
    gate_sum = gate_sum * factor_in

    projected = (rs_end(proj_refs[0]) * factor_in).astype(BF16)
    query, key_new, value_new = (projected[:, i * width : (i + 1) * width] for i in range(3))

    scale = HD ** (-0.5)
    contract = (((1,), (1,)), ((), ()))
    mixed = []
    for h in range(H):
        cols = slice(h * HD, (h + 1) * HD)
        q, k, v = query[:, cols], key_new[:, cols], value_new[:, cols]
        past, past_top, carried = base[h]
        ig = gate_sum[:, h : h + 1] + bias_igate[h]
        raw = gate_sum[:, H + h : H + h + 1] + bias_fgate[h]
        fg = jnp.minimum(raw, 0.0) - jnp.log1p(jnp.exp(-jnp.abs(raw)))
        carried = carried + fg
        top = jnp.maximum(jnp.maximum(carried, ig), past_top + fg)
        decay = jnp.exp(past + (fg - top))
        scores = jnp.zeros((S, B), F32)
        state_term = jnp.zeros((S, HD), F32)
        for s in range(S):
            mine = row == s
            got = lax.dot_general(q, keys_v[s, h], contract, preferred_element_type=F32)
            scores = jnp.where(mine, got, scores)
            mem = lax.dot_general(
                q, state_hi[s, h], contract, preferred_element_type=F32
            ) + lax.dot_general(q, state_lo[s, h], contract, preferred_element_type=F32)
            state_term = jnp.where(mine, mem, state_term)
        weights = (decay * (scores * scale)).astype(BF16)
        block_term = jnp.zeros((S, HD), F32)
        for s in range(S):
            got = jnp.dot(weights, values_v[s, h], preferred_element_type=F32)
            block_term = jnp.where(row == s, got, block_term)
        own = jnp.sum(q.astype(F32) * k.astype(F32), axis=1, keepdims=True) * scale
        numerator = (
            state_term * jnp.exp(carried - top)
            + block_term
            + (jnp.exp(ig - top) * own) * v.astype(F32)
        )
        spread = jnp.mean(numerator * numerator, axis=1, keepdims=True)
        mixed_all[me, :, cols] = (numerator * lax.rsqrt(spread + EPS) * gain_head[...]).astype(BF16)

    def mix_out(d):
        return to_kv(d, mixed_all.at[me], mixed_all.at[me], mix_ssem.at[d], mix_rsem.at[d])

    def mix_in(d):
        slot = lax.rem(me - d + kv, kv)
        return to_kv(d, mixed_all.at[me], mixed_all.at[slot], mix_ssem.at[d], mix_rsem.at[d])

    each(kv, mix_out, start)
    for i in (6, 7, 8):
        loads[i].wait()
    each(kv, mix_in, wait_recv)
    for j in range(kv):
        mixed_rows[j * S : (j + 1) * S] = mixed_all[j].astype(F32)
    att_all[core] = jnp.dot(
        mixed_rows[...].astype(BF16), wo_v[...], preferred_element_type=F32
    ).astype(BF16)

    def att_out(d):
        return to_tp(d, att_all.at[core], att_all.at[core], att_ssem.at[d], att_rsem.at[d])

    def att_in(d):
        slot = lax.rem(core - d + tp, tp)
        return to_tp(d, att_all.at[core], att_all.at[slot], att_ssem.at[d], att_rsem.at[d])

    each(tp, att_out, start)
    each(tp, att_in, wait_recv)
    attended = att_all[0].astype(F32)
    for t in range(1, tp):
        attended = attended + att_all[t].astype(F32)
    restored = (widened + attended).astype(BF16).astype(F32)
    res_rows[...] = restored.reshape(tp, rows, feats)
    square_mid = jnp.sum(restored * restored, axis=1, keepdims=True)
    square_wide = jnp.broadcast_to(square_mid, (total_rows, 128))
    for j in range(kv):
        sq_send[j] = square_wide[j * S : (j + 1) * S]

    def sq_out(d):
        return to_kv(
            d, sq_send.at[lax.rem(me + d, kv)], sq_recv.at[d], sq_ssem.at[d], sq_rsem.at[d]
        )

    each(kv, sq_out, start)
    scaled_mid = (restored * gain_mlp[...]).astype(BF16)

    up_refs = [views(c, up_send, up_recv, up_ssem, up_rsem) for c in range(chunks)]
    hid_refs = [views(c, hid_all, hid_ssem, hid_rsem) for c in range(chunks)]

    for c in range(chunks):
        part = jnp.dot(
            scaled_mid, wu_v[:, c * chunk : (c + 1) * chunk], preferred_element_type=F32
        )
        for j in range(kv):
            up_send[c, j] = part[j * S : (j + 1) * S].astype(BF16)
        rs_start(up_refs[c])

    def sq_add(d, total):
        sq_out(d).wait_recv()
        return total + sq_recv[d]

    square_sum = lax.fori_loop(1, kv, sq_add, sq_send[me])
    factor_mid = lax.rsqrt(square_sum[:, 0:1] / D + EPS)

    for refs in up_refs:
        rs_middle(refs)
    for c in range(chunks):
        active = jnp.maximum(rs_end(up_refs[c]) * factor_mid, 0.0)
        hid_all[c, me] = (active * active).astype(BF16)
        ag_start(hid_refs[c])
        if c > 0:
            ag_relay(hid_refs[c - 1])
    ag_relay(hid_refs[-1])

    down = jnp.zeros((total_rows, feats), F32)
    for c in range(chunks):
        ag_end(hid_refs[c])
        for j in range(kv):
            hid_rows[j * S : (j + 1) * S] = hid_all[c, j].astype(F32)
        down = down + jnp.dot(
            hid_rows[...].astype(BF16),
            wd_v[c * chunk : (c + 1) * chunk],
            preferred_element_type=F32,
        )
    down_send[...] = down.astype(BF16).reshape(tp, rows, feats)

    def down_out(d):
        return to_tp(
            d, down_send.at[lax.rem(core + d, tp)], down_recv.at[d], down_ssem.at[d], down_rsem.at[d]
        )

    each(tp, down_out, start)

    each(tp, tok_out, wait_send)
    each(kv, gate_out, wait_send)
    for refs in proj_refs + up_refs:
        rs_close(refs)
    for refs in hid_refs:
        ag_close(refs)
    each(kv, mix_out, wait_send)
    each(tp, att_out, wait_send)
    each(kv, sq_out, wait_send)

    def down_add(d, total):
        down_out(d).wait_recv()
        return total + down_recv[d].astype(F32)

    total = lax.fori_loop(1, tp, down_add, down_send[core].astype(F32))
    out[...] = (res_rows[core] + total).astype(out.dtype)
    each(tp, down_out, wait_send)


def any_body(kv, tp, *args):
    (
        tokens,
        gain_mix,
        w_query,
        w_key,
        w_value,
        w_igate,
        w_fgate,
        bias_igate,
        bias_fgate,
        state_mem,
        state_max,
        keys_blk,
        values_blk,
        igate_blk,
        fgate_blk,
        lengths,
        gain_head,
        w_mixout,
        gain_mlp,
        w_up,
        w_down,
    ) = args
    rows, feats = tokens.shape
    S, H, HD, _ = state_mem.shape
    width = H * HD
    hidden = w_up.shape[1]
    chunks = ceil_chunks(hidden)
    chunk = hidden // chunks
    vm = pl.BlockSpec(memory_space=pltpu.VMEM)
    sm = pl.BlockSpec(memory_space=pltpu.SMEM)
    hbm = pl.BlockSpec(memory_space=pl.ANY)
    in_specs = [
        vm,
        vm,
        hbm,
        hbm,
        hbm,
        vm,
        vm,
        sm,
        sm,
        hbm,
        vm,
        hbm,
        hbm,
        vm,
        vm,
        sm,
        vm,
        hbm,
        vm,
        hbm,
        hbm,
    ]
    V = pltpu.VMEM
    dma = pltpu.SemaphoreType.DMA
    scratch = [
        V(w_query.shape, BF16),
        V(w_key.shape, BF16),
        V(w_value.shape, BF16),
        V(state_mem.shape, F32),
        V(state_mem.shape, BF16),
        V(state_mem.shape, BF16),
        V(keys_blk.shape, BF16),
        V(values_blk.shape, BF16),
        V(w_mixout.shape, BF16),
        V(w_up.shape, BF16),
        V(w_down.shape, BF16),
        V((tp, rows, feats), BF16),
        V((1, kv, S, 3 * width), BF16),
        V((1, kv, S, 3 * width), BF16),
        V((kv, S, 128), F32),
        V((kv, S, 128), F32),
        V((kv, S, width), BF16),
        V((kv * S, width), F32),
        V((tp, kv * S, feats), BF16),
        V((tp, rows, feats), F32),
        V((kv, S, 128), F32),
        V((kv, S, 128), F32),
        V((chunks, kv, S, chunk), BF16),
        V((chunks, kv, S, chunk), BF16),
        V((chunks, kv, S, chunk), BF16),
        V((kv * S, chunk), F32),
        V((tp, rows, feats), BF16),
        V((tp, rows, feats), BF16),
        dma((9,)),
        dma((tp,)),
        dma((tp,)),
        dma((1, kv)),
        dma((1, kv)),
        dma((kv,)),
        dma((kv,)),
        dma((kv,)),
        dma((kv,)),
        dma((tp,)),
        dma((tp,)),
        dma((kv,)),
        dma((kv,)),
        dma((chunks, kv)),
        dma((chunks, kv)),
        dma((chunks, kv)),
        dma((chunks, kv)),
        dma((tp,)),
        dma((tp,)),
    ]
    return pl.pallas_call(
        functools.partial(any_kernel, (kv, tp, kv * feats)),
        out_shape=jax.ShapeDtypeStruct((rows, feats), BF16),
        in_specs=in_specs,
        out_specs=vm,
        scratch_shapes=scratch,
        compiler_params=pltpu.CompilerParams(
            collective_id=0, has_side_effects=True, vmem_limit_bytes=56 * 1024 * 1024
        ),
    )(
        tokens,
        gain_mix.reshape(1, -1),
        w_query,
        w_key,
        w_value,
        w_igate,
        w_fgate,
        bias_igate,
        bias_fgate,
        state_mem,
        state_max,
        keys_blk,
        values_blk,
        igate_blk,
        fgate_blk,
        lengths,
        gain_head.reshape(1, -1),
        w_mixout,
        gain_mlp.reshape(1, -1),
        w_up,
        w_down,
    )


def flip(index, mask):
    bit = 1
    while bit <= mask:
        if mask & bit:
            index = index + bit * (1 - 2 * lax.rem(lax.div(index, bit), 2))
        bit *= 2
    return index


def stages(kv):
    inner = inner_size(kv)
    outer = kv // inner
    if (inner, outer) != (4, 4):
        return (([m for m in range(inner)], [m * inner for m in range(outer)]),)
    ways = (((1, 2), (4, 8)), ((1, 4), (2, 8)), ((2, 4), (1, 8)))
    return tuple(tuple([0, a, b, a + b] for a, b in way) for way in ways)


def kernel(cfg, names, *refs):
    kv, tp, D = cfg
    r = SimpleNamespace(**dict(zip(names, refs, strict=True)))
    me, core = lax.axis_index("kv"), lax.axis_index("tp")
    inner = inner_size(kv)
    outer = kv // inner
    other = 1 - core
    ways = stages(kv)

    def split(way):
        def place(masks):
            total, step = 0, 1
            while step < len(masks):
                total = total + step * lax.rem(lax.div(me, masks[step]), 2)
                step *= 2
            return total

        return place(way[1]), place(way[0])
    S, H, HD, _ = r.state_mem.shape
    B = r.fgate_blk.shape[2]
    width = H * HD
    R, F = r.tokens.shape
    per = kv // tp
    half = lax.div(me, per)
    jj_me = lax.rem(me, per)
    chunks, _, _, CW = r.up_send.shape
    proj_way = [ways[a % len(ways)] for a in range(4)]
    up_way = [ways[c % len(ways)] for c in range(chunks)]

    cube = kv // 2
    reach = {m for first, _ in ways for m in first if m}
    reach |= {m % cube for _, second in ways for m in second if m % cube}

    barrier = pltpu.get_barrier_semaphore()

    def greet(target, c):
        pl.semaphore_signal(barrier, inc=1, device_id=(target, c), device_id_type=MESH)

    greet(me, other)
    for m in sorted(reach, reverse=True):
        greet(flip(me, m), 1)

    @pl.when(core == 1)
    def _():
        greet(flip(me, cube), 1)


    taken = iter(range(r.local_sem.shape[0]))

    def load(whole, *pieces):
        sem = r.local_sem.at[next(taken)]
        for i, piece in enumerate(pieces):
            dst = whole if len(pieces) == 1 else whole.at[i]
            pltpu.make_async_copy(piece, dst, sem).start()
        return pltpu.make_async_copy(whole, whole, sem)

    got_tokens = load(r.v_tokens, r.tokens)
    got_gain_mix = load(r.v_gain_mix, r.gain_mix)
    got_w_gate = load(r.v_w_gate, r.w_igate, r.w_fgate)
    got_w_qkv = load(r.v_w_qkv, r.w_query, r.w_key, r.w_value)
    got_blk = [
        load(r.v_gate_blk, r.fgate_blk, r.igate_blk),
        load(r.v_lengths, r.lengths),
        load(r.v_state_max, r.state_max),
        load(r.v_bias, r.bias_igate, r.bias_fgate),
    ]
    got_memory = [
        load(r.v_state_mem, r.state_mem),
        load(r.v_kv_blk, r.keys_blk, r.values_blk),
        load(r.v_gain_head, r.gain_head),
    ]
    got_gain_mlp = load(r.v_gain_mlp, r.gain_mlp)

    def loaded(copies):
        for copy in copies:
            copy.wait()

    def remote(src, dst, ssem, rsem, target, c):
        return pltpu.make_async_remote_copy(
            src_ref=src,
            dst_ref=dst,
            send_sem=ssem,
            recv_sem=rsem,
            device_id=(target, c),
            device_id_type=MESH,
        )

    def drain(ref, sem):
        remote(ref, ref, sem, sem, me, other).wait_send()

    tok_copy = remote(
        r.v_tokens, r.tok_peer, r.pair_ssem.at[0], r.pair_rsem.at[0], me, other
    )

    @pl.when(core == 0)
    def _():
        pl.semaphore_wait(barrier, 1)
        pl.semaphore_signal(r.hello_sem, inc=1, device_id=(me, other), device_id_type=MESH)

    @pl.when(core == 1)
    def _():
        pl.semaphore_wait(r.hello_sem, 1)

    got_tokens.wait()
    tok_copy.start()

    loaded([got_gain_mix, got_w_gate])
    lane = lax.broadcasted_iota(jnp.int32, (H, 128), 1)
    sub = lax.broadcasted_iota(jnp.int32, (H, 128), 0)
    pick_i = (lane == sub).astype(F32).astype(BF16)
    pick_f = (lane == sub + H).astype(F32).astype(BF16)
    first = (((0,), (0,)), ((), ()))
    w_gates = (
        lax.dot_general(r.v_w_gate[0], pick_i, first, preferred_element_type=F32)
        + lax.dot_general(r.v_w_gate[1], pick_f, first, preferred_element_type=F32)
    ).astype(BF16)
    lane_r = lax.broadcasted_iota(jnp.int32, (R, 128), 1)
    gain_mix = r.v_gain_mix[...]
    gate_send = r.gate_send
    proj_send = r.proj_send
    send_of = [*(proj_send.at[a] for a in range(3)), gate_send]
    recv_of = [*(r.proj_recv.at[a] for a in range(3)), r.gate_recv]
    mid_of = [*(r.proj_mid.at[a] for a in range(3)), r.gate_mid]
    last_of = [*(r.proj_last.at[a] for a in range(3)), r.gate_last]

    def project(rows, group):
        scaled = (rows * gain_mix).astype(BF16)
        square = jnp.sum(rows * rows, axis=1, keepdims=True)
        gates = jnp.dot(scaled, w_gates, preferred_element_type=F32)
        gates = jnp.where(lane_r == 2 * H, square, gates)
        for jj in range(per):
            gate_send[group * per + jj] = gates[jj * S : (jj + 1) * S]
        for i in range(3):
            part = jnp.dot(scaled, r.v_w_qkv[i], preferred_element_type=F32)
            for jj in range(per):
                proj_send[i, group * per + jj] = part[jj * S : (jj + 1) * S].astype(BF16)

    own_rows = r.v_tokens[...].astype(F32)
    got_w_qkv.wait()
    project(own_rows, core)

    tok_copy.wait_recv()
    project(r.tok_peer[...].astype(F32), other)

    @pl.when(core == 1)
    def _():
        pl.semaphore_wait(barrier, 2 * len(reach) + 2)
        pl.semaphore_signal(r.go_sem, inc=1, device_id=(me, other), device_id_type=MESH)
        pl.semaphore_signal(
            r.half_sem, inc=1, device_id=(flip(me, cube), core), device_id_type=MESH
        )

    @pl.when(core == 0)
    def _():
        pl.semaphore_wait(r.go_sem, 1)


    def pair(i, ref):
        return remote(ref.at[0], ref.at[1], r.pair_ssem.at[i], r.pair_rsem.at[i], me, other)

    pairs = [pair(1, r.v_w_mixout), pair(2, r.v_w_up), pair(3, r.v_w_down)]

    def proj_one(a, mz, mp):
        first, second = proj_way[a]
        return remote(
            send_of[a].at[flip(me, first[mp] + second[mz])],
            recv_of[a].at[mz, mp],
            r.proj_ssem.at[a],
            r.proj_rsem.at[a, mz // (outer // 2)],
            flip(me, first[mp]),
            other,
        )

    def proj_two(a, mz):
        return remote(
            mid_of[a].at[mz],
            last_of[a].at[mz],
            r.mid_ssem.at[a],
            r.mid_rsem.at[a],
            flip(me, proj_way[a][1][mz]),
            other,
        )

    far = [mz for mz in reversed(range(outer)) if mz >= outer // 2]
    near = [mz for mz in reversed(range(outer)) if mz < outer // 2]
    peers = list(reversed(range(inner)))

    def send_groups(a, groups):
        for mz in groups:
            for mp in peers:
                proj_one(a, mz, mp).start()

    for a in (3, 0, 1, 2):
        send_groups(a, far)
        send_groups(a, near)

    got_w_mixout = load(r.v_w_mixout.at[0], r.w_mixout)
    got_w_up = load(r.v_w_up.at[0], r.w_up)
    got_w_down = load(r.v_w_down.at[0], r.w_down)

    loaded(got_memory)

    def narrow(i, carry):
        s, h = lax.div(i, H), lax.rem(i, H)
        r.state_t[s, h] = r.v_state_mem[s, h].T.astype(BF16)
        r.keys_t[s, h] = r.v_kv_blk[0, s, h].T
        return carry

    lax.fori_loop(0, S * H, narrow, 0)
    got_w_mixout.wait()
    pairs[0].start()

    def summed(ref):
        total = ref[0].astype(F32)
        for i in range(1, ref.shape[0]):
            total = total + ref[i].astype(F32)
        return total

    def proj_middle(a):
        for side, groups in ((1, far), (0, near)):
            drain(
                recv_of[a].at[pl.ds(side * (outer // 2), outer // 2)], r.proj_rsem.at[a, side]
            )
            for mz in groups:
                mid_of[a][mz] = summed(recv_of[a].at[mz]).astype(mid_of[a].dtype)
                proj_two(a, mz).start()

    def proj_end(a):
        drain(last_of[a], r.mid_rsem.at[a])
        return summed(last_of[a])

    @pl.when(core == 1)
    def _():
        pl.semaphore_wait(r.half_sem, 1)
        pl.semaphore_signal(r.half_sem, inc=1, device_id=(me, other), device_id_type=MESH)

    @pl.when(core == 0)
    def _():
        pl.semaphore_wait(r.half_sem, 1)

    for a in (3, 0, 1, 2):
        proj_middle(a)
    got_w_up.wait()
    pairs[1].start()

    loaded(got_blk)
    row = lax.broadcasted_iota(jnp.int32, (S, 1), 0)
    eye_s = lax.broadcasted_iota(jnp.int32, (S, S), 0) == lax.broadcasted_iota(jnp.int32, (S, S), 1)
    length = jnp.sum(
        jnp.where(eye_s, r.v_lengths[...].astype(F32), 0.0), axis=1, keepdims=True
    )
    live = lax.broadcasted_iota(jnp.int32, (S, B), 1).astype(F32) < length
    later = (
        lax.broadcasted_iota(jnp.int32, (B, B), 0) > lax.broadcasted_iota(jnp.int32, (B, B), 1)
    ).astype(F32)
    base = []
    for h in range(H):
        forget = jnp.where(live, r.v_gate_blk[0, :, h, :], 0.0)
        suffix = jnp.dot(
            forget, later, preferred_element_type=F32, precision=lax.Precision.HIGHEST
        )
        past = jnp.where(live, r.v_gate_blk[1, :, h, :] + suffix, -jnp.inf)
        carried = r.v_state_max[:, h : h + 1] + jnp.sum(forget, axis=1, keepdims=True)
        base.append((past, jnp.max(past, axis=1, keepdims=True), carried))
    gate_sum = proj_end(3)
    factor_in = lax.rsqrt(gate_sum[:, 2 * H : 2 * H + 1] / D + EPS)
    gate_sum = gate_sum * factor_in
    scale = HD ** (-0.5)
    shares = []
    for h in range(H):
        past, past_top, carried = base[h]
        ig = gate_sum[:, h : h + 1] + r.v_bias[0, :, h : h + 1]
        raw = gate_sum[:, H + h : H + h + 1] + r.v_bias[1, :, h : h + 1]
        fg = jnp.minimum(raw, 0.0) - jnp.log1p(jnp.exp(-jnp.abs(raw)))
        carried = carried + fg
        top = jnp.maximum(jnp.maximum(carried, ig), past_top + fg)
        shares.append((jnp.exp(past + (fg - top)) * scale, jnp.exp(carried - top), jnp.exp(ig - top)))
    query = (proj_end(0) * factor_in).astype(BF16)

    cells, weights_of, state_of = [], [], []
    for h in range(H):
        q = query[:, h * HD : (h + 1) * HD]
        scores = jnp.zeros((S, B), F32)
        for s in range(S):
            got = jnp.dot(q, r.keys_t[s, h], preferred_element_type=F32)
            scores = jnp.where(row == s, got, scores)
        weights_of.append((shares[h][0] * scores).astype(BF16))
    for h in range(H):
        q = query[:, h * HD : (h + 1) * HD]
        state_term = jnp.zeros((S, HD), F32)
        for s in range(S):
            mem = jnp.dot(q, r.state_t[s, h], preferred_element_type=F32)
            state_term = jnp.where(row == s, mem, state_term)
        state_of.append(state_term)
    for h in range(H):
        weights, state_term = weights_of[h], state_of[h]
        _, remaining, entering = shares[h]
        block_term = jnp.zeros((S, HD), F32)
        for s in range(S):
            got = jnp.dot(weights, r.v_kv_blk[1, s, h], preferred_element_type=F32)
            block_term = jnp.where(row == s, got, block_term)
        cells.append((state_term * remaining + block_term, entering))

    key_new = (proj_end(1) * factor_in).astype(BF16)
    value_new = (proj_end(2) * factor_in).astype(BF16)
    for h in range(H):
        cols = slice(h * HD, (h + 1) * HD)
        q, k, v = query[:, cols], key_new[:, cols], value_new[:, cols]
        older, entering = cells[h]
        own = jnp.sum(q.astype(F32) * k.astype(F32), axis=1, keepdims=True) * scale
        numerator = older + (entering * own) * v.astype(F32)
        spread = jnp.mean(numerator * numerator, axis=1, keepdims=True)
        r.mixed_own[:, cols] = (
            numerator * lax.rsqrt(spread + EPS) * r.v_gain_head[...]
        ).astype(BF16)

    mixed_all = r.mixed_all
    slot = lax.rem(half + core, 2)
    mine_at = slot * per + jj_me

    def mix_copy(m):
        return remote(
            r.mixed_own,
            mixed_all.at[mine_at],
            r.mix_ssem,
            r.mix_rsem,
            flip(me, m),
            half,
        )

    for m in reversed(range(1, kv)):
        mix_copy(m).start()

    @pl.when(slot == 1)
    def _():
        mix_copy(0).start()

    @pl.when(slot == 0)
    def _():
        mixed_all[mine_at] = r.mixed_own[...]

    loaded([got_w_down, got_gain_mlp])
    pairs[0].wait()

    @pl.when(half == core)
    def _():
        drain(mixed_all.at[pl.ds(0, kv - 1)], r.mix_rsem)

    @pl.when(half != core)
    def _():
        drain(mixed_all, r.mix_rsem)

    mixed_rows = r.mixed_rows
    attended = jnp.zeros((R, F), F32)
    for c in range(tp):
        for jj in range(per):
            mixed_rows[jj * S : (jj + 1) * S, c * width : (c + 1) * width] = mixed_all[
                c * per + jj
            ].astype(F32)
        attended = attended + jnp.dot(
            mixed_rows[:, c * width : (c + 1) * width].astype(BF16),
            r.v_w_mixout[c],
            preferred_element_type=F32,
        ).astype(BF16).astype(F32)

    restored = (own_rows + attended).astype(BF16).astype(F32)
    r.res_rows[...] = restored
    scaled_mid = (restored * r.v_gain_mlp[...]).astype(BF16)

    up_send, up_recv, up_mid, up_last = r.up_send, r.up_recv, r.up_mid, r.up_last

    def up_one(c, mz, mp):
        place = split(up_way[c])
        return remote(
            up_send.at[c, flip(place[0], mz) * inner + flip(place[1], mp)],
            up_recv.at[c, mz, mp],
            r.up_ssem,
            r.up_rsem.at[c, mz // (outer // 2)],
            flip(me, up_way[c][0][mp]),
            other,
        )

    def up_two(c, mz):
        return remote(
            up_mid.at[c, mz],
            up_last.at[c, mz],
            r.mid_ssem.at[4],
            r.up_lsem.at[c],
            flip(me, up_way[c][1][mz]),
            other,
        )

    parts = chunks // tp
    span = kv * CW

    def up_start(c, groups):
        for mz in groups:
            for mp in peers:
                up_one(c, mz, mp).start()

    def up_compute(c):
        if c == parts:
            pairs[1].wait()
        begin = (c % parts) * span
        part = jnp.dot(
            scaled_mid,
            r.v_w_up[c // parts, :, begin : begin + span],
            preferred_element_type=F32,
        ).astype(BF16)
        for j in range(kv):
            up_send[c, j] = part[:, j * CW : (j + 1) * CW]

    plan = [(c, side) for c in range(chunks) for side in (1, 0)]
    for i, (c, side) in enumerate(plan):
        if c not in [x for x, _ in plan[:i]]:
            up_compute(c)
        up_start(c, far if side else near)
    pairs[2].start()

    square_mid = jnp.sum(restored * restored, axis=1, keepdims=True)
    eye_r = lax.broadcasted_iota(jnp.int32, (R, 128), 0) == lane_r
    r.sq_all[0] = jnp.sum(jnp.where(eye_r, square_mid, 0.0), axis=0, keepdims=True)

    def sq_copy(m):
        return remote(
            r.sq_all.at[0],
            r.sq_all.at[m],
            r.sq_ssem,
            r.sq_rsem,
            flip(me, m),
            core,
        )

    for m in reversed(range(1, kv)):
        sq_copy(m).start()

    def up_middle(c, side):
        drain(up_recv.at[c, pl.ds(side * (outer // 2), outer // 2)], r.up_rsem.at[c, side])
        for mz in far if side else near:
            up_mid[c, mz] = summed(up_recv.at[c, mz]).astype(BF16)
            up_two(c, mz).start()

    hid_mid, hid_all = r.hid_mid, r.hid_all

    def hid_near(c, mp):
        mine = hid_all.at[c, 0, split(up_way[c])[1]]
        return remote(
            mine,
            mine,
            r.hid_ssem.at[2],
            r.hid_rsem.at[c],
            flip(me, up_way[c][0][mp]),
            core,
        )

    def hid_one(c, mz):
        return remote(
            hid_all.at[c, 0, split(up_way[c])[1]],
            hid_mid.at[c, mz],
            r.hid_ssem.at[0],
            r.hid_msem.at[c, mz - 1],
            flip(me, up_way[c][1][mz]),
            other,
        )

    def hid_two(c, mz, mp):
        return remote(
            hid_mid.at[c, mz],
            hid_all.at[c, mz, split(up_way[c])[1]],
            r.hid_ssem.at[1],
            r.hid_rsem.at[c],
            flip(me, up_way[c][0][mp]),
            other,
        )

    def hid_start(c):
        drain(up_last.at[c], r.up_lsem.at[c])
        active = jnp.maximum(summed(up_last.at[c]), 0.0)
        hid_all[c, 0, split(up_way[c])[1]] = (active * active).astype(BF16)
        for mz in reversed(range(1, outer)):
            hid_one(c, mz).start()
        for mp in peers[:-1]:
            hid_near(c, mp).start()

    def hid_relay(c, mz):
        drain(hid_mid.at[c, mz], r.hid_msem.at[c, mz - 1])
        for mp in peers:
            hid_two(c, mz, mp).start()

    def hops(mz):
        return 1.8 + 0.7 * ((mz & 1) + 2 * (mz >> 1)) if mz else 0.9

    steps, ready = [], [0.0] * chunks
    for i, (c, side) in enumerate(plan):
        due = 3.2 * (i + 1) / len(plan) + 2.8
        steps.append((due, up_middle, c, side))
        ready[c] = max([ready[c], *(due + hops(mz) for mz in (far if side else near))])
    for c in range(chunks):
        steps.append((ready[c] + 0.2, hid_start, c))
        for mz in range(1, outer):
            steps.append((ready[c] + 0.4 + hops(mz), hid_relay, c, mz))
    order = [step[1:] for step in sorted(steps, key=lambda step: step[0])]
    for step, *which in order:
        step(*which)

    tok_copy.wait_send()
    for a in range(4):
        drain(recv_of[a], r.proj_ssem.at[a])
        drain(last_of[a], r.mid_ssem.at[a])

    @pl.when(slot == 0)
    def _():
        drain(mixed_all.at[pl.ds(0, kv - 1)], r.mix_ssem)

    @pl.when(slot == 1)
    def _():
        drain(mixed_all, r.mix_ssem)

    drain(r.sq_all.at[pl.ds(1, kv - 1)], r.sq_ssem)
    drain(up_recv, r.up_ssem)
    drain(up_last, r.mid_ssem.at[4])
    pairs[2].wait()
    drain(r.sq_all.at[pl.ds(1, kv - 1)], r.sq_rsem)
    squares = r.sq_all[0]
    for m in range(1, kv):
        squares = squares + r.sq_all[m]
    square_sum = jnp.sum(jnp.where(eye_r, squares, 0.0), axis=1, keepdims=True)
    factor_mid = lax.rsqrt(square_sum / D + EPS)
    drain(hid_mid.at[:, pl.ds(1, outer - 1)], r.hid_ssem.at[0])
    drain(hid_all.at[:, 0, pl.ds(1, inner - 1)], r.hid_ssem.at[2])

    flat = r.up_send.at[0]
    down = jnp.zeros((R, F), F32)
    for c in range(chunks):
        drain(flat.at[pl.ds(0, kv - 1)], r.hid_rsem.at[c])
        for mz in range(outer):
            group = flip(split(up_way[c])[0], mz)
            begin = pl.multiple_of((c % parts) * span + group * (inner * CW), inner * CW)
            down = down + jnp.dot(
                jnp.concatenate([hid_all[c, mz, pt] for pt in range(inner)], axis=1),
                r.v_w_down[c // parts, pl.ds(begin, inner * CW), :],
                preferred_element_type=F32,
            )
    r.out[...] = (r.res_rows[...] + down * (factor_mid * factor_mid)).astype(BF16)
    drain(hid_all.at[:, pl.ds(1, outer - 1)], r.hid_ssem.at[1])


def named(
    tokens,
    gain_mix,
    w_query,
    w_key,
    w_value,
    w_igate,
    w_fgate,
    bias_igate,
    bias_fgate,
    state_mem,
    state_max,
    keys_blk,
    values_blk,
    igate_blk,
    fgate_blk,
    lengths,
    gain_head,
    w_mixout,
    gain_mlp,
    w_up,
    w_down,
):
    return SimpleNamespace(**locals())


def body(kv, tp, *args):
    a = named(*args)
    a.gain_mix, a.gain_head, a.gain_mlp, a.bias_igate, a.bias_fgate, a.lengths = (
        x.reshape(1, -1)
        for x in (a.gain_mix, a.gain_head, a.gain_mlp, a.bias_igate, a.bias_fgate, a.lengths)
    )
    a.w_igate, a.w_fgate = a.w_igate.T, a.w_fgate.T
    rows, feats = a.tokens.shape
    S, H, HD, _ = a.state_mem.shape
    B = a.keys_blk.shape[2]
    width = H * HD
    inner = inner_size(kv)
    outer = kv // inner
    per = kv // tp
    hidden = a.w_up.shape[1]
    chunks = tp * max(n for n in (1, 2) if hidden % (n * kv * 128) == 0)
    cw = hidden * tp // (chunks * kv)
    V = pltpu.VMEM
    dma = pltpu.SemaphoreType.DMA

    def room(x, *many):
        return V((*many, *x.shape), x.dtype)

    scratch = dict(
        v_tokens=room(a.tokens),
        v_gain_mix=room(a.gain_mix),
        v_lengths=room(a.lengths),
        v_state_max=room(a.state_max),
        v_gain_head=room(a.gain_head),
        v_gain_mlp=room(a.gain_mlp),
        v_state_mem=room(a.state_mem),
        v_w_gate=room(a.w_igate, 2),
        v_w_qkv=room(a.w_query, 3),
        v_gate_blk=room(a.fgate_blk, 2),
        v_bias=room(a.bias_igate, 2),
        v_kv_blk=room(a.keys_blk, 2),
        v_w_mixout=room(a.w_mixout, tp),
        v_w_up=room(a.w_up, tp),
        v_w_down=room(a.w_down, tp),
        state_t=V(a.state_mem.shape, BF16),
        keys_t=V((S, H, HD, B), BF16),
        tok_peer=room(a.tokens),
        proj_send=V((3, kv, S, width), BF16),
        proj_recv=V((3, outer, inner, S, width), BF16),
        proj_mid=V((3, outer, S, width), BF16),
        proj_last=V((3, outer, S, width), BF16),
        gate_send=V((kv, S, 128), F32),
        gate_recv=V((outer, inner, S, 128), F32),
        gate_mid=V((outer, S, 128), F32),
        gate_last=V((outer, S, 128), F32),
        mixed_own=V((S, width), BF16),
        mixed_all=V((tp * per, S, width), BF16),
        mixed_rows=V((rows, tp * width), F32),
        res_rows=V((rows, feats), F32),
        sq_all=V((kv, 1, 128), F32),
        up_send=V((chunks, kv, rows, cw), BF16),
        up_recv=V((chunks, outer, inner, rows, cw), BF16),
        up_mid=V((chunks, outer, rows, cw), BF16),
        up_last=V((chunks, outer, rows, cw), BF16),
        hid_mid=V((chunks, outer, rows, cw), BF16),
        hid_all=V((chunks, outer, inner, rows, cw), BF16),
        local_sem=dma((15,)),
        pair_ssem=dma((4,)),
        pair_rsem=dma((4,)),
        proj_ssem=dma((4,)),
        proj_rsem=dma((4, 2)),
        mid_ssem=dma((5,)),
        mid_rsem=dma((4,)),
        mix_ssem=dma,
        mix_rsem=dma,
        sq_ssem=dma,
        sq_rsem=dma,
        up_ssem=dma,
        up_rsem=dma((chunks, 2)),
        up_lsem=dma((chunks,)),
        hid_ssem=dma((3,)),
        hid_msem=dma((chunks, outer - 1)),
        hid_rsem=dma((chunks,)),
        go_sem=pltpu.SemaphoreType.REGULAR,
        half_sem=pltpu.SemaphoreType.REGULAR,
        hello_sem=pltpu.SemaphoreType.REGULAR,
    )
    operands = vars(a)
    names = (*operands, "out", *scratch)
    return pl.pallas_call(
        functools.partial(kernel, (kv, tp, kv * feats), names),
        out_shape=V((rows, feats), BF16),
        in_specs=[pl.BlockSpec(memory_space=pl.ANY)] * len(operands),
        out_specs=pl.BlockSpec(memory_space=V),
        scratch_shapes=list(scratch.values()),
        compiler_params=pltpu.CompilerParams(
            collective_id=0, has_side_effects=True, vmem_limit_bytes=56 * 1024 * 1024
        ),
    )(*operands.values())


def suits(kv, tp, *args):
    a = named(*args)
    inner = inner_size(kv)
    outer = kv // inner
    return (
        tp == 2
        and kv & (kv - 1) == 0
        and outer > 1
        and inner > 1
        and a.tokens.shape[1] % 128 == 0
        and a.tokens.shape[0] <= 128
        and a.w_up.shape[1] % (kv * 128) == 0
    )


def either(kv, tp, *args):
    return (body if suits(kv, tp, *args) else any_body)(kv, tp, *args)


def solution(mesh):
    in_specs = (
        P("tp", "kv"),
        P("kv"),
        P("kv", "tp"),
        P("kv", "tp"),
        P("kv", "tp"),
        P("kv", "tp"),
        P("kv", "tp"),
        P("tp"),
        P("tp"),
        P("kv", "tp", None, None),
        P("kv", "tp"),
        P("kv", "tp", None, None),
        P("kv", "tp", None, None),
        P("kv", "tp", None),
        P("kv", "tp", None),
        P("kv"),
        P(),
        P("tp", "kv"),
        P("kv"),
        P("kv", "tp"),
        P("tp", "kv"),
    )
    out_specs = P("tp", "kv")
    run = functools.partial(either, mesh.shape["kv"], mesh.shape["tp"])
    return jax.shard_map(run, mesh=mesh, in_specs=in_specs, out_specs=out_specs, check_vma=False)
```

```python
import functools
from types import SimpleNamespace

import jax
import jax.numpy as jnp
from jax import lax
from jax.experimental import pallas as pl
from jax.experimental.pallas import tpu as pltpu
from jax.sharding import PartitionSpec as P

EPS = 1e-06
F32 = jnp.float32
BF16 = jnp.bfloat16
MESH = pl.DeviceIdType.MESH


def ceil_chunks(width):
    return 2 if width % 256 == 0 else 1


def inner_size(count):
    return max(d for d in range(1, count + 1) if count % d == 0 and d * d <= count)


def any_kernel(
    cfg,
    tokens,
    gain_mix,
    w_query,
    w_key,
    w_value,
    w_igate,
    w_fgate,
    bias_igate,
    bias_fgate,
    state_mem,
    state_max,
    keys_blk,
    values_blk,
    igate_blk,
    fgate_blk,
    lengths,
    gain_head,
    w_mixout,
    gain_mlp,
    w_up,
    w_down,
    out,
    wq_v,
    wk_v,
    wv_v,
    state_v,
    state_hi,
    state_lo,
    keys_v,
    values_v,
    wo_v,
    wu_v,
    wd_v,
    tok_all,
    proj_send,
    proj_recv,
    gate_send,
    gate_recv,
    mixed_all,
    mixed_rows,
    att_all,
    res_rows,
    sq_send,
    sq_recv,
    up_send,
    up_recv,
    hid_all,
    hid_rows,
    down_send,
    down_recv,
    local_sem,
    tok_ssem,
    tok_rsem,
    proj_ssem,
    proj_rsem,
    gate_ssem,
    gate_rsem,
    mix_ssem,
    mix_rsem,
    att_ssem,
    att_rsem,
    sq_ssem,
    sq_rsem,
    up_ssem,
    up_rsem,
    hid_ssem,
    hid_rsem,
    down_ssem,
    down_rsem,
):
    kv, tp, D = cfg
    me, core = lax.axis_index("kv"), lax.axis_index("tp")
    S, H, HD, _ = state_mem.shape
    B = keys_blk.shape[2]
    width = H * HD
    rows, feats = tokens.shape
    total_rows = rows * tp
    chunks, _, _, chunk = up_send.shape

    loads = [
        pltpu.make_async_copy(a, b, local_sem.at[i])
        for i, (a, b) in enumerate(
            (
                (w_query, wq_v),
                (w_key, wk_v),
                (w_value, wv_v),
                (state_mem, state_v),
                (keys_blk, keys_v),
                (values_blk, values_v),
                (w_mixout, wo_v),
                (w_up, wu_v),
                (w_down, wd_v),
            )
        )
    ]
    for load in loads:
        load.start()

    barrier = pltpu.get_barrier_semaphore()

    def greet_kv(d, carry):
        pl.semaphore_signal(
            barrier, inc=1, device_id=(lax.rem(me + d, kv), core), device_id_type=MESH
        )
        return carry

    def greet_tp(d, carry):
        pl.semaphore_signal(
            barrier, inc=1, device_id=(me, lax.rem(core + d, tp)), device_id_type=MESH
        )
        return carry

    lax.fori_loop(1, tp, greet_tp, 0)
    lax.fori_loop(1, kv, greet_kv, 0)

    lane = lax.broadcasted_iota(jnp.int32, (H, 128), 1)
    sub = lax.broadcasted_iota(jnp.int32, (H, 128), 0)
    pick_i = (lane == sub).astype(F32).astype(BF16)
    pick_f = (lane == sub + H).astype(F32).astype(BF16)
    w_gates = (
        jnp.dot(w_igate[...], pick_i, preferred_element_type=F32)
        + jnp.dot(w_fgate[...], pick_f, preferred_element_type=F32)
    ).astype(BF16)

    row = lax.broadcasted_iota(jnp.int32, (S, 1), 0)
    length = jnp.zeros((S, 1), jnp.int32)
    for s in range(S):
        length = jnp.where(row == s, lengths[s], length)
    live = lax.broadcasted_iota(jnp.int32, (S, B), 1) < length
    later = (
        lax.broadcasted_iota(jnp.int32, (B, B), 0) > lax.broadcasted_iota(jnp.int32, (B, B), 1)
    ).astype(F32)
    base = []
    for h in range(H):
        forget = jnp.where(live, fgate_blk[:, h, :], 0.0)
        suffix = jnp.dot(
            forget, later, preferred_element_type=F32, precision=lax.Precision.HIGHEST
        )
        past = jnp.where(live, igate_blk[:, h, :] + suffix, -jnp.inf)
        carried = state_max[:, h : h + 1] + jnp.sum(forget, axis=1, keepdims=True)
        base.append((past, jnp.max(past, axis=1, keepdims=True), carried))
    pl.semaphore_wait(barrier, kv + tp - 2)

    def to_kv(d, src, dst, ssem, rsem):
        return pltpu.make_async_remote_copy(
            src_ref=src,
            dst_ref=dst,
            send_sem=ssem,
            recv_sem=rsem,
            device_id=(lax.rem(me + d, kv), core),
            device_id_type=MESH,
        )

    def to_tp(d, src, dst, ssem, rsem):
        return pltpu.make_async_remote_copy(
            src_ref=src,
            dst_ref=dst,
            send_sem=ssem,
            recv_sem=rsem,
            device_id=(me, lax.rem(core + d, tp)),
            device_id_type=MESH,
        )

    def each(n, make, act):
        def step(d, carry):
            act(make(d))
            return carry

        lax.fori_loop(1, n, step, 0)

    start = lambda copy: copy.start()
    wait_send = lambda copy: copy.wait_send()
    wait_recv = lambda copy: copy.wait_recv()


    inner = inner_size(kv)
    outer = kv // inner
    z, p = me // inner, lax.rem(me, inner)

    def at(dz, dp):
        return lax.rem(z + dz + outer, outer) * inner + lax.rem(p + dp + inner, inner)

    def remote(src, dst, ssem, rsem, target):
        return pltpu.make_async_remote_copy(
            src_ref=src,
            dst_ref=dst,
            send_sem=ssem,
            recv_sem=rsem,
            device_id=(target, core),
            device_id_type=MESH,
        )

    def rs_inner(send, recv, ssem, rsem, dz, dp):
        i = dz * inner + dp
        return remote(send(at(dz, dp)), recv(i), ssem(i), rsem(i), at(0, dp))

    def rs_outer(send, recv, ssem, rsem, dz):
        i = dz * inner
        return remote(send(at(dz, 0)), recv(i), ssem(i), rsem(i), at(dz, 0))

    def rs_start(refs):
        for dz in list(range(1, outer)) + [0]:
            each(inner, lambda dp, dz=dz: rs_inner(*refs, dz, dp), start)

    def rs_group(refs, dz):
        send, recv = refs[:2]

        def add(dp, total):
            rs_inner(*refs, dz, dp).wait_recv()
            return total + recv(dz * inner + dp)[...].astype(F32)

        return lax.fori_loop(1, inner, add, send(at(dz, 0))[...].astype(F32))

    def rs_middle(refs):
        send = refs[0]
        for dz in range(1, outer):
            send(at(dz, 0))[...] = rs_group(refs, dz).astype(BF16)
            rs_outer(*refs, dz).start()

    def rs_end(refs):
        recv = refs[1]

        def add(dz, total):
            rs_outer(*refs, dz).wait_recv()
            return total + recv(dz * inner)[...].astype(F32)

        return lax.fori_loop(1, outer, add, rs_group(refs, 0))

    def rs_close(refs):
        for dz in range(outer):
            each(inner, lambda dp, dz=dz: rs_inner(*refs, dz, dp), wait_send)
        each(outer, lambda dz: rs_outer(*refs, dz), wait_send)

    def ag_outer(block, ssem, rsem, dz, slot):
        i = dz * inner
        return remote(block(slot), block(slot), ssem(i), rsem(i), at(dz, 0))

    def ag_inner(block, ssem, rsem, dz, dp, slot):
        i = dz * inner + dp
        return remote(block(slot), block(slot), ssem(i), rsem(i), at(0, dp))

    def ag_start(refs):
        each(outer, lambda dz: ag_outer(*refs, dz, me), start)
        each(inner, lambda dp: ag_inner(*refs, 0, dp, me), start)

    def ag_relay(refs):
        for dz in range(1, outer):
            ag_outer(*refs, dz, at(-dz, 0)).wait_recv()
            each(inner, lambda dp, dz=dz: ag_inner(*refs, dz, dp, at(-dz, 0)), start)

    def ag_end(refs):
        for dz in range(outer):
            each(inner, lambda dp, dz=dz: ag_inner(*refs, dz, dp, at(-dz, -dp)), wait_recv)

    def ag_close(refs):
        each(outer, lambda dz: ag_outer(*refs, dz, me), wait_send)
        for dz in range(outer):
            each(inner, lambda dp, dz=dz: ag_inner(*refs, dz, dp, at(-dz, 0)), wait_send)

    def views(c, *refs):
        return tuple(lambda i, ref=ref: ref.at[c, i] for ref in refs)

    def tok_out(d):
        return to_tp(d, tokens, tok_all.at[core], tok_ssem.at[d], tok_rsem.at[d])

    def tok_in(d):
        slot = lax.rem(core - d + tp, tp)
        return to_tp(d, tokens, tok_all.at[slot], tok_ssem.at[d], tok_rsem.at[d])

    each(tp, tok_out, start)
    tok_all[core] = tokens[...]

    each(tp, tok_in, wait_recv)
    widened = tok_all[...].astype(F32).reshape(total_rows, feats)
    square_in = jnp.sum(widened * widened, axis=1, keepdims=True)
    scaled_in = (widened * gain_mix[...]).astype(BF16)

    gates = jnp.dot(scaled_in, w_gates, preferred_element_type=F32)
    lane_r = lax.broadcasted_iota(jnp.int32, gates.shape, 1)
    gates = jnp.where(lane_r == 2 * H, square_in, gates)
    for j in range(kv):
        gate_send[j] = gates[j * S : (j + 1) * S]

    def gate_out(d):
        return to_kv(
            d, gate_send.at[lax.rem(me + d, kv)], gate_recv.at[d], gate_ssem.at[d], gate_rsem.at[d]
        )

    each(kv, gate_out, start)

    proj_refs = [views(i, proj_send, proj_recv, proj_ssem, proj_rsem) for i in range(1)]
    for i, w in enumerate((wq_v, wk_v, wv_v)):
        loads[i].wait()
        part = jnp.dot(scaled_in, w[...], preferred_element_type=F32)
        for j in range(kv):
            proj_send[0, j, :, i * width : (i + 1) * width] = part[j * S : (j + 1) * S].astype(BF16)
    rs_start(proj_refs[0])

    for refs in proj_refs:
        rs_middle(refs)
    loads[3].wait()

    def split(i, carry):
        s, h = i // H, lax.rem(i, H)
        full = state_v[s, h]
        hi = full.astype(BF16)
        state_hi[s, h] = hi
        state_lo[s, h] = (full - hi.astype(F32)).astype(BF16)
        return carry

    lax.fori_loop(0, S * H, split, 0)
    loads[4].wait()
    loads[5].wait()

    def gate_add(d, total):
        gate_out(d).wait_recv()
        return total + gate_recv[d]

    gate_sum = lax.fori_loop(1, kv, gate_add, gate_send[me])
    factor_in = lax.rsqrt(gate_sum[:, 2 * H : 2 * H + 1] / D + EPS)
    gate_sum = gate_sum * factor_in

    projected = (rs_end(proj_refs[0]) * factor_in).astype(BF16)
    query, key_new, value_new = (projected[:, i * width : (i + 1) * width] for i in range(3))

    scale = HD ** (-0.5)
    contract = (((1,), (1,)), ((), ()))
    mixed = []
    for h in range(H):
        cols = slice(h * HD, (h + 1) * HD)
        q, k, v = query[:, cols], key_new[:, cols], value_new[:, cols]
        past, past_top, carried = base[h]
        ig = gate_sum[:, h : h + 1] + bias_igate[h]
        raw = gate_sum[:, H + h : H + h + 1] + bias_fgate[h]
        fg = jnp.minimum(raw, 0.0) - jnp.log1p(jnp.exp(-jnp.abs(raw)))
        carried = carried + fg
        top = jnp.maximum(jnp.maximum(carried, ig), past_top + fg)
        decay = jnp.exp(past + (fg - top))
        scores = jnp.zeros((S, B), F32)
        state_term = jnp.zeros((S, HD), F32)
        for s in range(S):
            mine = row == s
            got = lax.dot_general(q, keys_v[s, h], contract, preferred_element_type=F32)
            scores = jnp.where(mine, got, scores)
            mem = lax.dot_general(
                q, state_hi[s, h], contract, preferred_element_type=F32
            ) + lax.dot_general(q, state_lo[s, h], contract, preferred_element_type=F32)
            state_term = jnp.where(mine, mem, state_term)
        weights = (decay * (scores * scale)).astype(BF16)
        block_term = jnp.zeros((S, HD), F32)
        for s in range(S):
            got = jnp.dot(weights, values_v[s, h], preferred_element_type=F32)
            block_term = jnp.where(row == s, got, block_term)
        own = jnp.sum(q.astype(F32) * k.astype(F32), axis=1, keepdims=True) * scale
        numerator = (
            state_term * jnp.exp(carried - top)
            + block_term
            + (jnp.exp(ig - top) * own) * v.astype(F32)
        )
        spread = jnp.mean(numerator * numerator, axis=1, keepdims=True)
        mixed_all[me, :, cols] = (numerator * lax.rsqrt(spread + EPS) * gain_head[...]).astype(BF16)

    def mix_out(d):
        return to_kv(d, mixed_all.at[me], mixed_all.at[me], mix_ssem.at[d], mix_rsem.at[d])

    def mix_in(d):
        slot = lax.rem(me - d + kv, kv)
        return to_kv(d, mixed_all.at[me], mixed_all.at[slot], mix_ssem.at[d], mix_rsem.at[d])

    each(kv, mix_out, start)
    for i in (6, 7, 8):
        loads[i].wait()
    each(kv, mix_in, wait_recv)
    for j in range(kv):
        mixed_rows[j * S : (j + 1) * S] = mixed_all[j].astype(F32)
    att_all[core] = jnp.dot(
        mixed_rows[...].astype(BF16), wo_v[...], preferred_element_type=F32
    ).astype(BF16)

    def att_out(d):
        return to_tp(d, att_all.at[core], att_all.at[core], att_ssem.at[d], att_rsem.at[d])

    def att_in(d):
        slot = lax.rem(core - d + tp, tp)
        return to_tp(d, att_all.at[core], att_all.at[slot], att_ssem.at[d], att_rsem.at[d])

    each(tp, att_out, start)
    each(tp, att_in, wait_recv)
    attended = att_all[0].astype(F32)
    for t in range(1, tp):
        attended = attended + att_all[t].astype(F32)
    restored = (widened + attended).astype(BF16).astype(F32)
    res_rows[...] = restored.reshape(tp, rows, feats)
    square_mid = jnp.sum(restored * restored, axis=1, keepdims=True)
    square_wide = jnp.broadcast_to(square_mid, (total_rows, 128))
    for j in range(kv):
        sq_send[j] = square_wide[j * S : (j + 1) * S]

    def sq_out(d):
        return to_kv(
            d, sq_send.at[lax.rem(me + d, kv)], sq_recv.at[d], sq_ssem.at[d], sq_rsem.at[d]
        )

    each(kv, sq_out, start)
    scaled_mid = (restored * gain_mlp[...]).astype(BF16)

    up_refs = [views(c, up_send, up_recv, up_ssem, up_rsem) for c in range(chunks)]
    hid_refs = [views(c, hid_all, hid_ssem, hid_rsem) for c in range(chunks)]

    for c in range(chunks):
        part = jnp.dot(
            scaled_mid, wu_v[:, c * chunk : (c + 1) * chunk], preferred_element_type=F32
        )
        for j in range(kv):
            up_send[c, j] = part[j * S : (j + 1) * S].astype(BF16)
        rs_start(up_refs[c])

    def sq_add(d, total):
        sq_out(d).wait_recv()
        return total + sq_recv[d]

    square_sum = lax.fori_loop(1, kv, sq_add, sq_send[me])
    factor_mid = lax.rsqrt(square_sum[:, 0:1] / D + EPS)

    for refs in up_refs:
        rs_middle(refs)
    for c in range(chunks):
        active = jnp.maximum(rs_end(up_refs[c]) * factor_mid, 0.0)
        hid_all[c, me] = (active * active).astype(BF16)
        ag_start(hid_refs[c])
        if c > 0:
            ag_relay(hid_refs[c - 1])
    ag_relay(hid_refs[-1])

    down = jnp.zeros((total_rows, feats), F32)
    for c in range(chunks):
        ag_end(hid_refs[c])
        for j in range(kv):
            hid_rows[j * S : (j + 1) * S] = hid_all[c, j].astype(F32)
        down = down + jnp.dot(
            hid_rows[...].astype(BF16),
            wd_v[c * chunk : (c + 1) * chunk],
            preferred_element_type=F32,
        )
    down_send[...] = down.astype(BF16).reshape(tp, rows, feats)

    def down_out(d):
        return to_tp(
            d, down_send.at[lax.rem(core + d, tp)], down_recv.at[d], down_ssem.at[d], down_rsem.at[d]
        )

    each(tp, down_out, start)

    each(tp, tok_out, wait_send)
    each(kv, gate_out, wait_send)
    for refs in proj_refs + up_refs:
        rs_close(refs)
    for refs in hid_refs:
        ag_close(refs)
    each(kv, mix_out, wait_send)
    each(tp, att_out, wait_send)
    each(kv, sq_out, wait_send)

    def down_add(d, total):
        down_out(d).wait_recv()
        return total + down_recv[d].astype(F32)

    total = lax.fori_loop(1, tp, down_add, down_send[core].astype(F32))
    out[...] = (res_rows[core] + total).astype(out.dtype)
    each(tp, down_out, wait_send)


def any_body(kv, tp, *args):
    (
        tokens,
        gain_mix,
        w_query,
        w_key,
        w_value,
        w_igate,
        w_fgate,
        bias_igate,
        bias_fgate,
        state_mem,
        state_max,
        keys_blk,
        values_blk,
        igate_blk,
        fgate_blk,
        lengths,
        gain_head,
        w_mixout,
        gain_mlp,
        w_up,
        w_down,
    ) = args
    rows, feats = tokens.shape
    S, H, HD, _ = state_mem.shape
    width = H * HD
    hidden = w_up.shape[1]
    chunks = ceil_chunks(hidden)
    chunk = hidden // chunks
    vm = pl.BlockSpec(memory_space=pltpu.VMEM)
    sm = pl.BlockSpec(memory_space=pltpu.SMEM)
    hbm = pl.BlockSpec(memory_space=pl.ANY)
    in_specs = [
        vm,
        vm,
        hbm,
        hbm,
        hbm,
        vm,
        vm,
        sm,
        sm,
        hbm,
        vm,
        hbm,
        hbm,
        vm,
        vm,
        sm,
        vm,
        hbm,
        vm,
        hbm,
        hbm,
    ]
    V = pltpu.VMEM
    dma = pltpu.SemaphoreType.DMA
    scratch = [
        V(w_query.shape, BF16),
        V(w_key.shape, BF16),
        V(w_value.shape, BF16),
        V(state_mem.shape, F32),
        V(state_mem.shape, BF16),
        V(state_mem.shape, BF16),
        V(keys_blk.shape, BF16),
        V(values_blk.shape, BF16),
        V(w_mixout.shape, BF16),
        V(w_up.shape, BF16),
        V(w_down.shape, BF16),
        V((tp, rows, feats), BF16),
        V((1, kv, S, 3 * width), BF16),
        V((1, kv, S, 3 * width), BF16),
        V((kv, S, 128), F32),
        V((kv, S, 128), F32),
        V((kv, S, width), BF16),
        V((kv * S, width), F32),
        V((tp, kv * S, feats), BF16),
        V((tp, rows, feats), F32),
        V((kv, S, 128), F32),
        V((kv, S, 128), F32),
        V((chunks, kv, S, chunk), BF16),
        V((chunks, kv, S, chunk), BF16),
        V((chunks, kv, S, chunk), BF16),
        V((kv * S, chunk), F32),
        V((tp, rows, feats), BF16),
        V((tp, rows, feats), BF16),
        dma((9,)),
        dma((tp,)),
        dma((tp,)),
        dma((1, kv)),
        dma((1, kv)),
        dma((kv,)),
        dma((kv,)),
        dma((kv,)),
        dma((kv,)),
        dma((tp,)),
        dma((tp,)),
        dma((kv,)),
        dma((kv,)),
        dma((chunks, kv)),
        dma((chunks, kv)),
        dma((chunks, kv)),
        dma((chunks, kv)),
        dma((tp,)),
        dma((tp,)),
    ]
    return pl.pallas_call(
        functools.partial(any_kernel, (kv, tp, kv * feats)),
        out_shape=jax.ShapeDtypeStruct((rows, feats), BF16),
        in_specs=in_specs,
        out_specs=vm,
        scratch_shapes=scratch,
        compiler_params=pltpu.CompilerParams(
            collective_id=0, has_side_effects=True, vmem_limit_bytes=56 * 1024 * 1024
        ),
    )(
        tokens,
        gain_mix.reshape(1, -1),
        w_query,
        w_key,
        w_value,
        w_igate,
        w_fgate,
        bias_igate,
        bias_fgate,
        state_mem,
        state_max,
        keys_blk,
        values_blk,
        igate_blk,
        fgate_blk,
        lengths,
        gain_head.reshape(1, -1),
        w_mixout,
        gain_mlp.reshape(1, -1),
        w_up,
        w_down,
    )


def flip(index, mask):
    bit = 1
    while bit <= mask:
        if mask & bit:
            index = index + bit * (1 - 2 * lax.rem(lax.div(index, bit), 2))
        bit *= 2
    return index


def stages(kv):
    inner = inner_size(kv)
    outer = kv // inner
    if (inner, outer) != (4, 4):
        return (([m for m in range(inner)], [m * inner for m in range(outer)]),)
    ways = (((1, 2), (4, 8)), ((1, 4), (2, 8)), ((2, 4), (1, 8)))
    return tuple(tuple([0, a, b, a + b] for a, b in way) for way in ways)


def kernel(cfg, names, *refs):
    kv, tp, D = cfg
    r = SimpleNamespace(**dict(zip(names, refs, strict=True)))
    me, core = lax.axis_index("kv"), lax.axis_index("tp")
    inner = inner_size(kv)
    outer = kv // inner
    other = 1 - core
    ways = stages(kv)

    def split(way):
        def place(masks):
            total, step = 0, 1
            while step < len(masks):
                total = total + step * lax.rem(lax.div(me, masks[step]), 2)
                step *= 2
            return total

        return place(way[1]), place(way[0])
    S, H, HD, _ = r.state_mem.shape
    B = r.fgate_blk.shape[2]
    width = H * HD
    R, F = r.tokens.shape
    per = kv // tp
    half = lax.div(me, per)
    jj_me = lax.rem(me, per)
    chunks, _, _, CW = r.up_send.shape
    proj_way = [ways[a % len(ways)] for a in range(4)]
    up_way = [ways[c % len(ways)] for c in range(chunks)]

    cube = kv // 2
    reach = {m for first, _ in ways for m in first if m}
    reach |= {m % cube for _, second in ways for m in second if m % cube}

    barrier = pltpu.get_barrier_semaphore()

    def greet(target, c):
        pl.semaphore_signal(barrier, inc=1, device_id=(target, c), device_id_type=MESH)

    greet(me, other)
    for m in sorted(reach, reverse=True):
        greet(flip(me, m), 1)

    @pl.when(core == 1)
    def _():
        greet(flip(me, cube), 1)


    taken = iter(range(r.local_sem.shape[0]))

    def load(whole, *pieces):
        sem = r.local_sem.at[next(taken)]
        for i, piece in enumerate(pieces):
            dst = whole if len(pieces) == 1 else whole.at[i]
            pltpu.make_async_copy(piece, dst, sem).start()
        return pltpu.make_async_copy(whole, whole, sem)

    got_tokens = load(r.v_tokens, r.tokens)
    got_gain_mix = load(r.v_gain_mix, r.gain_mix)
    got_w_gate = load(r.v_w_gate, r.w_igate, r.w_fgate)
    got_w_qkv = load(r.v_w_qkv, r.w_query, r.w_key, r.w_value)
    got_blk = [
        load(r.v_gate_blk, r.fgate_blk, r.igate_blk),
        load(r.v_lengths, r.lengths),
        load(r.v_state_max, r.state_max),
        load(r.v_bias, r.bias_igate, r.bias_fgate),
    ]
    got_memory = [
        load(r.v_state_mem, r.state_mem),
        load(r.v_kv_blk, r.keys_blk, r.values_blk),
        load(r.v_gain_head, r.gain_head),
    ]
    got_gain_mlp = load(r.v_gain_mlp, r.gain_mlp)

    def loaded(copies):
        for copy in copies:
            copy.wait()

    def remote(src, dst, ssem, rsem, target, c):
        return pltpu.make_async_remote_copy(
            src_ref=src,
            dst_ref=dst,
            send_sem=ssem,
            recv_sem=rsem,
            device_id=(target, c),
            device_id_type=MESH,
        )

    def drain(ref, sem):
        remote(ref, ref, sem, sem, me, other).wait_send()

    tok_copy = remote(
        r.v_tokens, r.tok_peer, r.pair_ssem.at[0], r.pair_rsem.at[0], me, other
    )

    @pl.when(core == 0)
    def _():
        pl.semaphore_wait(barrier, 1)
        pl.semaphore_signal(r.hello_sem, inc=1, device_id=(me, other), device_id_type=MESH)

    @pl.when(core == 1)
    def _():
        pl.semaphore_wait(r.hello_sem, 1)

    got_tokens.wait()
    tok_copy.start()

    loaded([got_gain_mix, got_w_gate])
    lane = lax.broadcasted_iota(jnp.int32, (H, 128), 1)
    sub = lax.broadcasted_iota(jnp.int32, (H, 128), 0)
    pick_i = (lane == sub).astype(F32).astype(BF16)
    pick_f = (lane == sub + H).astype(F32).astype(BF16)
    first = (((0,), (0,)), ((), ()))
    w_gates = (
        lax.dot_general(r.v_w_gate[0], pick_i, first, preferred_element_type=F32)
        + lax.dot_general(r.v_w_gate[1], pick_f, first, preferred_element_type=F32)
    ).astype(BF16)
    lane_r = lax.broadcasted_iota(jnp.int32, (R, 128), 1)
    gain_mix = r.v_gain_mix[...]
    gate_send = r.gate_send
    proj_send = r.proj_send
    send_of = [*(proj_send.at[a] for a in range(3)), gate_send]
    recv_of = [*(r.proj_recv.at[a] for a in range(3)), r.gate_recv]
    mid_of = [*(r.proj_mid.at[a] for a in range(3)), r.gate_mid]
    last_of = [*(r.proj_last.at[a] for a in range(3)), r.gate_last]

    def project(rows, group):
        scaled = (rows * gain_mix).astype(BF16)
        square = jnp.sum(rows * rows, axis=1, keepdims=True)
        gates = jnp.dot(scaled, w_gates, preferred_element_type=F32)
        gates = jnp.where(lane_r == 2 * H, square, gates)
        for jj in range(per):
            gate_send[group * per + jj] = gates[jj * S : (jj + 1) * S]
        for i in range(3):
            part = jnp.dot(scaled, r.v_w_qkv[i], preferred_element_type=F32)
            for jj in range(per):
                proj_send[i, group * per + jj] = part[jj * S : (jj + 1) * S].astype(BF16)

    own_rows = r.v_tokens[...].astype(F32)
    got_w_qkv.wait()
    project(own_rows, core)

    tok_copy.wait_recv()
    project(r.tok_peer[...].astype(F32), other)

    @pl.when(core == 1)
    def _():
        pl.semaphore_wait(barrier, 2 * len(reach) + 2)
        pl.semaphore_signal(r.go_sem, inc=1, device_id=(me, other), device_id_type=MESH)
        pl.semaphore_signal(
            r.half_sem, inc=1, device_id=(flip(me, cube), core), device_id_type=MESH
        )

    @pl.when(core == 0)
    def _():
        pl.semaphore_wait(r.go_sem, 1)


    def pair(i, ref):
        return remote(ref.at[0], ref.at[1], r.pair_ssem.at[i], r.pair_rsem.at[i], me, other)

    pairs = [pair(1, r.v_w_mixout), pair(2, r.v_w_up), pair(3, r.v_w_down)]

    def proj_one(a, mz, mp):
        first, second = proj_way[a]
        return remote(
            send_of[a].at[flip(me, first[mp] + second[mz])],
            recv_of[a].at[mz, mp],
            r.proj_ssem.at[a // 3],
            r.proj_rsem.at[a, mz // (outer // 2)],
            flip(me, first[mp]),
            other,
        )

    def proj_two(a, mz):
        return remote(
            mid_of[a].at[mz],
            last_of[a].at[mz],
            r.mid_ssem.at[a // 3],
            r.mid_rsem.at[a],
            flip(me, proj_way[a][1][mz]),
            other,
        )

    far = [mz for mz in reversed(range(outer)) if mz >= outer // 2]
    near = [mz for mz in reversed(range(outer)) if mz < outer // 2]
    peers = list(reversed(range(inner)))

    def send_groups(a, groups):
        for mz in groups:
            for mp in peers:
                proj_one(a, mz, mp).start()

    for a in (3, 0, 1, 2):
        send_groups(a, far)
        send_groups(a, near)

    got_w_mixout = load(r.v_w_mixout.at[0], r.w_mixout)
    got_w_up = load(r.v_w_up.at[0], r.w_up)
    got_w_down = load(r.v_w_down.at[0], r.w_down)

    loaded(got_memory)

    def narrow(i, carry):
        s, h = lax.div(i, H), lax.rem(i, H)
        r.state_t[s, h] = r.v_state_mem[s, h].T.astype(BF16)
        r.keys_t[s, h] = r.v_kv_blk[0, s, h].T
        return carry

    lax.fori_loop(0, S * H, narrow, 0)
    got_w_mixout.wait()
    pairs[0].start()

    def summed(ref):
        total = ref[0].astype(F32)
        for i in range(1, ref.shape[0]):
            total = total + ref[i].astype(F32)
        return total

    def proj_middle(a):
        for side, groups in ((1, far), (0, near)):
            drain(
                recv_of[a].at[pl.ds(side * (outer // 2), outer // 2)], r.proj_rsem.at[a, side]
            )
            for mz in groups:
                mid_of[a][mz] = summed(recv_of[a].at[mz]).astype(mid_of[a].dtype)
                proj_two(a, mz).start()

    def proj_end(a):
        drain(last_of[a], r.mid_rsem.at[a])
        return summed(last_of[a])

    @pl.when(core == 1)
    def _():
        pl.semaphore_wait(r.half_sem, 1)
        pl.semaphore_signal(r.half_sem, inc=1, device_id=(me, other), device_id_type=MESH)

    @pl.when(core == 0)
    def _():
        pl.semaphore_wait(r.half_sem, 1)

    for a in (3, 0, 1, 2):
        proj_middle(a)
    got_w_up.wait()
    pairs[1].start()

    loaded(got_blk)
    row = lax.broadcasted_iota(jnp.int32, (S, 1), 0)
    eye_s = lax.broadcasted_iota(jnp.int32, (S, S), 0) == lax.broadcasted_iota(jnp.int32, (S, S), 1)
    length = jnp.sum(
        jnp.where(eye_s, r.v_lengths[...].astype(F32), 0.0), axis=1, keepdims=True
    )
    live = lax.broadcasted_iota(jnp.int32, (S, B), 1).astype(F32) < length
    later = (
        lax.broadcasted_iota(jnp.int32, (B, B), 0) > lax.broadcasted_iota(jnp.int32, (B, B), 1)
    ).astype(F32)
    base = []
    for h in range(H):
        forget = jnp.where(live, r.v_gate_blk[0, :, h, :], 0.0)
        suffix = jnp.dot(
            forget, later, preferred_element_type=F32, precision=lax.Precision.HIGHEST
        )
        past = jnp.where(live, r.v_gate_blk[1, :, h, :] + suffix, -jnp.inf)
        carried = r.v_state_max[:, h : h + 1] + jnp.sum(forget, axis=1, keepdims=True)
        base.append((past, jnp.max(past, axis=1, keepdims=True), carried))
    gate_sum = proj_end(3)
    factor_in = lax.rsqrt(gate_sum[:, 2 * H : 2 * H + 1] / D + EPS)
    gate_sum = gate_sum * factor_in
    scale = HD ** (-0.5)
    shares = []
    for h in range(H):
        past, past_top, carried = base[h]
        ig = gate_sum[:, h : h + 1] + r.v_bias[0, :, h : h + 1]
        raw = gate_sum[:, H + h : H + h + 1] + r.v_bias[1, :, h : h + 1]
        fg = jnp.minimum(raw, 0.0) - jnp.log1p(jnp.exp(-jnp.abs(raw)))
        carried = carried + fg
        top = jnp.maximum(jnp.maximum(carried, ig), past_top + fg)
        shares.append((jnp.exp(past + (fg - top)) * scale, jnp.exp(carried - top), jnp.exp(ig - top)))
    query = (proj_end(0) * factor_in).astype(BF16)

    cells, weights_of, state_of = [], [], []
    for h in range(H):
        q = query[:, h * HD : (h + 1) * HD]
        scores = jnp.zeros((S, B), F32)
        for s in range(S):
            got = jnp.dot(q, r.keys_t[s, h], preferred_element_type=F32)
            scores = jnp.where(row == s, got, scores)
        weights_of.append((shares[h][0] * scores).astype(BF16))
    for h in range(H):
        q = query[:, h * HD : (h + 1) * HD]
        state_term = jnp.zeros((S, HD), F32)
        for s in range(S):
            mem = jnp.dot(q, r.state_t[s, h], preferred_element_type=F32)
            state_term = jnp.where(row == s, mem, state_term)
        state_of.append(state_term)
    for h in range(H):
        weights, state_term = weights_of[h], state_of[h]
        _, remaining, entering = shares[h]
        block_term = jnp.zeros((S, HD), F32)
        for s in range(S):
            got = jnp.dot(weights, r.v_kv_blk[1, s, h], preferred_element_type=F32)
            block_term = jnp.where(row == s, got, block_term)
        cells.append((state_term * remaining + block_term, entering))

    key_new = (proj_end(1) * factor_in).astype(BF16)
    value_new = (proj_end(2) * factor_in).astype(BF16)
    for h in range(H):
        cols = slice(h * HD, (h + 1) * HD)
        q, k, v = query[:, cols], key_new[:, cols], value_new[:, cols]
        older, entering = cells[h]
        own = jnp.sum(q.astype(F32) * k.astype(F32), axis=1, keepdims=True) * scale
        numerator = older + (entering * own) * v.astype(F32)
        spread = jnp.mean(numerator * numerator, axis=1, keepdims=True)
        r.mixed_own[:, cols] = (
            numerator * lax.rsqrt(spread + EPS) * r.v_gain_head[...]
        ).astype(BF16)

    mixed_all = r.mixed_all
    slot = lax.rem(half + core, 2)
    mine_at = slot * per + jj_me

    def mix_copy(m):
        return remote(
            r.mixed_own,
            mixed_all.at[mine_at],
            r.mix_ssem,
            r.mix_rsem,
            flip(me, m),
            half,
        )

    for m in reversed(range(1, kv)):
        mix_copy(m).start()

    @pl.when(slot == 1)
    def _():
        mix_copy(0).start()

    @pl.when(slot == 0)
    def _():
        mixed_all[mine_at] = r.mixed_own[...]

    loaded([got_w_down, got_gain_mlp])
    pairs[0].wait()

    @pl.when(half == core)
    def _():
        drain(mixed_all.at[pl.ds(0, kv - 1)], r.mix_rsem)

    @pl.when(half != core)
    def _():
        drain(mixed_all, r.mix_rsem)

    mixed_rows = r.mixed_rows
    attended = jnp.zeros((R, F), F32)
    for c in range(tp):
        for jj in range(per):
            mixed_rows[jj * S : (jj + 1) * S, c * width : (c + 1) * width] = mixed_all[
                c * per + jj
            ].astype(F32)
        attended = attended + jnp.dot(
            mixed_rows[:, c * width : (c + 1) * width].astype(BF16),
            r.v_w_mixout[c],
            preferred_element_type=F32,
        ).astype(BF16).astype(F32)

    restored = (own_rows + attended).astype(BF16).astype(F32)
    r.res_rows[...] = restored
    scaled_mid = (restored * r.v_gain_mlp[...]).astype(BF16)

    up_send, up_recv, up_mid, up_last = r.up_send, r.up_recv, r.up_mid, r.up_last

    def up_one(c, mz, mp):
        place = split(up_way[c])
        return remote(
            up_send.at[c, flip(place[0], mz) * inner + flip(place[1], mp)],
            up_recv.at[c, mz, mp],
            r.up_ssem,
            r.up_rsem.at[c, mz // (outer // 2)],
            flip(me, up_way[c][0][mp]),
            other,
        )

    def up_two(c, mz):
        return remote(
            up_mid.at[c, mz],
            up_last.at[c, mz],
            r.mid_ssem.at[2],
            r.up_lsem.at[c],
            flip(me, up_way[c][1][mz]),
            other,
        )

    parts = chunks // tp
    span = kv * CW

    def up_start(c, groups):
        for mz in groups:
            for mp in peers:
                up_one(c, mz, mp).start()

    def up_compute(c):
        if c == parts:
            pairs[1].wait()
        begin = (c % parts) * span
        part = jnp.dot(
            scaled_mid,
            r.v_w_up[c // parts, :, begin : begin + span],
            preferred_element_type=F32,
        ).astype(BF16)
        for j in range(kv):
            up_send[c, j] = part[:, j * CW : (j + 1) * CW]

    plan = [(c, side) for c in range(chunks) for side in (1, 0)]
    for i, (c, side) in enumerate(plan):
        if c not in [x for x, _ in plan[:i]]:
            up_compute(c)
        up_start(c, far if side else near)
    pairs[2].start()

    square_mid = jnp.sum(restored * restored, axis=1, keepdims=True)
    eye_r = lax.broadcasted_iota(jnp.int32, (R, 128), 0) == lane_r
    r.sq_all[0] = jnp.sum(jnp.where(eye_r, square_mid, 0.0), axis=0, keepdims=True)

    def sq_copy(m):
        return remote(
            r.sq_all.at[0],
            r.sq_all.at[m],
            r.sq_ssem,
            r.sq_rsem,
            flip(me, m),
            core,
        )

    for m in reversed(range(1, kv)):
        sq_copy(m).start()

    def up_middle(c, side):
        drain(up_recv.at[c, pl.ds(side * (outer // 2), outer // 2)], r.up_rsem.at[c, side])
        for mz in far if side else near:
            up_mid[c, mz] = summed(up_recv.at[c, mz]).astype(BF16)
            up_two(c, mz).start()

    hid_mid, hid_all = r.hid_mid, r.hid_all

    def hid_near(c, mp):
        mine = hid_all.at[c, 0, split(up_way[c])[1]]
        return remote(
            mine,
            mine,
            r.hid_ssem.at[2],
            r.hid_rsem.at[c],
            flip(me, up_way[c][0][mp]),
            core,
        )

    def hid_one(c, mz):
        return remote(
            hid_all.at[c, 0, split(up_way[c])[1]],
            hid_mid.at[c, mz],
            r.hid_ssem.at[0],
            r.hid_msem.at[c, mz - 1],
            flip(me, up_way[c][1][mz]),
            other,
        )

    def hid_two(c, mz, mp):
        return remote(
            hid_mid.at[c, mz],
            hid_all.at[c, mz, split(up_way[c])[1]],
            r.hid_ssem.at[1],
            r.hid_rsem.at[c],
            flip(me, up_way[c][0][mp]),
            other,
        )

    def hid_start(c):
        drain(up_last.at[c], r.up_lsem.at[c])
        active = jnp.maximum(summed(up_last.at[c]), 0.0)
        hid_all[c, 0, split(up_way[c])[1]] = (active * active).astype(BF16)
        for mz in reversed(range(1, outer)):
            hid_one(c, mz).start()
        for mp in peers[:-1]:
            hid_near(c, mp).start()

    def hid_relay(c, mz):
        drain(hid_mid.at[c, mz], r.hid_msem.at[c, mz - 1])
        for mp in peers:
            hid_two(c, mz, mp).start()

    def hops(mz):
        return 2.2 + 0.5 * ((mz & 1) + 2 * (mz >> 1)) if mz else 0.9

    steps, ready = [], [0.0] * chunks
    for i, (c, side) in enumerate(plan):
        due = 3.2 * (i + 1) / len(plan) + 2.8
        steps.append((due, up_middle, c, side))
        ready[c] = max([ready[c], *(due + hops(mz) for mz in (far if side else near))])
    for c in range(chunks):
        steps.append((ready[c] + 0.2, hid_start, c))
        for mz in range(1, outer):
            steps.append((ready[c] + 0.4 + hops(mz), hid_relay, c, mz))
    order = [step[1:] for step in sorted(steps, key=lambda step: step[0])]
    for step, *which in order:
        step(*which)

    tok_copy.wait_send()
    for i, (sent, then) in enumerate(((r.proj_recv, r.proj_last), (r.gate_recv, r.gate_last))):
        drain(sent, r.proj_ssem.at[i])
        drain(then, r.mid_ssem.at[i])

    @pl.when(slot == 0)
    def _():
        drain(mixed_all.at[pl.ds(0, kv - 1)], r.mix_ssem)

    @pl.when(slot == 1)
    def _():
        drain(mixed_all, r.mix_ssem)

    drain(r.sq_all.at[pl.ds(1, kv - 1)], r.sq_ssem)
    drain(up_recv, r.up_ssem)
    drain(up_last, r.mid_ssem.at[2])
    pairs[2].wait()
    drain(r.sq_all.at[pl.ds(1, kv - 1)], r.sq_rsem)
    squares = r.sq_all[0]
    for m in range(1, kv):
        squares = squares + r.sq_all[m]
    square_sum = jnp.sum(jnp.where(eye_r, squares, 0.0), axis=1, keepdims=True)
    factor_mid = lax.rsqrt(square_sum / D + EPS)
    drain(hid_mid.at[:, pl.ds(1, outer - 1)], r.hid_ssem.at[0])
    drain(hid_all.at[:, 0, pl.ds(1, inner - 1)], r.hid_ssem.at[2])

    flat = r.up_send.at[0]
    down = jnp.zeros((R, F), F32)
    for c in range(chunks):
        drain(flat.at[pl.ds(0, kv - 1)], r.hid_rsem.at[c])
        for mz in range(outer):
            group = flip(split(up_way[c])[0], mz)
            begin = pl.multiple_of((c % parts) * span + group * (inner * CW), inner * CW)
            down = down + jnp.dot(
                jnp.concatenate([hid_all[c, mz, pt] for pt in range(inner)], axis=1),
                r.v_w_down[c // parts, pl.ds(begin, inner * CW), :],
                preferred_element_type=F32,
            )
    r.out[...] = (r.res_rows[...] + down * (factor_mid * factor_mid)).astype(BF16)
    drain(hid_all.at[:, pl.ds(1, outer - 1)], r.hid_ssem.at[1])


def named(
    tokens,
    gain_mix,
    w_query,
    w_key,
    w_value,
    w_igate,
    w_fgate,
    bias_igate,
    bias_fgate,
    state_mem,
    state_max,
    keys_blk,
    values_blk,
    igate_blk,
    fgate_blk,
    lengths,
    gain_head,
    w_mixout,
    gain_mlp,
    w_up,
    w_down,
):
    return SimpleNamespace(**locals())


def body(kv, tp, *args):
    a = named(*args)
    a.gain_mix, a.gain_head, a.gain_mlp, a.bias_igate, a.bias_fgate, a.lengths = (
        x.reshape(1, -1)
        for x in (a.gain_mix, a.gain_head, a.gain_mlp, a.bias_igate, a.bias_fgate, a.lengths)
    )
    a.w_igate, a.w_fgate = a.w_igate.T, a.w_fgate.T
    rows, feats = a.tokens.shape
    S, H, HD, _ = a.state_mem.shape
    B = a.keys_blk.shape[2]
    width = H * HD
    inner = inner_size(kv)
    outer = kv // inner
    per = kv // tp
    hidden = a.w_up.shape[1]
    chunks = tp * max(n for n in (1, 2) if hidden % (n * kv * 128) == 0)
    cw = hidden * tp // (chunks * kv)
    V = pltpu.VMEM
    dma = pltpu.SemaphoreType.DMA

    def room(x, *many):
        return V((*many, *x.shape), x.dtype)

    scratch = dict(
        v_tokens=room(a.tokens),
        v_gain_mix=room(a.gain_mix),
        v_lengths=room(a.lengths),
        v_state_max=room(a.state_max),
        v_gain_head=room(a.gain_head),
        v_gain_mlp=room(a.gain_mlp),
        v_state_mem=room(a.state_mem),
        v_w_gate=room(a.w_igate, 2),
        v_w_qkv=room(a.w_query, 3),
        v_gate_blk=room(a.fgate_blk, 2),
        v_bias=room(a.bias_igate, 2),
        v_kv_blk=room(a.keys_blk, 2),
        v_w_mixout=room(a.w_mixout, tp),
        v_w_up=room(a.w_up, tp),
        v_w_down=room(a.w_down, tp),
        state_t=V(a.state_mem.shape, BF16),
        keys_t=V((S, H, HD, B), BF16),
        tok_peer=room(a.tokens),
        proj_send=V((3, kv, S, width), BF16),
        proj_recv=V((3, outer, inner, S, width), BF16),
        proj_mid=V((3, outer, S, width), BF16),
        proj_last=V((3, outer, S, width), BF16),
        gate_send=V((kv, S, 128), F32),
        gate_recv=V((outer, inner, S, 128), F32),
        gate_mid=V((outer, S, 128), F32),
        gate_last=V((outer, S, 128), F32),
        mixed_own=V((S, width), BF16),
        mixed_all=V((tp * per, S, width), BF16),
        mixed_rows=V((rows, tp * width), F32),
        res_rows=V((rows, feats), F32),
        sq_all=V((kv, 1, 128), F32),
        up_send=V((chunks, kv, rows, cw), BF16),
        up_recv=V((chunks, outer, inner, rows, cw), BF16),
        up_mid=V((chunks, outer, rows, cw), BF16),
        up_last=V((chunks, outer, rows, cw), BF16),
        hid_mid=V((chunks, outer, rows, cw), BF16),
        hid_all=V((chunks, outer, inner, rows, cw), BF16),
        local_sem=dma((15,)),
        pair_ssem=dma((4,)),
        pair_rsem=dma((4,)),
        proj_ssem=dma((2,)),
        proj_rsem=dma((4, 2)),
        mid_ssem=dma((3,)),
        mid_rsem=dma((4,)),
        mix_ssem=dma,
        mix_rsem=dma,
        sq_ssem=dma,
        sq_rsem=dma,
        up_ssem=dma,
        up_rsem=dma((chunks, 2)),
        up_lsem=dma((chunks,)),
        hid_ssem=dma((3,)),
        hid_msem=dma((chunks, outer - 1)),
        hid_rsem=dma((chunks,)),
        go_sem=pltpu.SemaphoreType.REGULAR,
        half_sem=pltpu.SemaphoreType.REGULAR,
        hello_sem=pltpu.SemaphoreType.REGULAR,
    )
    operands = vars(a)
    names = (*operands, "out", *scratch)
    return pl.pallas_call(
        functools.partial(kernel, (kv, tp, kv * feats), names),
        out_shape=V((rows, feats), BF16),
        in_specs=[pl.BlockSpec(memory_space=pl.ANY)] * len(operands),
        out_specs=pl.BlockSpec(memory_space=V),
        scratch_shapes=list(scratch.values()),
        compiler_params=pltpu.CompilerParams(
            collective_id=0, has_side_effects=True, vmem_limit_bytes=56 * 1024 * 1024
        ),
    )(*operands.values())


def suits(kv, tp, *args):
    a = named(*args)
    inner = inner_size(kv)
    outer = kv // inner
    return (
        tp == 2
        and kv & (kv - 1) == 0
        and outer > 1
        and inner > 1
        and a.tokens.shape[1] % 128 == 0
        and a.tokens.shape[0] <= 128
        and a.w_up.shape[1] % (kv * 128) == 0
    )


def either(kv, tp, *args):
    return (body if suits(kv, tp, *args) else any_body)(kv, tp, *args)


def solution(mesh):
    in_specs = (
        P("tp", "kv"),
        P("kv"),
        P("kv", "tp"),
        P("kv", "tp"),
        P("kv", "tp"),
        P("kv", "tp"),
        P("kv", "tp"),
        P("tp"),
        P("tp"),
        P("kv", "tp", None, None),
        P("kv", "tp"),
        P("kv", "tp", None, None),
        P("kv", "tp", None, None),
        P("kv", "tp", None),
        P("kv", "tp", None),
        P("kv"),
        P(),
        P("tp", "kv"),
        P("kv"),
        P("kv", "tp"),
        P("tp", "kv"),
    )
    out_specs = P("tp", "kv")
    run = functools.partial(either, mesh.shape["kv"], mesh.shape["tp"])
    return jax.shard_map(run, mesh=mesh, in_specs=in_specs, out_specs=out_specs, check_vma=False)
```
